32 devices in a mesh: rep: 2 (over y), fs: 4 (over z), tp: 4 (over x, core).
Axes of the slice: x: 2, y: 2, z: 4, core: 2. Of those that a mesh axis runs over, the one named last changes fastest.
Arguments:
- stream: bfloat16 [2048, 2048], P(('rep', 'fs')), may hold values from -6 to 6
- gain_mix: float32 [2048], replicated, may hold values from 0.1 to 1.9
- w_query: float32 [2048, 2048], P('fs', 'tp'), may hold values from -0.125 to 0.125
- scale_query: float32 [2048], P('tp'), may hold values from 0.5 to 2
- w_key: float32 [2048, 2048], P('fs', 'tp'), may hold values from -0.125 to 0.125
- scale_key: float32 [2048], P('tp'), may hold values from 0.5 to 2
- w_value: float32 [2048, 2048], P('fs', 'tp'), may hold values from -0.125 to 0.125
- scale_value: float32 [2048], P('tp'), may hold values from 0.5 to 2
- gain_ffn: float32 [2048], replicated, may hold values from 0.1 to 1.9
- w_gate: float32 [2048, 2816], P('fs', 'tp'), may hold values from -0.125 to 0.125
- scale_gate: float32 [2816], P('tp'), may hold values from 0.5 to 2
- w_up: float32 [2048, 2816], P('fs', 'tp'), may hold values from -0.125 to 0.125
- scale_up: float32 [2816], P('tp'), may hold values from 0.5 to 2
- w_down: float32 [2048, 2816], P('fs', 'tp'), may hold values from -0.109375 to 0.109375
- scale_down: float32 [2048], P('fs'), may hold values from 0.5 to 2
Outputs:
- layer_out: bfloat16 [2048, 2048], P(('rep', 'fs', 'tp'))
The draws below stay inside these ranges and needn't reach their ends.
All inputs are finite; a program needn't handle non-finite values.
Results may differ from the reference program's by a relative error of at most 0.015.
Values may be sent and summed in bfloat16 or wider, within the bound.
A program may use at most 64 MiB of HBM per device.

```python
import math
import jax
import jax.numpy as jnp
from jax import lax

D = 2048
HEADS = 8
DK = 256
DV = 256
FF = 2816
LEN = 128
BLK = 64
TOKENS = 2048
N_TP = 4


def block_scale(stream_key, shape, pieces, smallest, top_value):
    factor_of = 1.0
    for position, parts in pieces:
        heights = jax.random.uniform(jax.random.fold_in(jax.random.fold_in(stream_key, 6), position), (parts,), jnp.float32, smallest / len(pieces), top_value / len(pieces))
        factor_of = factor_of * jnp.repeat(jnp.exp(heights), shape[position] // parts).reshape((-1,) + (1,) * (len(shape) - 1 - position))
    return factor_of


def scatter_about(rng, extent, width, reach, cuts=(), kind=jnp.bfloat16):
    level = block_scale(rng, extent, cuts, -0.22, 0.18) if cuts else 1.0
    drawn = jax.random.normal(rng, extent, jnp.float32) * width * level
    return jnp.minimum(jnp.maximum(drawn, -reach), reach).astype(kind)


def setup_inputs(seed: int = 0) -> dict:
    arg_keys = jax.random.split(jax.random.key(seed), 16)
    return {
        "stream": scatter_about(arg_keys[0], (TOKENS, D), 1.0, 6.0, ((0, 8),)),
        "gain_mix": jnp.clip(1.0 + 0.18 * jax.random.normal(arg_keys[1], (D,), jnp.float32), 0.1, 1.9),
        "w_query": scatter_about(arg_keys[2], (D, HEADS * DK), D ** -0.5, 0.125, ((0, 4), (1, 4)), jnp.float32),
        "scale_query": jnp.clip(jnp.exp(math.log(2.0) - 1.3862944 * jax.random.uniform(arg_keys[3], (HEADS * DK,), jnp.float32) ** block_scale(arg_keys[3], (HEADS * DK,), ((0, 4),), -0.2, 0.2)), 0.5, 2.0),
        "w_key": scatter_about(arg_keys[4], (D, HEADS * DK), D ** -0.5, 0.125, ((0, 4), (1, 4)), jnp.float32),
        "scale_key": jnp.clip(jnp.exp(math.log(2.0) - 1.3862944 * jax.random.uniform(arg_keys[5], (HEADS * DK,), jnp.float32) ** block_scale(arg_keys[5], (HEADS * DK,), ((0, 4),), -0.2, 0.2)), 0.5, 2.0),
        "w_value": scatter_about(arg_keys[6], (D, HEADS * DV), D ** -0.5, 0.125, ((0, 4), (1, 4)), jnp.float32),
        "scale_value": jnp.clip(jnp.exp(math.log(2.0) - 1.3862944 * jax.random.uniform(arg_keys[7], (HEADS * DV,), jnp.float32) ** block_scale(arg_keys[7], (HEADS * DV,), ((0, 4),), -0.2, 0.2)), 0.5, 2.0),
        "gain_ffn": jnp.clip(1.0 + 0.18 * jax.random.normal(arg_keys[8], (D,), jnp.float32), 0.1, 1.9),
        "w_gate": scatter_about(arg_keys[9], (D, FF), D ** -0.5, 0.125, ((0, 4), (1, 4)), jnp.float32),
        "scale_gate": jnp.clip(jnp.exp(math.log(2.0) - 1.3862944 * jax.random.uniform(arg_keys[10], (FF,), jnp.float32) ** block_scale(arg_keys[10], (FF,), ((0, 4),), -0.2, 0.2)), 0.5, 2.0),
        "w_up": scatter_about(arg_keys[11], (D, FF), D ** -0.5, 0.125, ((0, 4), (1, 4)), jnp.float32),
        "scale_up": jnp.clip(jnp.exp(math.log(2.0) - 1.3862944 * jax.random.uniform(arg_keys[12], (FF,), jnp.float32) ** block_scale(arg_keys[12], (FF,), ((0, 4),), -0.2, 0.2)), 0.5, 2.0),
        "w_down": scatter_about(arg_keys[13], (D, FF), FF ** -0.5, 0.109375, ((0, 4), (1, 4)), jnp.float32),
        "scale_down": jnp.clip(jnp.exp(math.log(2.0) - 1.3862944 * jax.random.uniform(arg_keys[14], (D,), jnp.float32) ** block_scale(arg_keys[14], (D,), ((0, 4),), -0.2, 0.2)), 0.5, 2.0),
    }


EPS = 1e-06
THETA = 10000.0
HIGH = lax.Precision.HIGHEST

def rms_scale(values):
    return lax.rsqrt(lax.optimization_barrier(jnp.mean(values * values, axis=-1, keepdims=True)) + EPS)

def head_scale(values):
    return 1.0 / jnp.maximum(jnp.sqrt(lax.optimization_barrier(jnp.mean(values * values, axis=-1, keepdims=True))), 1.0)

def rotate(heads_data, positions):
    half = heads_data.shape[-1] // 2
    frequency = THETA ** (-(jnp.arange(half, dtype=jnp.float32) / half))
    angle = positions.astype(jnp.float32)[:, None, None] * frequency
    cosine = jnp.cos(angle)
    sine = jnp.sin(angle)
    first = heads_data[..., :half]
    second = heads_data[..., half:]
    return jnp.concatenate([first * cosine - second * sine, second * cosine + first * sine], axis=-1)

def retention_blocks(queries, keys, values, log_decay):
    total_rows, heads, key_width = queries.shape
    value_width = values.shape[-1]
    queries = queries.reshape((-1, LEN // BLK, BLK, heads, key_width))
    keys = keys.reshape((-1, LEN // BLK, BLK, heads, key_width))
    values = values.reshape((-1, LEN // BLK, BLK, heads, value_width))
    offsets = jnp.arange(BLK, dtype=jnp.float32)
    distance = offsets[:, None] - offsets[None, :]
    decay_mask = jnp.where(distance >= 0, jnp.exp(log_decay[:, None, None] * jnp.maximum(distance, 0.0)), 0.0)
    scores = jnp.einsum('snihd,snjhd->snhij', queries, keys, precision=HIGH) * decay_mask
    inner = jnp.einsum('snhij,snjhe->snihe', scores, values, precision=HIGH)
    query_decay = jnp.exp(log_decay[None, :] * (offsets[:, None] + 1.0))[:, :, None]
    key_decay = jnp.exp(log_decay[None, :] * (BLK - 1.0 - offsets[:, None]))[:, :, None]
    block_decay = jnp.exp(log_decay * BLK)[None, :, None, None]

    def advance(state, inputs):
        block_query, block_key, block_value = inputs
        carried = jnp.einsum('sihd,shde->sihe', block_query, state, precision=HIGH)
        state = state * block_decay + jnp.einsum('sjhd,sjhe->shde', block_key, block_value, precision=HIGH)
        return (state, carried)
    moved = (jnp.moveaxis(queries * query_decay, 1, 0), jnp.moveaxis(keys * key_decay, 1, 0), jnp.moveaxis(values, 1, 0))
    initial = jnp.zeros((queries.shape[0], heads, key_width, value_width), jnp.float32)
    _, carried = lax.scan(advance, initial, moved)
    return (inner + jnp.moveaxis(carried, 0, 1)).reshape(total_rows, heads, value_width)

def reference(stream, gain_mix, w_query, scale_query, w_key, scale_key, w_value, scale_value, gain_ffn, w_gate, scale_gate, w_up, scale_up, w_down, scale_down):
    stream_f = stream.astype(jnp.float32)
    normed = (stream_f * rms_scale(stream_f) * gain_mix).astype(jnp.bfloat16)

    def project(weight, scale):
        return (jnp.dot(normed, weight.astype(jnp.bfloat16), preferred_element_type=jnp.float32) * scale).astype(jnp.bfloat16)
    query = project(w_query, scale_query)
    key = project(w_key, scale_key)
    value = project(w_value, scale_value)
    total_rows = stream.shape[0]
    positions = jnp.arange(total_rows, dtype=jnp.int32) % LEN
    queries = rotate(query.astype(jnp.float32).reshape(total_rows, HEADS, DK), positions)
    keys = rotate(key.astype(jnp.float32).reshape(total_rows, HEADS, DK), positions) * DK ** (-0.5)
    values = value.astype(jnp.float32).reshape(total_rows, HEADS, DV)
    log_decay = jnp.log(1.0 - jnp.power(2.0, -5.0 - jnp.arange(HEADS, dtype=jnp.float32)))
    retained = retention_blocks(queries, keys, values, log_decay)
    mixed = (retained * head_scale(retained)).astype(jnp.bfloat16).reshape(total_rows, HEADS * DV)
    resid = stream_f + mixed.astype(jnp.float32)
    normed_ffn = (resid * rms_scale(resid) * gain_ffn).astype(jnp.bfloat16)
    gate = jnp.dot(normed_ffn, w_gate.astype(jnp.bfloat16), preferred_element_type=jnp.float32) * scale_gate
    upward = jnp.dot(normed_ffn, w_up.astype(jnp.bfloat16), preferred_element_type=jnp.float32) * scale_up
    hidden = (jax.nn.silu(gate) * upward).astype(jnp.bfloat16)
    down_rounded = w_down.astype(jnp.bfloat16)
    block_width = FF // N_TP
    channel_out = jnp.zeros((total_rows, D), jnp.float32)
    for number in range(N_TP):
        piece = hidden[:, number * block_width:(number + 1) * block_width]
        columns = down_rounded[:, number * block_width:(number + 1) * block_width]
        partial_sum = lax.dot_general(piece, columns, (((1,), (1,)), ((), ())), preferred_element_type=jnp.float32) * scale_down
        partial_sum = lax.optimization_barrier(partial_sum.astype(jnp.bfloat16))
        channel_out = channel_out + partial_sum.astype(jnp.float32)
    return (resid + channel_out).astype(jnp.bfloat16)
```

```python
import numpy as np
import jax
import jax.numpy as jnp
from jax import lax
from jax.experimental import pallas as pl
from jax.experimental.pallas import tpu as pltpu
from jax.sharding import PartitionSpec as P

DK = 256
DV = 256
LEN = 128


EPS = 1e-06
THETA = 10000.0
HIGH = lax.Precision.HIGHEST


def rms_scale(values):
    return lax.rsqrt(jnp.mean(values * values, axis=-1, keepdims=True) + EPS)


def head_scale(values):
    return 1.0 / jnp.maximum(jnp.sqrt(jnp.mean(values * values, axis=-1, keepdims=True)), 1.0)


def rotate(heads_data, positions):
    half = heads_data.shape[-1] // 2
    frequency = THETA ** (-(jnp.arange(half, dtype=jnp.float32) / half))
    angle = positions.astype(jnp.float32)[:, None] * frequency
    cosine = jnp.cos(angle)
    sine = jnp.sin(angle)
    first = heads_data[..., :half]
    second = heads_data[..., half:]
    return jnp.concatenate(
        [first * cosine - second * sine, second * cosine + first * sine], axis=-1
    )


def retention(queries, keys, values, log_decay):
    offsets = jnp.arange(LEN, dtype=jnp.float32)
    distance = offsets[:, None] - offsets[None, :]
    decay = jnp.where(distance >= 0, jnp.exp(log_decay * jnp.maximum(distance, 0.0)), 0.0)
    queries, keys, values = (
        part.reshape(-1, LEN, part.shape[-1]) for part in (queries, keys, values)
    )
    scores = jnp.einsum("sid,sjd->sij", queries, keys, precision=HIGH) * decay
    retained = jnp.einsum("sij,sje->sie", scores, values, precision=HIGH)
    return retained.reshape(-1, values.shape[-1])


def dot(left, right):
    return jnp.dot(left, right, preferred_element_type=jnp.float32)


def dot_t(left, right):
    return lax.dot_general(left, right, (((1,), (1,)), ((), ())), preferred_element_type=jnp.float32)


MESH = pl.DeviceIdType.MESH
PIECES = 8
HALF = PIECES // 2


def greet(peers):
    barrier = pltpu.get_barrier_semaphore()
    total = 0
    for axis, count in peers:
        me = lax.axis_index(axis)
        for step in range(1, count):
            peer = lax.rem(me + step, count)
            pl.semaphore_signal(barrier, inc=1, device_id={axis: peer}, device_id_type=MESH)
            total += 1
    pl.semaphore_wait(barrier, total)


def remote(source, target, send, recv, device):
    return pltpu.make_async_remote_copy(
        src_ref=source,
        dst_ref=target,
        send_sem=send,
        recv_sem=recv,
        device_id=device,
        device_id_type=MESH,
    )


def span(index, size):
    return pl.ds(pl.multiple_of(index * size, size), size)


def layer_kernel(
    stream, w_query, w_key, w_value, w_gate, w_up, w_down, decays,
    cosine, sine, gain_mix, gain_ffn, scale_query, scale_key, scale_value, scale_gate, scale_up,
    scale_down,
    out,
    f_query, f_key, f_value, f_gate, f_up, f_down, rows, decay,
    mix_w, up_w, down_w, normed, end_rows, mix_acc, mixed, arrived, resid, normed_ffn, up_acc,
    hidden, partial, from_core, from_diag, from_line, paired, final, down_scale,
    local, z_send, z_recv, y_send, y_recv, scale_send, scale_recv, end_send, end_recv,
    norm_send, norm_recv, mix_send, mix_recv, row_send, row_recv, core_send, core_recv,
    line_send, line_recv, out_send, out_recv,
):
    z, y, t = lax.axis_index("fs"), lax.axis_index("rep"), lax.axis_index("tp")
    group, width = stream.shape
    share = group // 4
    depth, heads_width = w_query.shape
    units = w_gate.shape[1]
    whole = units // 128 * 128
    rest = units - whole
    piece = depth // PIECES
    local_heads = heads_width // DK
    middle = (z == 1) | (z == 2)
    end = jnp.where(z == 1, 0, 3)
    other = 3 - z
    other_end = 3 - end
    partner = t + 1 - 2 * lax.rem(t, 2)
    twin = lax.rem(t + 2, 4)
    diagonal = lax.rem(partner + 2, 4)

    loads = [
        pltpu.make_async_copy(source, target, local.at[index])
        for index, (source, target) in enumerate(
            (
                (w_query, f_query), (w_key, f_key), (w_value, f_value), (stream, rows),
                (w_gate, f_gate), (w_up, f_up), (w_down, f_down),
                (decays.at[pl.ds(t * local_heads, local_heads)], decay),
            )
        )
    ]
    for load in loads:
        load.start()

    def cast(matrix, number):
        here = span(number, piece)
        there = pl.ds(pl.multiple_of(z * depth + number * piece, piece), piece)
        if matrix == 0:
            for place, full in enumerate((f_query, f_key, f_value)):
                columns = slice(place * heads_width, (place + 1) * heads_width)
                mix_w[there, columns] = full[here, :].astype(jnp.bfloat16)
        elif matrix == 1:
            up_w[there, :whole] = f_gate[here, :whole].astype(jnp.bfloat16)
            up_w[there, whole : 2 * whole] = f_up[here, :whole].astype(jnp.bfloat16)
            if rest:
                last = jnp.concatenate([f_gate[here, whole:], f_up[here, whole:]], axis=1)
                up_w[there, 2 * whole :] = last.astype(jnp.bfloat16)
        else:
            down_w[there, :] = f_down[here, :].astype(jnp.bfloat16)

    needs = ((0, 1, 2), (4, 5), (6,))
    weights = (mix_w, up_w, down_w)

    def z_copy(matrix, slot, block, number, target):
        part = pl.ds(pl.multiple_of(block * depth + number * piece, piece), piece)
        view = weights[matrix].at[part]
        return remote(
            view, view, z_send.at[matrix, slot, number], z_recv.at[matrix, slot, number],
            {"fs": target},
        )

    def y_copy(matrix, slot, block, number):
        part = pl.ds(pl.multiple_of(block * depth + number * piece, piece), piece)
        view = weights[matrix].at[part]
        return remote(
            view, view, y_send.at[matrix, slot, number], y_recv.at[matrix, slot, number],
            {"rep": 1 - y},
        )

    def rms_rows(values, gain):
        factor = lax.rsqrt(jnp.mean(values * values, axis=1, keepdims=True) + EPS)
        return (values * factor * gain).astype(jnp.bfloat16)

    def end_copy(target):
        return remote(
            rows.at[span(t, share)], end_rows, end_send.at[0], end_recv.at[0], {"fs": target}
        )

    def scale_copy(index, target):
        return remote(
            scale_down, down_scale.at[z], scale_send.at[index], scale_recv.at[z], {"fs": target}
        )

    greet((("fs", 4), ("rep", 2), ("tp", 4)))

    @pl.when(jnp.logical_not(middle))
    def _():
        near = jnp.where(z == 0, 1, 2)
        loads[3].wait()
        end_copy(near).start()
        for index in range(2):
            scale_copy(index, index + 1).start()
        queue = []
        for matrix in range(3):
            for index in needs[matrix]:
                loads[index].wait()
            for step in range(PIECES):
                number = lax.rem(HALF * y + step, PIECES)
                cast(matrix, number)
                copy = z_copy(matrix, 0, z, number, near)
                copy.start()
                queue.append(copy)
                if len(queue) > 3:
                    queue.pop(0).wait_send()
        for copy in queue:
            copy.wait_send()
        loads[7].wait()
        end_copy(near).wait_send()
        for index in range(2):
            scale_copy(index, index + 1).wait_send()
        for block in range(4):
            part = final.at[block, pl.ds(0, share)]
            remote(part, part, out_send.at[block], out_recv.at[block], {"fs": near}).wait_recv()
        for block in range(4):
            out[:, block * depth : (block + 1) * depth] = final[block, :share, :]

    @pl.when(middle)
    def _():
        def own_send(matrix):
            for step in range(HALF):
                z_copy(matrix, 1, z, HALF * y + step, other).start()

        def cast_half(matrix, half):
            for step in range(HALF):
                cast(matrix, HALF * half + step)

        def pump_near(matrix, step):
            number = HALF * y + step
            z_copy(matrix, 0, end, number, other).wait_recv()
            z_copy(matrix, 2, end, number, other).start()
            z_copy(matrix, 1, other, number, other).wait_recv()
            y_copy(matrix, 0, other, number).start()

        def pump_far(matrix, step):
            number = HALF * y + step
            z_copy(matrix, 2, other_end, number, other).wait_recv()
            y_copy(matrix, 1, other_end, number).start()

        def wait_end(matrix):
            for step in range(HALF):
                z_copy(matrix, 0, end, HALF * (1 - y) + step, other).wait_recv()

        def wait_y(matrix, slot):
            block = (other, other_end)[slot]
            for step in range(HALF):
                y_copy(matrix, slot, block, HALF * (1 - y) + step).wait_recv()

        def norm_copy(step, owner):
            part = normed.at[:, pl.ds(pl.multiple_of(group + owner * share, share), share)]
            peer = lax.rem(t + step, 4)
            return remote(part, part, norm_send.at[step - 1], norm_recv.at[step - 1], {"tp": peer})

        def mix_copy(g, step, peer, owner):
            return remote(
                mixed.at[pl.ds(pl.multiple_of(g * group + peer * share, share), share)],
                arrived.at[owner, pl.ds(g * share, share)],
                mix_send.at[g, step - 1],
                mix_recv.at[g, step - 1],
                {"tp": lax.rem(t + step, 4)},
            )

        def row_copy(g, way, owner):
            part = normed_ffn.at[
                pl.ds(pl.multiple_of(owner * 2 * share + g * share, share), share)
            ]
            return remote(
                part, part, row_send.at[g, way], row_recv.at[g, way],
                {"tp": twin if way == 1 else partner},
            )

        def project(block, first):
            left = normed[block]
            step = depth
            for start in range(0, 3 * heads_width, step):
                columns = slice(start, start + step)
                product = dot(left, mix_w[span(block, depth), columns])
                if first:
                    mix_acc[:, columns] = product
                else:
                    mix_acc[:, columns] += product

        def retain(g, s):
            here = slice(g * group + s * LEN, g * group + (s + 1) * LEN)
            cos, sin = cosine[...], sine[...]

            def turned(offset, scale):
                values = mix_acc[here, offset : offset + DK] * scale
                values = values.astype(jnp.bfloat16).astype(jnp.float32)
                first, second = values[:, : DK // 2], values[:, DK // 2 :]
                return jnp.concatenate(
                    [first * cos - second * sin, second * cos + first * sin], axis=1
                ).astype(jnp.bfloat16)

            for head in range(local_heads):
                columns = slice(head * DK, (head + 1) * DK)
                queries = turned(head * DK, scale_query[:, columns])
                keys = turned(heads_width + head * DK, scale_key[:, columns])
                start = 2 * heads_width + head * DV
                values = (mix_acc[here, start : start + DV] * scale_value[:, columns]).astype(
                    jnp.bfloat16
                )
                scores = (dot_t(queries, keys) * decay[head]).astype(jnp.bfloat16)
                retained = dot(scores, values)
                mixed[here, columns] = (retained * head_scale(retained)).astype(jnp.bfloat16)

        def send_mixed(g):
            for step in range(1, 4):
                mix_copy(g, step, lax.rem(t + step, 4), t).start()
            own = mixed[pl.ds(pl.multiple_of(g * group + t * share, share), share), :]
            arrived[t, g * share : (g + 1) * share, :] = own

        def norm_ffn(g):
            for step in range(1, 4):
                mix_copy(g, step, t, lax.rem(t + 4 - step, 4)).wait_recv()
            here = slice(g * share, (g + 1) * share)
            squares = 0.0
            for block in range(4):
                columns = slice(block * depth, (block + 1) * depth)
                base = rows[span(t, share), columns] if g == 0 else end_rows[:, columns]
                values = base.astype(jnp.float32) + arrived[block, here, :].astype(jnp.float32)
                resid[block, here, :] = values
                squares += jnp.sum(values * values, axis=1, keepdims=True)
            factor = lax.rsqrt(squares / width + EPS)
            target = pl.ds(pl.multiple_of(t * 2 * share + g * share, share), share)
            for block in range(4):
                columns = slice(block * depth, (block + 1) * depth)
                normed_ffn[target, columns] = (
                    resid[block, here, :] * factor * gain_ffn[:, columns]
                ).astype(jnp.bfloat16)
            row_copy(g, 0, t).start()
            row_copy(g, 1, t).start()

        def forward_rows(g):
            row_copy(g, 1, twin).wait_recv()
            row_copy(g, 2, twin).start()

        def hidden_rows(side):
            here = span(side, group)
            left = normed_ffn[here, :]
            for start in range(0, 2 * units, 512):
                columns = slice(start, min(start + 512, 2 * units))
                up_acc[:, columns] = dot(left, up_w[:, columns])

            def gated(gate, upward):
                return (gate / (1.0 + jnp.exp(-gate)) * upward).astype(jnp.bfloat16)

            hidden[here, :whole] = gated(
                up_acc[:, :whole] * scale_gate[:, :whole],
                up_acc[:, whole : 2 * whole] * scale_up[:, :whole],
            )
            if rest:
                last = up_acc[:, 2 * whole :]
                hidden[here, whole:] = gated(
                    last[:, :rest] * scale_gate[:, whole:], last[:, rest:] * scale_up[:, whole:]
                )

        def core_copy(k, way):
            part = span(partner if way == 0 else diagonal, 2 * share)
            return remote(
                partial.at[k, part],
                (from_core if way == 0 else from_diag).at[k],
                core_send.at[k, way],
                core_recv.at[k, way],
                {"tp": partner},
            )

        def line_copy(k):
            return remote(
                paired.at[k], from_line.at[k], line_send.at[k], line_recv.at[k], {"tp": twin}
            )

        def out_copy(block):
            return remote(
                final.at[block, pl.ds(share, share)],
                final.at[block, pl.ds(0, share)],
                out_send.at[block],
                out_recv.at[block],
                {"fs": end},
            )

        def down(k, block):
            products = dot_t(hidden[...], down_w[span(block, depth), :])
            partial[k] = (products * down_scale[block]).astype(jnp.bfloat16)
            core_copy(k, 0).start()
            core_copy(k, 1).start()

        def pair(k):
            core_copy(k, 1).wait_recv()
            mine = partial[k, span(twin, 2 * share), :].astype(jnp.float32)
            paired[k] = (mine + from_diag[k].astype(jnp.float32)).astype(jnp.bfloat16)
            line_copy(k).start()

        def finish(k, block):
            core_copy(k, 0).wait_recv()
            line_copy(k).wait_recv()
            total = partial[k, span(t, 2 * share), :].astype(jnp.float32)
            total += from_core[k].astype(jnp.float32)
            total += from_line[k].astype(jnp.float32)
            final[block] = (resid[block] + total).astype(jnp.bfloat16)
            out_copy(block).start()

        scale_copy(0, other).start()
        for index in needs[0]:
            loads[index].wait()
        cast_half(0, y)
        own_send(0)
        cast_half(0, 1 - y)
        loads[3].wait()
        for start in range(0, group, share):
            values = rms_rows(rows[start : start + share, :].astype(jnp.float32), gain_mix[...])
            for block in range(4):
                normed[block, start : start + share, :] = values[
                    :, block * depth : (block + 1) * depth
                ]
        end_copy(end).wait_recv()
        values = rms_rows(end_rows[...].astype(jnp.float32), gain_mix[...])
        target = pl.ds(pl.multiple_of(group + t * share, share), share)
        for block in range(4):
            normed[block, target, :] = values[:, block * depth : (block + 1) * depth]
        for step in range(1, 4):
            norm_copy(step, t).start()
        pump_near(0, 0)
        for index in needs[1]:
            loads[index].wait()
        cast_half(1, y)
        pump_near(0, 1)
        cast_half(1, 1 - y)
        pump_near(0, 2)
        loads[6].wait()
        loads[7].wait()
        for half in range(2):
            cast_half(2, half)
        pump_near(0, 3)
        own_send(1)
        for step in range(1, 4):
            norm_copy(step, lax.rem(t + 4 - step, 4)).wait_recv()
        project(z, True)
        pump_far(0, 0)
        pump_far(0, 1)
        wait_y(0, 0)
        project(other, False)
        pump_far(0, 2)
        pump_far(0, 3)
        wait_end(0)
        project(end, False)
        wait_y(0, 1)
        project(other_end, False)

        retain(0, 0)
        pump_near(1, 0)
        retain(0, 1)
        send_mixed(0)
        pump_near(1, 1)
        retain(1, 0)
        pump_near(1, 2)
        retain(1, 1)
        send_mixed(1)
        pump_near(1, 3)
        own_send(2)
        norm_ffn(0)
        norm_ffn(1)
        pump_far(1, 0)
        forward_rows(0)
        pump_far(1, 1)
        pump_far(1, 2)
        forward_rows(1)
        pump_far(1, 3)
        wait_end(1)
        wait_y(1, 0)
        for g in range(2):
            row_copy(g, 0, partner).wait_recv()
        pump_near(2, 0)
        wait_y(1, 1)
        x = t // 2
        hidden_rows(x)
        pump_near(2, 1)
        for g in range(2):
            row_copy(g, 2, diagonal).wait_recv()
        hidden_rows(1 - x)
        pump_near(2, 2)
        pump_near(2, 3)
        down_scale[z] = scale_down[...]
        for source in range(4):
            @pl.when(source != z)
            def _():
                remote(
                    down_scale.at[source], down_scale.at[source], scale_send.at[0],
                    scale_recv.at[source], {"fs": other},
                ).wait_recv()
        down(0, z)
        pump_far(2, 0)
        pump_far(2, 1)
        pair(0)
        pump_far(2, 2)
        pump_far(2, 3)
        wait_y(2, 0)
        down(1, other)
        finish(0, z)
        pair(1)
        wait_end(2)
        down(2, end)
        finish(1, other)
        pair(2)
        wait_y(2, 1)
        down(3, other_end)
        finish(2, end)
        pair(3)
        finish(3, other_end)
        for block in range(4):
            out[:, block * depth : (block + 1) * depth] = final[block, :share, :]

        scale_copy(0, other).wait_send()
        for matrix in range(3):
            for step in range(HALF):
                number = HALF * y + step
                for slot in (1, 2):
                    z_copy(matrix, slot, z, number, other).wait_send()
                for slot in (0, 1):
                    y_copy(matrix, slot, z, number).wait_send()
        for step in range(1, 4):
            norm_copy(step, t).wait_send()
            for g in range(2):
                mix_copy(g, step, t, t).wait_send()
        for g in range(2):
            for way in range(3):
                row_copy(g, way, t).wait_send()
        for k in range(4):
            core_copy(k, 0).wait_send()
            core_copy(k, 1).wait_send()
            line_copy(k).wait_send()
            out_copy(k).wait_send()


ANYWHERE = pl.BlockSpec(memory_space=pl.ANY)
INSIDE = pl.BlockSpec(memory_space=pltpu.VMEM)


def tables(heads):
    places = np.arange(LEN, dtype=np.float64)
    half = DK // 2
    frequency = (THETA ** (-(np.arange(half) / half))).astype(np.float32)
    angle = (places[:, None].astype(np.float32) * frequency).astype(np.float32)
    distance = places[:, None] - places[None, :]
    gamma = 1.0 - 2.0 ** (-5.0 - np.arange(heads, dtype=np.float64))
    powers = gamma[:, None, None] ** np.maximum(distance, 0.0)
    decay = np.where(distance >= 0, powers, 0.0) * DK ** (-0.5)
    wide = angle.astype(np.float64)
    return (
        decay.astype(np.float32),
        np.cos(wide).astype(np.float32),
        np.sin(wide).astype(np.float32),
    )


def layer(stream, gains, mix_w, mix_scales, up_w, up_scales, w_down, scale_down, tp_count):
    group, width = stream.shape
    share = group // tp_count
    depth, heads_width = mix_w[0].shape
    units = w_down.shape[1]
    blocks = width // depth
    narrow, wide = jnp.bfloat16, jnp.float32
    local_heads = heads_width // DK
    decays, cosine, sine = tables(local_heads * tp_count)
    row = lambda vector: vector[None, :]
    dma = pltpu.SemaphoreType.DMA
    scratch = (
        [pltpu.VMEM(w.shape, wide) for w in (*mix_w, *up_w, w_down)]
        + [
            pltpu.VMEM(stream.shape, narrow),
            pltpu.VMEM((local_heads, LEN, LEN), wide),
            pltpu.VMEM((width, 3 * heads_width), narrow),
            pltpu.VMEM((width, 2 * units), narrow),
            pltpu.VMEM((width, units), narrow),
            pltpu.VMEM((blocks, 2 * group, depth), narrow),
            pltpu.VMEM((share, width), narrow),
            pltpu.VMEM((2 * group, 3 * heads_width), wide),
            pltpu.VMEM((2 * group, heads_width), narrow),
            pltpu.VMEM((tp_count, 2 * share, heads_width), narrow),
            pltpu.VMEM((blocks, 2 * share, depth), wide),
            pltpu.VMEM((2 * group, width), narrow),
            pltpu.VMEM((group, 2 * units), wide),
            pltpu.VMEM((2 * group, units), narrow),
            pltpu.VMEM((blocks, 2 * group, depth), narrow),
        ]
        + [pltpu.VMEM((blocks, 2 * share, depth), narrow)] * 5
        + [pltpu.VMEM((blocks, 1, depth), wide)]
        + [
            dma((8,)),
            dma((3, 3, PIECES)), dma((3, 3, PIECES)), dma((3, 2, PIECES)), dma((3, 2, PIECES)),
            dma((2,)), dma((4,)), dma((1,)), dma((1,)),
            dma((3,)), dma((3,)), dma((2, 3)), dma((2, 3)), dma((2, 3)), dma((2, 3)),
            dma((4, 2)), dma((4, 2)), dma((4,)), dma((4,)), dma((4,)), dma((4,)),
        ]
    )
    return pl.pallas_call(
        layer_kernel,
        out_shape=jax.ShapeDtypeStruct((share, width), narrow),
        in_specs=[ANYWHERE] * 8 + [INSIDE] * 10,
        out_specs=INSIDE,
        scratch_shapes=scratch,
        compiler_params=pltpu.CompilerParams(
            collective_id=0, has_side_effects=True, vmem_limit_bytes=60 * 2**20
        ),
    )(
        stream, *mix_w, *up_w, w_down, decays, cosine, sine, *(row(gain) for gain in gains),
        *(row(scale) for scale in (*mix_scales, *up_scales)), row(scale_down),
    )


def summed_over_tp(partial_sum, share):
    partial_sum = partial_sum.reshape(-1, share, partial_sum.shape[1])
    pieces = lax.all_to_all(partial_sum, "tp", split_axis=0, concat_axis=0)
    return jnp.sum(pieces.astype(jnp.float32), axis=0)


def shards(
    stream,
    gain_mix,
    w_query,
    scale_query,
    w_key,
    scale_key,
    w_value,
    scale_value,
    gain_ffn,
    w_gate,
    scale_gate,
    w_up,
    scale_up,
    w_down,
    scale_down,
):
    group_rows = stream.shape[0]
    tp_count = lax.axis_size("tp")
    if (lax.axis_size("rep"), lax.axis_size("fs"), tp_count) == (2, 4, 4):
        return layer(
            stream, (gain_mix, gain_ffn), (w_query, w_key, w_value),
            (scale_query, scale_key, scale_value), (w_gate, w_up), (scale_gate, scale_up),
            w_down, scale_down, tp_count,
        )
    stream_f = stream.astype(jnp.float32)
    normed = (stream_f * rms_scale(stream_f) * gain_mix).astype(jnp.bfloat16)
    mix_w = jnp.concatenate([w.astype(jnp.bfloat16) for w in (w_query, w_key, w_value)], axis=1)
    up_w = jnp.concatenate([w.astype(jnp.bfloat16) for w in (w_gate, w_up)], axis=1)
    down_w = w_down.astype(jnp.bfloat16)
    down_scale = lax.all_gather(scale_down, "fs", axis=0, tiled=True)
    mix_acc = dot(normed, lax.all_gather(mix_w, "fs", axis=0, tiled=True))
    mix_scale = jnp.concatenate([scale_query, scale_key, scale_value])
    query, key, value = jnp.split(
        (mix_acc * mix_scale).astype(jnp.bfloat16),
        [w_query.shape[1], w_query.shape[1] + w_key.shape[1]],
        axis=1,
    )
    local_heads = query.shape[1] // DK
    positions = jnp.arange(group_rows, dtype=jnp.int32) % LEN
    mixed = []
    for head in range(local_heads):
        columns = slice(head * DK, (head + 1) * DK)
        queries = rotate(query[:, columns].astype(jnp.float32), positions)
        keys = rotate(key[:, columns].astype(jnp.float32), positions) * DK ** (-0.5)
        values = value[:, head * DV : (head + 1) * DV].astype(jnp.float32)
        head_id = (lax.axis_index("tp") * local_heads + head).astype(jnp.float32)
        log_decay = jnp.log(1.0 - jnp.power(2.0, -5.0 - head_id))
        retained = retention(queries, keys, values, log_decay)
        mixed.append((retained * head_scale(retained)).astype(jnp.bfloat16))
    mixed = jnp.concatenate(mixed, axis=1)
    share = group_rows // tp_count
    own_rows = lax.dynamic_slice_in_dim(stream, lax.axis_index("tp") * share, share, 0)
    arrived = lax.all_to_all(mixed, "tp", split_axis=0, concat_axis=1, tiled=True)
    resid = own_rows.astype(jnp.float32) + arrived.astype(jnp.float32)
    normed_ffn = (resid * rms_scale(resid) * gain_ffn).astype(jnp.bfloat16)
    piece = lax.all_gather(normed_ffn, "tp", axis=0, tiled=True)
    up_acc = dot(piece, lax.all_gather(up_w, "fs", axis=0, tiled=True))
    units = w_gate.shape[1]
    gate = up_acc[:, :units] * scale_gate
    upward = up_acc[:, units:] * scale_up
    hidden = (jax.nn.silu(gate) * upward).astype(jnp.bfloat16)
    whole = dot_t(hidden, lax.all_gather(down_w, "fs", axis=0, tiled=True))
    channel_out = summed_over_tp((whole * down_scale).astype(jnp.bfloat16), share)
    return (resid + channel_out).astype(jnp.bfloat16)


def solution(mesh):
    placed = (
        P(("rep", "fs"), None),
        P(),
        P("fs", "tp"),
        P("tp"),
        P("fs", "tp"),
        P("tp"),
        P("fs", "tp"),
        P("tp"),
        P(),
        P("fs", "tp"),
        P("tp"),
        P("fs", "tp"),
        P("tp"),
        P("fs", "tp"),
        P("fs"),
    )
    return jax.shard_map(
        shards, mesh=mesh, in_specs=placed, out_specs=P(("rep", "fs", "tp"), None), check_vma=False
    )
```

```python
import numpy as np
import jax
import jax.numpy as jnp
from jax import lax
from jax.experimental import pallas as pl
from jax.experimental.pallas import tpu as pltpu
from jax.sharding import PartitionSpec as P

DK = 256
DV = 256
LEN = 128


EPS = 1e-06
THETA = 10000.0
HIGH = lax.Precision.HIGHEST


def rms_scale(values):
    return lax.rsqrt(jnp.mean(values * values, axis=-1, keepdims=True) + EPS)


def head_scale(values):
    return 1.0 / jnp.maximum(jnp.sqrt(jnp.mean(values * values, axis=-1, keepdims=True)), 1.0)


def rotate(heads_data, positions):
    half = heads_data.shape[-1] // 2
    frequency = THETA ** (-(jnp.arange(half, dtype=jnp.float32) / half))
    angle = positions.astype(jnp.float32)[:, None] * frequency
    cosine = jnp.cos(angle)
    sine = jnp.sin(angle)
    first = heads_data[..., :half]
    second = heads_data[..., half:]
    return jnp.concatenate(
        [first * cosine - second * sine, second * cosine + first * sine], axis=-1
    )


def retention(queries, keys, values, log_decay):
    offsets = jnp.arange(LEN, dtype=jnp.float32)
    distance = offsets[:, None] - offsets[None, :]
    decay = jnp.where(distance >= 0, jnp.exp(log_decay * jnp.maximum(distance, 0.0)), 0.0)
    queries, keys, values = (
        part.reshape(-1, LEN, part.shape[-1]) for part in (queries, keys, values)
    )
    scores = jnp.einsum("sid,sjd->sij", queries, keys, precision=HIGH) * decay
    retained = jnp.einsum("sij,sje->sie", scores, values, precision=HIGH)
    return retained.reshape(-1, values.shape[-1])


def dot(left, right):
    return jnp.dot(left, right, preferred_element_type=jnp.float32)


def dot_t(left, right):
    return lax.dot_general(left, right, (((1,), (1,)), ((), ())), preferred_element_type=jnp.float32)


MESH = pl.DeviceIdType.MESH
PIECES = (8, 8, 4)


def greet(peers):
    barrier = pltpu.get_barrier_semaphore()
    total = 0
    for axis, count in peers:
        me = lax.axis_index(axis)
        for step in range(1, count):
            peer = lax.rem(me + step, count)
            pl.semaphore_signal(barrier, inc=1, device_id={axis: peer}, device_id_type=MESH)
            total += 1
    pl.semaphore_wait(barrier, total)


def remote(source, target, send, recv, device):
    return pltpu.make_async_remote_copy(
        src_ref=source,
        dst_ref=target,
        send_sem=send,
        recv_sem=recv,
        device_id=device,
        device_id_type=MESH,
    )


def span(index, size):
    return pl.ds(pl.multiple_of(index * size, size), size)


def layer_kernel(
    stream, w_query, w_key, w_value, w_gate, w_up, w_down, decays,
    cosine, sine, gain_mix, gain_ffn, scale_query, scale_key, scale_value, scale_gate, scale_up,
    scale_down,
    out,
    f_query, f_key, f_value, f_up, f_down, rows, decay,
    mix_w, up_w, down_w, normed, end_rows, mix_acc, mixed, arrived, resid, normed_ffn,
    hidden, partial, from_core, from_diag, from_line, paired, final, down_scale,
    local, z_send, z_recv, y_send, y_recv, scale_send, scale_recv, end_send, end_recv,
    norm_send, norm_recv, mix_send, mix_recv, row_send, row_recv, core_send, core_recv,
    line_send, line_recv, out_send, out_recv,
):
    z, y, t = lax.axis_index("fs"), lax.axis_index("rep"), lax.axis_index("tp")
    group, width = stream.shape
    share = group // 4
    depth, heads_width = w_query.shape
    units = w_gate.shape[0]
    heights = (depth, 2 * units, units)
    local_heads = heads_width // DK
    middle = (z == 1) | (z == 2)
    end = jnp.where(z == 1, 0, 3)
    other = 3 - z
    other_end = 3 - end
    partner = t + 1 - 2 * lax.rem(t, 2)
    twin = lax.rem(t + 2, 4)
    diagonal = lax.rem(partner + 2, 4)

    loads = [
        pltpu.make_async_copy(source, target, local.at[index])
        for index, (source, target) in enumerate(
            (
                (w_query, f_query), (w_key, f_key), (w_value, f_value), (stream, rows),
                (w_gate, f_up.at[pl.ds(0, units)]), (w_up, f_up.at[pl.ds(units, units)]), (w_down, f_down),
                (decays.at[pl.ds(t * local_heads, local_heads)], decay),
            )
        )
    ]
    for load in loads:
        load.start()

    def place_of(matrix, block, number):
        height = heights[matrix]
        piece = height // PIECES[matrix]
        return pl.ds(pl.multiple_of(block * height + number * piece, piece), piece)

    def cast(matrix, number):
        here, there = place_of(matrix, 0, number), place_of(matrix, z, number)
        if matrix == 0:
            for place, full in enumerate((f_query, f_key, f_value)):
                columns = slice(place * heads_width, (place + 1) * heads_width)
                mix_w[there, columns] = full[here, :].astype(jnp.bfloat16)
        elif matrix == 1:
            up_w[there, :] = f_up[here, :].astype(jnp.bfloat16)
        else:
            down_w[there, :] = f_down[here, :].astype(jnp.bfloat16)

    def half_numbers(matrix, half):
        count = PIECES[matrix] // 2
        return [count * half + step for step in range(count)]

    needs = ((0, 1, 2), (4, 5), (6,))
    weights = (mix_w, up_w, down_w)

    def z_copy(matrix, slot, block, number, target):
        view = weights[matrix].at[place_of(matrix, block, number)]
        return remote(
            view, view, z_send.at[matrix, slot, number], z_recv.at[matrix, slot, number],
            {"fs": target},
        )

    def y_copy(matrix, slot, block, number):
        view = weights[matrix].at[place_of(matrix, block, number)]
        return remote(
            view, view, y_send.at[matrix, slot, number], y_recv.at[matrix, slot, number],
            {"rep": 1 - y},
        )

    def rms_rows(values, gain):
        factor = lax.rsqrt(jnp.mean(values * values, axis=1, keepdims=True) + EPS)
        return (values * factor * gain).astype(jnp.bfloat16)

    def end_copy(target):
        return remote(
            rows.at[span(t, share)], end_rows, end_send.at[0], end_recv.at[0], {"fs": target}
        )

    def scale_copy(index, target):
        return remote(
            scale_down, down_scale.at[z], scale_send.at[index], scale_recv.at[z], {"fs": target}
        )

    greet((("fs", 4), ("rep", 2), ("tp", 4)))

    @pl.when(jnp.logical_not(middle))
    def _():
        near = jnp.where(z == 0, 1, 2)
        loads[3].wait()
        end_copy(near).start()
        for index in range(2):
            scale_copy(index, index + 1).start()
        queue = []
        for matrix in range(3):
            for index in needs[matrix]:
                loads[index].wait()
            for number in half_numbers(matrix, y) + half_numbers(matrix, 1 - y):
                cast(matrix, number)
                copy = z_copy(matrix, 0, z, number, near)
                copy.start()
                queue.append(copy)
                if len(queue) > 3:
                    queue.pop(0).wait_send()
        for copy in queue:
            copy.wait_send()
        loads[7].wait()
        end_copy(near).wait_send()
        for index in range(2):
            scale_copy(index, index + 1).wait_send()
        for block in range(4):
            part = final.at[block, pl.ds(0, share)]
            remote(part, part, out_send.at[block], out_recv.at[block], {"fs": near}).wait_recv()
        for block in range(4):
            out[:, block * depth : (block + 1) * depth] = final[block, :share, :].astype(jnp.float32)

    @pl.when(middle)
    def _():
        def own_send(matrix):
            for number in half_numbers(matrix, y):
                z_copy(matrix, 1, z, number, other).start()

        def cast_half(matrix, half):
            for number in half_numbers(matrix, half):
                cast(matrix, number)

        def pump_near(matrix, step):
            number = half_numbers(matrix, y)[step]
            z_copy(matrix, 0, end, number, other).wait_recv()
            z_copy(matrix, 2, end, number, other).start()
            z_copy(matrix, 1, other, number, other).wait_recv()
            y_copy(matrix, 0, other, number).start()

        def pump_far(matrix, step):
            number = half_numbers(matrix, y)[step]
            z_copy(matrix, 2, other_end, number, other).wait_recv()
            y_copy(matrix, 1, other_end, number).start()

        def wait_end(matrix):
            for number in half_numbers(matrix, 1 - y):
                z_copy(matrix, 0, end, number, other).wait_recv()

        def wait_y(matrix, slot):
            block = (other, other_end)[slot]
            for number in half_numbers(matrix, 1 - y):
                y_copy(matrix, slot, block, number).wait_recv()

        def norm_copy(step, owner):
            part = normed.at[:, pl.ds(pl.multiple_of(group + owner * share, share), share)]
            peer = lax.rem(t + step, 4)
            return remote(part, part, norm_send.at[step - 1], norm_recv.at[step - 1], {"tp": peer})

        def mix_copy(g, step, peer, owner):
            return remote(
                mixed.at[pl.ds(pl.multiple_of(g * group + peer * share, share), share)],
                arrived.at[owner, pl.ds(g * share, share)],
                mix_send.at[g, step - 1],
                mix_recv.at[g, step - 1],
                {"tp": lax.rem(t + step, 4)},
            )

        def row_copy(g, way, owner):
            part = normed_ffn.at[
                pl.ds(pl.multiple_of(owner * 2 * share + g * share, share), share)
            ]
            return remote(
                part, part, row_send.at[g, way], row_recv.at[g, way],
                {"tp": twin if way == 1 else partner},
            )

        def project(block, first):
            left = normed[block]
            step = depth
            for start in range(0, 3 * heads_width, step):
                columns = slice(start, start + step)
                product = dot(left, mix_w[span(block, depth), columns])
                if first:
                    mix_acc[:, columns] = product
                else:
                    mix_acc[:, columns] += product

        def retain(g, s):
            here = slice(g * group + s * LEN, g * group + (s + 1) * LEN)
            cos, sin = cosine[...], sine[...]

            def turned(offset, scale):
                values = mix_acc[here, offset : offset + DK] * scale
                values = values.astype(jnp.bfloat16).astype(jnp.float32)
                first, second = values[:, : DK // 2], values[:, DK // 2 :]
                return jnp.concatenate(
                    [first * cos - second * sin, second * cos + first * sin], axis=1
                ).astype(jnp.bfloat16)

            for head in range(local_heads):
                columns = slice(head * DK, (head + 1) * DK)
                queries = turned(head * DK, scale_query[:, columns])
                keys = turned(heads_width + head * DK, scale_key[:, columns])
                start = 2 * heads_width + head * DV
                values = (mix_acc[here, start : start + DV] * scale_value[:, columns]).astype(
                    jnp.bfloat16
                )
                scores = (dot_t(queries, keys) * decay[head]).astype(jnp.bfloat16)
                retained = dot(scores, values)
                mixed[here, columns] = (retained * head_scale(retained)).astype(jnp.bfloat16)

        def send_mixed(g):
            for step in range(1, 4):
                mix_copy(g, step, lax.rem(t + step, 4), t).start()
            own = mixed[pl.ds(pl.multiple_of(g * group + t * share, share), share), :]
            arrived[t, g * share : (g + 1) * share, :] = own

        def norm_ffn(g):
            for step in range(1, 4):
                mix_copy(g, step, t, lax.rem(t + 4 - step, 4)).wait_recv()
            here = slice(g * share, (g + 1) * share)
            squares = 0.0
            for block in range(4):
                columns = slice(block * depth, (block + 1) * depth)
                base = rows[span(t, share), columns] if g == 0 else end_rows[:, columns]
                values = base.astype(jnp.float32) + arrived[block, here, :].astype(jnp.float32)
                resid[block, here, :] = values
                squares += jnp.sum(values * values, axis=1, keepdims=True)
            factor = lax.rsqrt(squares / width + EPS)
            target = pl.ds(pl.multiple_of(t * 2 * share + g * share, share), share)
            for block in range(4):
                columns = slice(block * depth, (block + 1) * depth)
                normed_ffn[target, columns] = (
                    resid[block, here, :] * factor * gain_ffn[:, columns]
                ).astype(jnp.bfloat16)
            row_copy(g, 0, t).start()
            row_copy(g, 1, t).start()

        def forward_rows(g):
            row_copy(g, 1, twin).wait_recv()
            row_copy(g, 2, twin).start()

        def hidden_rows(side):
            here = span(side, group)

            def projected(start, size, scale):
                total = 0.0
                for block in range(4):
                    left = normed_ffn[here, block * depth : (block + 1) * depth]
                    first = block * 2 * units + start
                    total += dot_t(left, up_w[first : first + size, :])
                return total * scale

            for start in range(0, units, 256):
                size = min(256, units - start)
                columns = slice(start, start + size)
                gate = projected(start, size, scale_gate[columns][None, :])
                upward = projected(units + start, size, scale_up[columns][None, :])
                hidden[here, columns] = (gate / (1.0 + jnp.exp(-gate)) * upward).astype(
                    jnp.bfloat16
                )

        def core_copy(k, way):
            part = span(partner if way == 0 else diagonal, 2 * share)
            return remote(
                partial.at[k, part],
                (from_core if way == 0 else from_diag).at[k],
                core_send.at[k, way],
                core_recv.at[k, way],
                {"tp": partner},
            )

        def line_copy(k):
            return remote(
                paired.at[k], from_line.at[k], line_send.at[k], line_recv.at[k], {"tp": twin}
            )

        def out_copy(block):
            return remote(
                final.at[block, pl.ds(share, share)],
                final.at[block, pl.ds(0, share)],
                out_send.at[block],
                out_recv.at[block],
                {"fs": end},
            )

        def down(k, block):
            products = dot(hidden[...], down_w[span(block, units), :])
            partial[k] = (products * down_scale[block]).astype(jnp.bfloat16)
            core_copy(k, 0).start()
            core_copy(k, 1).start()

        def pair(k):
            core_copy(k, 1).wait_recv()
            mine = partial[k, span(twin, 2 * share), :].astype(jnp.float32)
            paired[k] = (mine + from_diag[k].astype(jnp.float32)).astype(jnp.bfloat16)
            line_copy(k).start()

        def finish(k, block):
            core_copy(k, 0).wait_recv()
            line_copy(k).wait_recv()
            total = partial[k, span(t, 2 * share), :].astype(jnp.float32)
            total += from_core[k].astype(jnp.float32)
            total += from_line[k].astype(jnp.float32)
            final[block] = (resid[block] + total).astype(jnp.bfloat16)
            out_copy(block).start()

        scale_copy(0, other).start()
        for index in needs[0]:
            loads[index].wait()
        cast_half(0, y)
        own_send(0)
        cast_half(0, 1 - y)
        loads[3].wait()
        for start in range(0, group, share):
            values = rms_rows(rows[start : start + share, :].astype(jnp.float32), gain_mix[...])
            for block in range(4):
                normed[block, start : start + share, :] = values[
                    :, block * depth : (block + 1) * depth
                ]
        end_copy(end).wait_recv()
        values = rms_rows(end_rows[...].astype(jnp.float32), gain_mix[...])
        target = pl.ds(pl.multiple_of(group + t * share, share), share)
        for block in range(4):
            normed[block, target, :] = values[:, block * depth : (block + 1) * depth]
        for step in range(1, 4):
            norm_copy(step, t).start()
        pump_near(0, 0)
        for index in needs[1]:
            loads[index].wait()
        cast_half(1, y)
        pump_near(0, 1)
        cast_half(1, 1 - y)
        pump_near(0, 2)
        loads[6].wait()
        loads[7].wait()
        for half in range(2):
            cast_half(2, half)
        pump_near(0, 3)
        own_send(1)
        for step in range(1, 4):
            norm_copy(step, lax.rem(t + 4 - step, 4)).wait_recv()
        project(z, True)
        pump_far(0, 0)
        pump_far(0, 1)
        wait_y(0, 0)
        project(other, False)
        pump_far(0, 2)
        pump_far(0, 3)
        wait_end(0)
        project(end, False)
        wait_y(0, 1)
        project(other_end, False)

        retain(0, 0)
        pump_near(1, 0)
        retain(0, 1)
        send_mixed(0)
        pump_near(1, 1)
        retain(1, 0)
        pump_near(1, 2)
        retain(1, 1)
        send_mixed(1)
        pump_near(1, 3)
        own_send(2)
        norm_ffn(0)
        norm_ffn(1)
        pump_far(1, 0)
        forward_rows(0)
        pump_far(1, 1)
        pump_far(1, 2)
        forward_rows(1)
        pump_far(1, 3)
        wait_end(1)
        wait_y(1, 0)
        for g in range(2):
            row_copy(g, 0, partner).wait_recv()
        wait_y(1, 1)
        x = t // 2
        hidden_rows(x)
        pump_near(2, 0)
        for g in range(2):
            row_copy(g, 2, diagonal).wait_recv()
        hidden_rows(1 - x)
        pump_near(2, 1)
        down_scale[z] = scale_down[...]
        for source in range(4):
            @pl.when(source != z)
            def _():
                remote(
                    down_scale.at[source], down_scale.at[source], scale_send.at[0],
                    scale_recv.at[source], {"fs": other},
                ).wait_recv()
        down(0, z)
        pump_far(2, 0)
        pump_far(2, 1)
        pair(0)
        wait_y(2, 0)
        down(1, other)
        finish(0, z)
        pair(1)
        wait_end(2)
        down(2, end)
        finish(1, other)
        pair(2)
        wait_y(2, 1)
        down(3, other_end)
        finish(2, end)
        pair(3)
        finish(3, other_end)
        for block in range(4):
            out[:, block * depth : (block + 1) * depth] = final[block, :share, :].astype(jnp.float32)

        scale_copy(0, other).wait_send()
        for matrix in range(3):
            for number in half_numbers(matrix, y):
                for slot in (1, 2):
                    z_copy(matrix, slot, z, number, other).wait_send()
                for slot in (0, 1):
                    y_copy(matrix, slot, z, number).wait_send()
        for step in range(1, 4):
            norm_copy(step, t).wait_send()
            for g in range(2):
                mix_copy(g, step, t, t).wait_send()
        for g in range(2):
            for way in range(3):
                row_copy(g, way, t).wait_send()
        for k in range(4):
            core_copy(k, 0).wait_send()
            core_copy(k, 1).wait_send()
            line_copy(k).wait_send()
            out_copy(k).wait_send()


ANYWHERE = pl.BlockSpec(memory_space=pl.ANY)
INSIDE = pl.BlockSpec(memory_space=pltpu.VMEM)


def tables(heads):
    places = np.arange(LEN, dtype=np.float64)
    half = DK // 2
    frequency = (THETA ** (-(np.arange(half) / half))).astype(np.float32)
    angle = (places[:, None].astype(np.float32) * frequency).astype(np.float32)
    distance = places[:, None] - places[None, :]
    gamma = 1.0 - 2.0 ** (-5.0 - np.arange(heads, dtype=np.float64))
    powers = gamma[:, None, None] ** np.maximum(distance, 0.0)
    decay = np.where(distance >= 0, powers, 0.0) * DK ** (-0.5)
    wide = angle.astype(np.float64)
    return (
        decay.astype(np.float32),
        np.cos(wide).astype(np.float32),
        np.sin(wide).astype(np.float32),
    )


def layer(stream, gains, mix_w, mix_scales, up_w, up_scales, w_down, scale_down, tp_count):
    group, width = stream.shape
    share = group // tp_count
    depth, heads_width = mix_w[0].shape
    units = w_down.shape[0]
    blocks = width // depth
    narrow, wide = jnp.bfloat16, jnp.float32
    local_heads = heads_width // DK
    decays, cosine, sine = tables(local_heads * tp_count)
    row = lambda vector: vector[None, :]
    most = max(PIECES)
    dma = pltpu.SemaphoreType.DMA
    scratch = (
        [pltpu.VMEM(w.shape, wide) for w in mix_w]
        + [
            pltpu.VMEM((2 * units, depth), wide),
            pltpu.VMEM((units, depth), wide),
            pltpu.VMEM(stream.shape, narrow),
            pltpu.VMEM((local_heads, LEN, LEN), wide),
            pltpu.VMEM((width, 3 * heads_width), narrow),
            pltpu.VMEM((blocks * 2 * units, depth), narrow),
            pltpu.VMEM((blocks * units, depth), narrow),
            pltpu.VMEM((blocks, 2 * group, depth), narrow),
            pltpu.VMEM((share, width), narrow),
            pltpu.VMEM((2 * group, 3 * heads_width), wide),
            pltpu.VMEM((2 * group, heads_width), narrow),
            pltpu.VMEM((tp_count, 2 * share, heads_width), narrow),
            pltpu.VMEM((blocks, 2 * share, depth), wide),
            pltpu.VMEM((2 * group, width), narrow),
            pltpu.VMEM((2 * group, units), narrow),
            pltpu.VMEM((blocks, 2 * group, depth), narrow),
        ]
        + [pltpu.VMEM((blocks, 2 * share, depth), narrow)] * 5
        + [pltpu.VMEM((blocks, 1, depth), wide)]
        + [
            dma((8,)),
            dma((3, 3, most)), dma((3, 3, most)), dma((3, 2, most)), dma((3, 2, most)),
            dma((2,)), dma((4,)), dma((1,)), dma((1,)),
            dma((3,)), dma((3,)), dma((2, 3)), dma((2, 3)), dma((2, 3)), dma((2, 3)),
            dma((4, 2)), dma((4, 2)), dma((4,)), dma((4,)), dma((4,)), dma((4,)),
        ]
    )
    return pl.pallas_call(
        layer_kernel,
        out_shape=jax.ShapeDtypeStruct((share, width), wide),
        in_specs=[ANYWHERE] * 8 + [INSIDE] * 10,
        out_specs=INSIDE,
        scratch_shapes=scratch,
        compiler_params=pltpu.CompilerParams(
            collective_id=0, has_side_effects=True, vmem_limit_bytes=60 * 2**20
        ),
    )(
        stream, *mix_w, *up_w, w_down, decays, cosine, sine, *(row(gain) for gain in gains),
        *(row(scale) for scale in mix_scales), *up_scales, row(scale_down),
    ).astype(narrow)


def summed_over_tp(partial_sum, share):
    partial_sum = partial_sum.reshape(-1, share, partial_sum.shape[1])
    pieces = lax.all_to_all(partial_sum, "tp", split_axis=0, concat_axis=0)
    return jnp.sum(pieces.astype(jnp.float32), axis=0)


def shards(
    stream,
    gain_mix,
    w_query,
    scale_query,
    w_key,
    scale_key,
    w_value,
    scale_value,
    gain_ffn,
    w_gate,
    scale_gate,
    w_up,
    scale_up,
    w_down,
    scale_down,
):
    group_rows = stream.shape[0]
    tp_count = lax.axis_size("tp")
    if (lax.axis_size("rep"), lax.axis_size("fs"), tp_count) == (2, 4, 4):
        return layer(
            stream, (gain_mix, gain_ffn), (w_query, w_key, w_value),
            (scale_query, scale_key, scale_value), (w_gate.T, w_up.T), (scale_gate, scale_up),
            w_down.T, scale_down, tp_count,
        )
    stream_f = stream.astype(jnp.float32)
    normed = (stream_f * rms_scale(stream_f) * gain_mix).astype(jnp.bfloat16)
    mix_w = jnp.concatenate([w.astype(jnp.bfloat16) for w in (w_query, w_key, w_value)], axis=1)
    up_w = jnp.concatenate([w.astype(jnp.bfloat16) for w in (w_gate, w_up)], axis=1)
    down_w = w_down.astype(jnp.bfloat16)
    down_scale = lax.all_gather(scale_down, "fs", axis=0, tiled=True)
    mix_acc = dot(normed, lax.all_gather(mix_w, "fs", axis=0, tiled=True))
    mix_scale = jnp.concatenate([scale_query, scale_key, scale_value])
    query, key, value = jnp.split(
        (mix_acc * mix_scale).astype(jnp.bfloat16),
        [w_query.shape[1], w_query.shape[1] + w_key.shape[1]],
        axis=1,
    )
    local_heads = query.shape[1] // DK
    positions = jnp.arange(group_rows, dtype=jnp.int32) % LEN
    mixed = []
    for head in range(local_heads):
        columns = slice(head * DK, (head + 1) * DK)
        queries = rotate(query[:, columns].astype(jnp.float32), positions)
        keys = rotate(key[:, columns].astype(jnp.float32), positions) * DK ** (-0.5)
        values = value[:, head * DV : (head + 1) * DV].astype(jnp.float32)
        head_id = (lax.axis_index("tp") * local_heads + head).astype(jnp.float32)
        log_decay = jnp.log(1.0 - jnp.power(2.0, -5.0 - head_id))
        retained = retention(queries, keys, values, log_decay)
        mixed.append((retained * head_scale(retained)).astype(jnp.bfloat16))
    mixed = jnp.concatenate(mixed, axis=1)
    share = group_rows // tp_count
    own_rows = lax.dynamic_slice_in_dim(stream, lax.axis_index("tp") * share, share, 0)
    arrived = lax.all_to_all(mixed, "tp", split_axis=0, concat_axis=1, tiled=True)
    resid = own_rows.astype(jnp.float32) + arrived.astype(jnp.float32)
    normed_ffn = (resid * rms_scale(resid) * gain_ffn).astype(jnp.bfloat16)
    piece = lax.all_gather(normed_ffn, "tp", axis=0, tiled=True)
    up_acc = dot(piece, lax.all_gather(up_w, "fs", axis=0, tiled=True))
    units = w_gate.shape[1]
    gate = up_acc[:, :units] * scale_gate
    upward = up_acc[:, units:] * scale_up
    hidden = (jax.nn.silu(gate) * upward).astype(jnp.bfloat16)
    whole = dot_t(hidden, lax.all_gather(down_w, "fs", axis=0, tiled=True))
    channel_out = summed_over_tp((whole * down_scale).astype(jnp.bfloat16), share)
    return (resid + channel_out).astype(jnp.bfloat16)


def solution(mesh):
    placed = (
        P(("rep", "fs"), None),
        P(),
        P("fs", "tp"),
        P("tp"),
        P("fs", "tp"),
        P("tp"),
        P("fs", "tp"),
        P("tp"),
        P(),
        P("fs", "tp"),
        P("tp"),
        P("fs", "tp"),
        P("tp"),
        P("fs", "tp"),
        P("fs"),
    )
    return jax.shard_map(
        shards, mesh=mesh, in_specs=placed, out_specs=P(("rep", "fs", "tp"), None), check_vma=False
    )
```

```python
import numpy as np
import jax
import jax.numpy as jnp
from jax import lax
from jax.experimental import pallas as pl
from jax.experimental.pallas import tpu as pltpu
from jax.sharding import PartitionSpec as P

DK = 256
DV = 256
LEN = 128


EPS = 1e-06
THETA = 10000.0
HIGH = lax.Precision.HIGHEST


def rms_scale(values):
    return lax.rsqrt(jnp.mean(values * values, axis=-1, keepdims=True) + EPS)


def head_scale(values):
    return 1.0 / jnp.maximum(jnp.sqrt(jnp.mean(values * values, axis=-1, keepdims=True)), 1.0)


def rotate(heads_data, positions):
    half = heads_data.shape[-1] // 2
    frequency = THETA ** (-(jnp.arange(half, dtype=jnp.float32) / half))
    angle = positions.astype(jnp.float32)[:, None] * frequency
    cosine = jnp.cos(angle)
    sine = jnp.sin(angle)
    first = heads_data[..., :half]
    second = heads_data[..., half:]
    return jnp.concatenate(
        [first * cosine - second * sine, second * cosine + first * sine], axis=-1
    )


def retention(queries, keys, values, log_decay):
    offsets = jnp.arange(LEN, dtype=jnp.float32)
    distance = offsets[:, None] - offsets[None, :]
    decay = jnp.where(distance >= 0, jnp.exp(log_decay * jnp.maximum(distance, 0.0)), 0.0)
    queries, keys, values = (
        part.reshape(-1, LEN, part.shape[-1]) for part in (queries, keys, values)
    )
    scores = jnp.einsum("sid,sjd->sij", queries, keys, precision=HIGH) * decay
    retained = jnp.einsum("sij,sje->sie", scores, values, precision=HIGH)
    return retained.reshape(-1, values.shape[-1])


def dot(left, right):
    return jnp.dot(left, right, preferred_element_type=jnp.float32)


def dot_t(left, right):
    return lax.dot_general(left, right, (((1,), (1,)), ((), ())), preferred_element_type=jnp.float32)


MESH = pl.DeviceIdType.MESH
PIECES = (8, 8, 4)


def signal(axis, peer):
    barrier = pltpu.get_barrier_semaphore()
    pl.semaphore_signal(barrier, inc=1, device_id={axis: peer}, device_id_type=MESH)


def remote(source, target, send, recv, device):
    return pltpu.make_async_remote_copy(
        src_ref=source,
        dst_ref=target,
        send_sem=send,
        recv_sem=recv,
        device_id=device,
        device_id_type=MESH,
    )


def span(index, size):
    return pl.ds(pl.multiple_of(index * size, size), size)


def layer_kernel(
    stream, w_query, w_key, w_value, w_gate, w_up, w_down, decays,
    cosine, sine, gain_mix, gain_ffn, scale_query, scale_key, scale_value, scale_gate, scale_up,
    scale_down,
    out,
    f_query, f_key, f_value, f_up, f_down, rows, decay,
    mix_w, up_w, down_w, normed, end_rows, mix_acc, mixed, arrived, resid, normed_ffn,
    hidden, partial, from_core, from_diag, from_line, paired, final, down_scale,
    local, z_send, z_recv, y_send, y_recv, scale_send, scale_recv, end_send, end_recv,
    norm_send, norm_recv, mix_send, mix_recv, row_send, row_recv, core_send, core_recv,
    line_send, line_recv, out_send, out_recv,
):
    z, y, t = lax.axis_index("fs"), lax.axis_index("rep"), lax.axis_index("tp")
    group, width = stream.shape
    share = group // 4
    depth, heads_width = w_query.shape
    units = w_gate.shape[0]
    heights = (depth, 2 * units, 2 * units)
    part_width = depth // 2
    local_heads = heads_width // DK
    middle = (z == 1) | (z == 2)
    end = jnp.where(z == 1, 0, 3)
    other = 3 - z
    other_end = 3 - end
    partner = t + 1 - 2 * lax.rem(t, 2)
    twin = lax.rem(t + 2, 4)
    diagonal = lax.rem(partner + 2, 4)

    near = jnp.where(z == 0, 1, 2)

    @pl.when(jnp.logical_not(middle))
    def _():
        signal("fs", near)

    @pl.when(middle)
    def _():
        signal("fs", end)
        signal("fs", other)
        signal("rep", 1 - y)
        for step in range(1, 4):
            signal("tp", lax.rem(t + step, 4))

    loads = [
        pltpu.make_async_copy(source, target, local.at[index])
        for index, (source, target) in enumerate(
            (
                (w_query, f_query), (w_key, f_key), (w_value, f_value), (stream, rows),
                (w_gate, f_up.at[pl.ds(0, units)]), (w_up, f_up.at[pl.ds(units, units)]),
                (w_down.at[:, pl.ds(0, part_width)], f_down.at[pl.ds(0, units)]),
                (w_down.at[:, pl.ds(part_width, part_width)], f_down.at[pl.ds(units, units)]),
                (decays.at[pl.ds(t * local_heads, local_heads)], decay),
            )
        )
    ]
    for load in loads:
        load.start()

    def place_of(matrix, block, number):
        height = heights[matrix]
        piece = height // PIECES[matrix]
        return pl.ds(pl.multiple_of(block * height + number * piece, piece), piece)

    def cast(matrix, number):
        here, there = place_of(matrix, 0, number), place_of(matrix, z, number)
        if matrix == 0:
            for place, full in enumerate((f_query, f_key, f_value)):
                columns = slice(place * heads_width, (place + 1) * heads_width)
                mix_w[there, columns] = full[here, :].astype(jnp.bfloat16)
        elif matrix == 1:
            up_w[there, :] = f_up[here, :].astype(jnp.bfloat16)
        else:
            down_w[there, :] = f_down[here, :].astype(jnp.bfloat16)

    def half_numbers(matrix, half):
        count = PIECES[matrix] // 2
        return [count * half + step for step in range(count)]

    needs = ((0, 1, 2), (4, 5), (6, 7))
    weights = (mix_w, up_w, down_w)

    def z_copy(matrix, slot, block, number, target):
        view = weights[matrix].at[place_of(matrix, block, number)]
        return remote(
            view, view, z_send.at[matrix, slot, number], z_recv.at[matrix, slot, number],
            {"fs": target},
        )

    def y_copy(matrix, slot, block, number):
        view = weights[matrix].at[place_of(matrix, block, number)]
        return remote(
            view, view, y_send.at[matrix, slot, number], y_recv.at[matrix, slot, number],
            {"rep": 1 - y},
        )

    def rms_rows(values, gain):
        factor = lax.rsqrt(jnp.mean(values * values, axis=1, keepdims=True) + EPS)
        return (values * factor * gain).astype(jnp.bfloat16)

    def end_copy(target):
        return remote(
            rows.at[span(t, share)], end_rows, end_send.at[0], end_recv.at[0], {"fs": target}
        )

    def scale_copy(slot, block, half, target):
        cell = down_scale.at[block * 2 + half]
        source = cell
        if slot == 0:
            source = scale_down.at[:, pl.ds(half * part_width, part_width)]
        return remote(
            source, cell, scale_send.at[slot, half], scale_recv.at[block * 2 + half], {"fs": target}
        )

    @pl.when(jnp.logical_not(middle))
    def _():
        loads[3].wait()
        pl.semaphore_wait(pltpu.get_barrier_semaphore(), 1)
        end_copy(near).start()
        for half in range(2):
            scale_copy(0, z, half, near).start()
        queue = []
        for matrix in range(3):
            for index in needs[matrix]:
                loads[index].wait()
            for number in half_numbers(matrix, y) + half_numbers(matrix, 1 - y):
                cast(matrix, number)
                copy = z_copy(matrix, 0, z, number, near)
                copy.start()
                queue.append(copy)
                if len(queue) > 3:
                    queue.pop(0).wait_send()
        for copy in queue:
            copy.wait_send()
        loads[8].wait()
        end_copy(near).wait_send()
        for half in range(2):
            scale_copy(0, z, half, near).wait_send()
        for cell in range(8):
            part = final.at[cell, pl.ds(0, share)]
            remote(part, part, out_send.at[cell], out_recv.at[cell], {"fs": near}).wait_recv()
            columns = slice(cell * part_width, (cell + 1) * part_width)
            out[:, columns] = final[cell, :share, :].astype(jnp.float32)

    @pl.when(middle)
    def _():
        def own_send(matrix):
            for number in half_numbers(matrix, y):
                z_copy(matrix, 1, z, number, other).start()

        def cast_half(matrix, half):
            for number in half_numbers(matrix, half):
                cast(matrix, number)

        def pump_end(matrix, step):
            number = half_numbers(matrix, y)[step]
            z_copy(matrix, 0, end, number, other).wait_recv()
            z_copy(matrix, 2, end, number, other).start()

        def pump_other(matrix, step):
            number = half_numbers(matrix, y)[step]
            z_copy(matrix, 1, other, number, other).wait_recv()
            y_copy(matrix, 0, other, number).start()

        def pump_far(matrix, step):
            number = half_numbers(matrix, y)[step]
            z_copy(matrix, 2, other_end, number, other).wait_recv()
            y_copy(matrix, 1, other_end, number).start()

        def wait_end(matrix):
            for number in half_numbers(matrix, 1 - y):
                z_copy(matrix, 0, end, number, other).wait_recv()

        def wait_y(matrix, slot):
            block = (other, other_end)[slot]
            for number in half_numbers(matrix, 1 - y):
                y_copy(matrix, slot, block, number).wait_recv()

        def norm_copy(step, owner):
            part = normed.at[:, pl.ds(pl.multiple_of(group + owner * share, share), share)]
            peer = lax.rem(t + step, 4)
            return remote(part, part, norm_send.at[step - 1], norm_recv.at[step - 1], {"tp": peer})

        def mix_copy(g, step, peer, owner):
            return remote(
                mixed.at[pl.ds(pl.multiple_of(g * group + peer * share, share), share)],
                arrived.at[owner, pl.ds(g * share, share)],
                mix_send.at[g, step - 1],
                mix_recv.at[g, step - 1],
                {"tp": lax.rem(t + step, 4)},
            )

        def row_copy(g, way, owner):
            part = normed_ffn.at[
                pl.ds(pl.multiple_of(owner * 2 * share + g * share, share), share)
            ]
            return remote(
                part, part, row_send.at[g, way], row_recv.at[g, way],
                {"tp": twin if way == 1 else partner},
            )

        def project(block, first):
            left = normed[block]
            step = depth
            for start in range(0, 3 * heads_width, step):
                columns = slice(start, start + step)
                product = dot(left, mix_w[span(block, depth), columns])
                if first:
                    mix_acc[:, columns] = product
                else:
                    mix_acc[:, columns] += product

        def retain(g, s):
            here = slice(g * group + s * LEN, g * group + (s + 1) * LEN)
            cos, sin = cosine[...], sine[...]

            def turned(offset, scale):
                values = mix_acc[here, offset : offset + DK] * scale
                values = values.astype(jnp.bfloat16).astype(jnp.float32)
                first, second = values[:, : DK // 2], values[:, DK // 2 :]
                return jnp.concatenate(
                    [first * cos - second * sin, second * cos + first * sin], axis=1
                ).astype(jnp.bfloat16)

            for head in range(local_heads):
                columns = slice(head * DK, (head + 1) * DK)
                queries = turned(head * DK, scale_query[:, columns])
                keys = turned(heads_width + head * DK, scale_key[:, columns])
                start = 2 * heads_width + head * DV
                values = (mix_acc[here, start : start + DV] * scale_value[:, columns]).astype(
                    jnp.bfloat16
                )
                scores = (dot_t(queries, keys) * decay[head]).astype(jnp.bfloat16)
                retained = dot(scores, values)
                mixed[here, columns] = (retained * head_scale(retained)).astype(jnp.bfloat16)

        def send_mixed(g):
            for step in range(1, 4):
                mix_copy(g, step, lax.rem(t + step, 4), t).start()
            own = mixed[pl.ds(pl.multiple_of(g * group + t * share, share), share), :]
            arrived[t, g * share : (g + 1) * share, :] = own

        def norm_ffn(g):
            for step in range(1, 4):
                mix_copy(g, step, t, lax.rem(t + 4 - step, 4)).wait_recv()
            here = slice(g * share, (g + 1) * share)
            squares = 0.0
            for cell in range(8):
                columns = slice(cell * part_width, (cell + 1) * part_width)
                inner = slice(cell % 2 * part_width, (cell % 2 + 1) * part_width)
                base = rows[span(t, share), columns] if g == 0 else end_rows[:, columns]
                values = base.astype(jnp.float32) + arrived[cell // 2, here, inner].astype(
                    jnp.float32
                )
                resid[cell, here, :] = values
                squares += jnp.sum(values * values, axis=1, keepdims=True)
            factor = lax.rsqrt(squares / width + EPS)
            target = pl.ds(pl.multiple_of(t * 2 * share + g * share, share), share)
            for cell in range(8):
                columns = slice(cell * part_width, (cell + 1) * part_width)
                normed_ffn[target, columns] = (
                    resid[cell, here, :] * factor * gain_ffn[:, columns]
                ).astype(jnp.bfloat16)
            row_copy(g, 0, t).start()
            row_copy(g, 1, t).start()

        def forward_rows(g):
            row_copy(g, 1, twin).wait_recv()
            row_copy(g, 2, twin).start()

        def hidden_rows(side):
            here = span(side, group)

            def projected(start, size, scale):
                total = 0.0
                for block in range(4):
                    left = normed_ffn[here, block * depth : (block + 1) * depth]
                    first = block * 2 * units + start
                    total += dot_t(left, up_w[first : first + size, :])
                return total * scale

            for start in range(0, units, 256):
                size = min(256, units - start)
                columns = slice(start, start + size)
                gate = projected(start, size, scale_gate[columns][None, :])
                upward = projected(units + start, size, scale_up[columns][None, :])
                hidden[here, columns] = (gate / (1.0 + jnp.exp(-gate)) * upward).astype(
                    jnp.bfloat16
                )

        def core_copy(k, way):
            part = span(partner if way == 0 else diagonal, 2 * share)
            return remote(
                partial.at[k, part],
                (from_core if way == 0 else from_diag).at[k],
                core_send.at[k, way],
                core_recv.at[k, way],
                {"tp": partner},
            )

        def line_copy(k):
            return remote(
                paired.at[k], from_line.at[k], line_send.at[k], line_recv.at[k], {"tp": twin}
            )

        def out_copy(cell):
            return remote(
                final.at[cell, pl.ds(share, share)],
                final.at[cell, pl.ds(0, share)],
                out_send.at[cell],
                out_recv.at[cell],
                {"fs": end},
            )

        def down(k, cell):
            products = dot(hidden[...], down_w[span(cell, units), :])
            partial[k] = (products * down_scale[cell]).astype(jnp.bfloat16)
            core_copy(k, 1).start()
            core_copy(k, 0).start()

        def pair(k):
            core_copy(k, 1).wait_recv()
            mine = partial[k, span(twin, 2 * share), :].astype(jnp.float32)
            paired[k] = (mine + from_diag[k].astype(jnp.float32)).astype(jnp.bfloat16)
            line_copy(k).start()

        def finish(k, cell):
            core_copy(k, 0).wait_recv()
            line_copy(k).wait_recv()
            total = partial[k, span(t, 2 * share), :].astype(jnp.float32)
            total += from_core[k].astype(jnp.float32)
            total += from_line[k].astype(jnp.float32)
            final[cell] = (resid[cell] + total).astype(jnp.bfloat16)
            out_copy(cell).start()

        for index in needs[0]:
            loads[index].wait()
        cast_half(0, y)
        pl.semaphore_wait(pltpu.get_barrier_semaphore(), 6)
        own_send(0)
        for half in range(2):
            scale_copy(0, z, half, other).start()
            down_scale[z * 2 + half] = scale_down[:, half * part_width : (half + 1) * part_width]
        cast_half(0, 1 - y)
        loads[3].wait()
        for start in range(0, group, share):
            values = rms_rows(rows[start : start + share, :].astype(jnp.float32), gain_mix[...])
            for block in range(4):
                normed[block, start : start + share, :] = values[
                    :, block * depth : (block + 1) * depth
                ]
        pump_other(0, 0)
        end_copy(end).wait_recv()
        values = rms_rows(end_rows[...].astype(jnp.float32), gain_mix[...])
        target = pl.ds(pl.multiple_of(group + t * share, share), share)
        for block in range(4):
            normed[block, target, :] = values[:, block * depth : (block + 1) * depth]
        for step in range(1, 4):
            norm_copy(step, t).start()
        for half in range(2):
            scale_copy(1, end, half, other).wait_recv()
            scale_copy(1, end, half, other).start()
        pump_other(0, 1)
        for index in needs[1]:
            loads[index].wait()
        cast_half(1, y)
        pump_end(0, 0)
        pump_other(0, 2)
        cast_half(1, 1 - y)
        pump_end(0, 1)
        pump_other(0, 3)
        for index in needs[2]:
            loads[index].wait()
        loads[8].wait()
        for half in range(2):
            cast_half(2, half)
        pump_end(0, 2)
        for step in range(1, 4):
            norm_copy(step, lax.rem(t + 4 - step, 4)).wait_recv()
        project(z, True)
        pump_far(0, 0)
        pump_end(0, 3)
        own_send(1)
        pump_far(0, 1)
        wait_y(0, 0)
        project(other, False)
        pump_far(0, 2)
        pump_far(0, 3)
        wait_end(0)
        project(end, False)
        pump_other(1, 0)
        wait_y(0, 1)
        project(other_end, False)

        retain(0, 0)
        pump_other(1, 1)
        retain(0, 1)
        send_mixed(0)
        pump_end(1, 0)
        pump_other(1, 2)
        retain(1, 0)
        pump_end(1, 1)
        retain(1, 1)
        send_mixed(1)
        pump_other(1, 3)
        norm_ffn(0)
        pump_end(1, 2)
        norm_ffn(1)
        pump_end(1, 3)
        own_send(2)
        pump_far(1, 0)
        pump_far(1, 1)
        forward_rows(0)
        pump_far(1, 2)
        forward_rows(1)
        pump_far(1, 3)
        wait_y(1, 0)
        for g in range(2):
            row_copy(g, 0, partner).wait_recv()
        pump_other(2, 0)
        wait_end(1)
        wait_y(1, 1)
        x = t // 2
        hidden_rows(x)
        pump_other(2, 1)
        pump_end(2, 0)
        for g in range(2):
            row_copy(g, 2, diagonal).wait_recv()
        hidden_rows(1 - x)
        for half in range(2):
            scale_copy(0, other, half, other).wait_recv()
            scale_copy(1, other_end, half, other).wait_recv()

        cells = (
            z * 2, z * 2 + 1, other * 2 + y, end * 2 + y, other * 2 + 1 - y, other_end * 2 + y,
            end * 2 + 1 - y, other_end * 2 + 1 - y,
        )
        down(0, cells[0])
        down(1, cells[1])
        pair(0)
        pump_end(2, 1)
        down(2, cells[2])
        pair(1)
        pump_far(2, 0)
        down(3, cells[3])
        pair(2)
        finish(0, cells[0])
        pump_far(2, 1)
        wait_y(2, 0)
        down(4, cells[4])
        pair(3)
        finish(1, cells[1])
        down(5, cells[5])
        pair(4)
        finish(2, cells[2])
        wait_end(2)
        down(6, cells[6])
        pair(5)
        finish(3, cells[3])
        wait_y(2, 1)
        down(7, cells[7])
        pair(6)
        finish(4, cells[4])
        pair(7)
        for k in range(5, 8):
            finish(k, cells[k])
        for cell in range(8):
            columns = slice(cell * part_width, (cell + 1) * part_width)
            out[:, columns] = final[cell, :share, :].astype(jnp.float32)

        for half in range(2):
            scale_copy(0, z, half, other).wait_send()
            scale_copy(1, end, half, other).wait_send()
        for matrix in range(3):
            for number in half_numbers(matrix, y):
                for slot in (1, 2):
                    z_copy(matrix, slot, z, number, other).wait_send()
                for slot in (0, 1):
                    y_copy(matrix, slot, z, number).wait_send()
        for step in range(1, 4):
            norm_copy(step, t).wait_send()
            for g in range(2):
                mix_copy(g, step, t, t).wait_send()
        for g in range(2):
            for way in range(3):
                row_copy(g, way, t).wait_send()
        for k in range(8):
            core_copy(k, 0).wait_send()
            core_copy(k, 1).wait_send()
            line_copy(k).wait_send()
            out_copy(k).wait_send()


ANYWHERE = pl.BlockSpec(memory_space=pl.ANY)
INSIDE = pl.BlockSpec(memory_space=pltpu.VMEM)


def tables(heads):
    places = np.arange(LEN, dtype=np.float64)
    half = DK // 2
    frequency = (THETA ** (-(np.arange(half) / half))).astype(np.float32)
    angle = (places[:, None].astype(np.float32) * frequency).astype(np.float32)
    distance = places[:, None] - places[None, :]
    gamma = 1.0 - 2.0 ** (-5.0 - np.arange(heads, dtype=np.float64))
    powers = gamma[:, None, None] ** np.maximum(distance, 0.0)
    decay = np.where(distance >= 0, powers, 0.0) * DK ** (-0.5)
    wide = angle.astype(np.float64)
    return (
        decay.astype(np.float32),
        np.cos(wide).astype(np.float32),
        np.sin(wide).astype(np.float32),
    )


def layer(stream, gains, mix_w, mix_scales, up_w, up_scales, w_down, scale_down, tp_count):
    group, width = stream.shape
    share = group // tp_count
    depth, heads_width = mix_w[0].shape
    units = w_down.shape[0]
    blocks = width // depth
    narrow, wide = jnp.bfloat16, jnp.float32
    local_heads = heads_width // DK
    decays, cosine, sine = tables(local_heads * tp_count)
    row = lambda vector: vector[None, :]
    most = max(PIECES)
    dma = pltpu.SemaphoreType.DMA
    scratch = (
        [pltpu.VMEM(w.shape, wide) for w in mix_w]
        + [
            pltpu.VMEM((2 * units, depth), wide),
            pltpu.VMEM((2 * units, depth // 2), wide),
            pltpu.VMEM(stream.shape, narrow),
            pltpu.VMEM((local_heads, LEN, LEN), wide),
            pltpu.VMEM((width, 3 * heads_width), narrow),
            pltpu.VMEM((blocks * 2 * units, depth), narrow),
            pltpu.VMEM((blocks * 2 * units, depth // 2), narrow),
            pltpu.VMEM((blocks, 2 * group, depth), narrow),
            pltpu.VMEM((share, width), narrow),
            pltpu.VMEM((2 * group, 3 * heads_width), wide),
            pltpu.VMEM((2 * group, heads_width), narrow),
            pltpu.VMEM((tp_count, 2 * share, heads_width), narrow),
            pltpu.VMEM((2 * blocks, 2 * share, depth // 2), wide),
            pltpu.VMEM((2 * group, width), narrow),
            pltpu.VMEM((2 * group, units), narrow),
            pltpu.VMEM((2 * blocks, 2 * group, depth // 2), narrow),
        ]
        + [pltpu.VMEM((2 * blocks, 2 * share, depth // 2), narrow)] * 5
        + [pltpu.VMEM((2 * blocks, 1, depth // 2), wide)]
        + [
            dma((9,)),
            dma((3, 3, most)), dma((3, 3, most)), dma((3, 2, most)), dma((3, 2, most)),
            dma((2, 2)), dma((8,)), dma((1,)), dma((1,)),
            dma((3,)), dma((3,)), dma((2, 3)), dma((2, 3)), dma((2, 3)), dma((2, 3)),
            dma((8, 2)), dma((8, 2)), dma((8,)), dma((8,)), dma((8,)), dma((8,)),
        ]
    )
    return pl.pallas_call(
        layer_kernel,
        out_shape=jax.ShapeDtypeStruct((share, width), wide),
        in_specs=[ANYWHERE] * 8 + [INSIDE] * 10,
        out_specs=INSIDE,
        scratch_shapes=scratch,
        compiler_params=pltpu.CompilerParams(
            collective_id=0, has_side_effects=True, vmem_limit_bytes=60 * 2**20
        ),
    )(
        stream, *mix_w, *up_w, w_down, decays, cosine, sine, *(row(gain) for gain in gains),
        *(row(scale) for scale in mix_scales), *up_scales, row(scale_down),
    ).astype(narrow)


def summed_over_tp(partial_sum, share):
    partial_sum = partial_sum.reshape(-1, share, partial_sum.shape[1])
    pieces = lax.all_to_all(partial_sum, "tp", split_axis=0, concat_axis=0)
    return jnp.sum(pieces.astype(jnp.float32), axis=0)


def shards(
    stream,
    gain_mix,
    w_query,
    scale_query,
    w_key,
    scale_key,
    w_value,
    scale_value,
    gain_ffn,
    w_gate,
    scale_gate,
    w_up,
    scale_up,
    w_down,
    scale_down,
):
    group_rows = stream.shape[0]
    tp_count = lax.axis_size("tp")
    if (lax.axis_size("rep"), lax.axis_size("fs"), tp_count) == (2, 4, 4):
        return layer(
            stream, (gain_mix, gain_ffn), (w_query, w_key, w_value),
            (scale_query, scale_key, scale_value), (w_gate.T, w_up.T), (scale_gate, scale_up),
            w_down.T, scale_down, tp_count,
        )
    stream_f = stream.astype(jnp.float32)
    normed = (stream_f * rms_scale(stream_f) * gain_mix).astype(jnp.bfloat16)
    mix_w = jnp.concatenate([w.astype(jnp.bfloat16) for w in (w_query, w_key, w_value)], axis=1)
    up_w = jnp.concatenate([w.astype(jnp.bfloat16) for w in (w_gate, w_up)], axis=1)
    down_w = w_down.astype(jnp.bfloat16)
    down_scale = lax.all_gather(scale_down, "fs", axis=0, tiled=True)
    mix_acc = dot(normed, lax.all_gather(mix_w, "fs", axis=0, tiled=True))
    mix_scale = jnp.concatenate([scale_query, scale_key, scale_value])
    query, key, value = jnp.split(
        (mix_acc * mix_scale).astype(jnp.bfloat16),
        [w_query.shape[1], w_query.shape[1] + w_key.shape[1]],
        axis=1,
    )
    local_heads = query.shape[1] // DK
    positions = jnp.arange(group_rows, dtype=jnp.int32) % LEN
    mixed = []
    for head in range(local_heads):
        columns = slice(head * DK, (head + 1) * DK)
        queries = rotate(query[:, columns].astype(jnp.float32), positions)
        keys = rotate(key[:, columns].astype(jnp.float32), positions) * DK ** (-0.5)
        values = value[:, head * DV : (head + 1) * DV].astype(jnp.float32)
        head_id = (lax.axis_index("tp") * local_heads + head).astype(jnp.float32)
        log_decay = jnp.log(1.0 - jnp.power(2.0, -5.0 - head_id))
        retained = retention(queries, keys, values, log_decay)
        mixed.append((retained * head_scale(retained)).astype(jnp.bfloat16))
    mixed = jnp.concatenate(mixed, axis=1)
    share = group_rows // tp_count
    own_rows = lax.dynamic_slice_in_dim(stream, lax.axis_index("tp") * share, share, 0)
    arrived = lax.all_to_all(mixed, "tp", split_axis=0, concat_axis=1, tiled=True)
    resid = own_rows.astype(jnp.float32) + arrived.astype(jnp.float32)
    normed_ffn = (resid * rms_scale(resid) * gain_ffn).astype(jnp.bfloat16)
    piece = lax.all_gather(normed_ffn, "tp", axis=0, tiled=True)
    up_acc = dot(piece, lax.all_gather(up_w, "fs", axis=0, tiled=True))
    units = w_gate.shape[1]
    gate = up_acc[:, :units] * scale_gate
    upward = up_acc[:, units:] * scale_up
    hidden = (jax.nn.silu(gate) * upward).astype(jnp.bfloat16)
    whole = dot_t(hidden, lax.all_gather(down_w, "fs", axis=0, tiled=True))
    channel_out = summed_over_tp((whole * down_scale).astype(jnp.bfloat16), share)
    return (resid + channel_out).astype(jnp.bfloat16)


def solution(mesh):
    placed = (
        P(("rep", "fs"), None),
        P(),
        P("fs", "tp"),
        P("tp"),
        P("fs", "tp"),
        P("tp"),
        P("fs", "tp"),
        P("tp"),
        P(),
        P("fs", "tp"),
        P("tp"),
        P("fs", "tp"),
        P("tp"),
        P("fs", "tp"),
        P("fs"),
    )
    return jax.shard_map(
        shards, mesh=mesh, in_specs=placed, out_specs=P(("rep", "fs", "tp"), None), check_vma=False
    )
```

```python
import numpy as np
import jax
import jax.numpy as jnp
from jax import lax
from jax.experimental import pallas as pl
from jax.experimental.pallas import tpu as pltpu
from jax.sharding import PartitionSpec as P

DK = 256
DV = 256
LEN = 128


EPS = 1e-06
THETA = 10000.0
HIGH = lax.Precision.HIGHEST


def rms_scale(values):
    return lax.rsqrt(jnp.mean(values * values, axis=-1, keepdims=True) + EPS)


def head_scale(values):
    return 1.0 / jnp.maximum(jnp.sqrt(jnp.mean(values * values, axis=-1, keepdims=True)), 1.0)


def rotate(heads_data, positions):
    half = heads_data.shape[-1] // 2
    frequency = THETA ** (-(jnp.arange(half, dtype=jnp.float32) / half))
    angle = positions.astype(jnp.float32)[:, None] * frequency
    cosine = jnp.cos(angle)
    sine = jnp.sin(angle)
    first = heads_data[..., :half]
    second = heads_data[..., half:]
    return jnp.concatenate(
        [first * cosine - second * sine, second * cosine + first * sine], axis=-1
    )


def retention(queries, keys, values, log_decay):
    offsets = jnp.arange(LEN, dtype=jnp.float32)
    distance = offsets[:, None] - offsets[None, :]
    decay = jnp.where(distance >= 0, jnp.exp(log_decay * jnp.maximum(distance, 0.0)), 0.0)
    queries, keys, values = (
        part.reshape(-1, LEN, part.shape[-1]) for part in (queries, keys, values)
    )
    scores = jnp.einsum("sid,sjd->sij", queries, keys, precision=HIGH) * decay
    retained = jnp.einsum("sij,sje->sie", scores, values, precision=HIGH)
    return retained.reshape(-1, values.shape[-1])


def dot(left, right):
    return jnp.dot(left, right, preferred_element_type=jnp.float32)


def dot_t(left, right):
    return lax.dot_general(left, right, (((1,), (1,)), ((), ())), preferred_element_type=jnp.float32)


MESH = pl.DeviceIdType.MESH
PIECES = (8, 4, 4)


def signal(peer):
    barrier = pltpu.get_barrier_semaphore()
    pl.semaphore_signal(barrier, inc=1, device_id=peer, device_id_type=MESH)


def remote(source, target, send, recv, device):
    return pltpu.make_async_remote_copy(
        src_ref=source,
        dst_ref=target,
        send_sem=send,
        recv_sem=recv,
        device_id=device,
        device_id_type=MESH,
    )


def span(index, size):
    return pl.ds(pl.multiple_of(index * size, size), size)


def layer_kernel(
    stream, w_query, w_key, w_value, w_gate, w_up, w_down, decays,
    cosine, sine, gain_mix, gain_ffn, scale_query, scale_key, scale_value, scale_gate, scale_up,
    scale_down,
    out,
    f_query, f_key, f_value, f_up, f_down, rows, decay,
    mix_w, up_w, down_w, normed, mix_acc, mixed, arrived, resid, normed_ffn,
    hidden, partial, from_core, paired, from_line, final, down_scale,
    local, cross_send, inward_send, z_recv, y_send, y_recv, scale_send, scale_recv,
    token_send, token_recv, norm_send, norm_recv, mix_send, mix_recv, row_send, row_recv,
    core_send, core_recv, line_send, line_recv,
):
    z, y, t = lax.axis_index("fs"), lax.axis_index("rep"), lax.axis_index("tp")
    group, width = stream.shape
    share = group // 4
    depth = w_query.shape[0]
    units = w_gate.shape[0] // 2
    part_width = depth // 2
    heights = (depth, 2 * units, 2 * units)
    inner = (z == 1) | (z == 2)
    mine = jnp.where(inner, 1, 0)
    pair_z = z + 1 - 2 * lax.rem(z, 2)
    outer_z, inner_z = jnp.where(inner, pair_z, z), jnp.where(inner, z, pair_z)
    near, far = 3 - inner_z, 3 - outer_z
    core, x = lax.rem(t, 2), t // 2
    partner = t + 1 - 2 * core
    twin = lax.rem(t + 2, 4)
    diagonal = lax.rem(partner + 2, 4)

    for step in range(4):
        for apart in range(2):
            if step or apart:
                signal({"fs": pair_z if apart else z, "tp": lax.rem(t + step, 4)})
    signal({"rep": 1 - y})

    @pl.when(inner)
    def _():
        signal({"fs": near})

    moves = [(w_query, f_query), (w_key, f_key), (w_value, f_value), (stream, rows)]
    for part in range(2):
        for place, matrix in enumerate((w_gate, w_up)):
            moves.append((
                matrix.at[pl.ds(part * units, units)],
                f_up.at[pl.ds((2 * part + place) * units, units)],
            ))
    for part in range(2):
        for half in range(2):
            moves.append((
                w_down.at[pl.ds(part * units, units), pl.ds(half * part_width, part_width)],
                f_down.at[pl.ds((2 * part + half) * units, units)],
            ))
    moves.append((decays.at[pl.ds(2 * t + mine, 1)], decay))
    loads = [
        pltpu.make_async_copy(source, target, local.at[index])
        for index, (source, target) in enumerate(moves)
    ]
    for load in loads:
        load.start()

    weights = (mix_w, up_w, down_w)

    def place_of(matrix, block, number):
        height = heights[matrix]
        piece = height // PIECES[matrix]
        return pl.ds(pl.multiple_of(block * height + number * piece, piece), piece)

    def numbers(matrix, half):
        count = PIECES[matrix] // 2
        return [count * half + step for step in range(count)]

    def cast(matrix, part, half):
        for number in numbers(matrix, half):
            there = place_of(matrix, part * 4 + z, number)
            if matrix == 0:
                here = place_of(0, 0, number)
                for place, full in enumerate((f_query, f_key, f_value)):
                    columns = slice(place * DK, (place + 1) * DK)
                    source = full[here, part * DK : (part + 1) * DK]
                    mix_w[there, columns] = source.astype(jnp.bfloat16)
            else:
                full = f_up if matrix == 1 else f_down
                source = full[place_of(matrix, part, number), :]
                weights[matrix][there, :] = source.astype(jnp.bfloat16)

    def z_copy(matrix, part, block, number, target, inward=False):
        cell = part * 4 + block
        view = weights[matrix].at[place_of(matrix, cell, number)]
        if inward:
            send = inward_send.at[matrix, block, number]
        else:
            send = cross_send.at[matrix, cell, number]
        return remote(view, view, send, z_recv.at[matrix, cell, number], {"fs": target})

    def y_copy(matrix, block, number):
        view = weights[matrix].at[place_of(matrix, mine * 4 + block, number)]
        return remote(
            view, view, y_send.at[matrix, block, number], y_recv.at[matrix, block, number],
            {"rep": 1 - y},
        )

    def send_own(matrix, part, half, target, inward=False):
        for number in numbers(matrix, half):
            z_copy(matrix, part, z, number, target, inward).start()

    def wait_y(matrix, block):
        for number in numbers(matrix, 1 - y):
            y_copy(matrix, block, number).wait_recv()

    def cross(matrix, part, step):
        number = numbers(matrix, y)[step]
        z_copy(matrix, part, outer_z, number, near).wait_recv()
        z_copy(matrix, part, outer_z, number, near).start()

    def inwards(matrix, block, step):
        number = numbers(matrix, y)[step]
        z_copy(matrix, 0, block, number, outer_z, True).wait_recv()
        z_copy(matrix, 0, block, number, outer_z, True).start()

    def swap(matrix, block, step):
        number = numbers(matrix, y)[step]
        z_copy(matrix, mine, block, number, pair_z).wait_recv()
        y_copy(matrix, block, number).start()

    def swap_all(matrix, block):
        for step in range(PIECES[matrix] // 2):
            swap(matrix, block, step)

    def wait_pair(matrix):
        for number in numbers(matrix, 1 - y):
            z_copy(matrix, 1, outer_z, number, near).wait_recv()

    def by_role(inside, outside):
        pl.when(inner)(inside)
        pl.when(jnp.logical_not(inner))(outside)

    def norm_rows(first):
        here = pl.ds(pl.multiple_of(first, share), share)
        there = pl.ds(pl.multiple_of(mine * group + first, share), share)
        values = rows[here, :].astype(jnp.float32)
        factor = lax.rsqrt(jnp.mean(values * values, axis=1, keepdims=True) + EPS)
        values = (values * factor * gain_mix[...]).astype(jnp.bfloat16)
        for block in range(4):
            normed[block, there, :] = values[:, block * depth : (block + 1) * depth]

    def token_copy(side):
        part = normed.at[:, pl.ds(pl.multiple_of(side * group + t * share, share), share)]
        return remote(part, part, token_send.at[0], token_recv.at[0], {"fs": pair_z})

    def norm_copy(step, owner):
        first = (1 - mine) * group + owner * share
        part = normed.at[:, pl.ds(pl.multiple_of(first, share), share)]
        peer = lax.rem(t + step, 4)
        return remote(part, part, norm_send.at[step - 1], norm_recv.at[step - 1], {"tp": peer})

    def scale_copy(slot, block, target):
        cells = down_scale.at[pl.ds(2 * block, 2)]
        return remote(cells, cells, scale_send.at[slot], scale_recv.at[block], {"fs": target})

    def project(block, first):
        product = dot(normed[block], mix_w[span(mine * 4 + block, depth), :])
        if first:
            mix_acc[...] = product
        else:
            mix_acc[...] += product

    lanes = pl.ds(pl.multiple_of(mine * DK, DK), DK)

    def retain(s):
        here = slice(s * LEN, (s + 1) * LEN)
        cos, sin = cosine[...], sine[...]

        def turned(offset, scale):
            values = mix_acc[here, offset : offset + DK] * scale
            values = values.astype(jnp.bfloat16).astype(jnp.float32)
            first, second = values[:, : DK // 2], values[:, DK // 2 :]
            return jnp.concatenate(
                [first * cos - second * sin, second * cos + first * sin], axis=1
            ).astype(jnp.bfloat16)

        queries = turned(0, scale_query[:, lanes])
        keys = turned(DK, scale_key[:, lanes])
        values = (mix_acc[here, 2 * DK :] * scale_value[:, lanes]).astype(jnp.bfloat16)
        scores = (dot_t(queries, keys) * decay[0]).astype(jnp.bfloat16)
        retained = dot(scores, values)
        mixed[here, :] = (retained * head_scale(retained)).astype(jnp.bfloat16)

    def mix_copy(side, step):
        peer = lax.rem(t + step, 4)
        return remote(
            mixed.at[pl.ds(pl.multiple_of(side * group + peer * share, share), share)],
            arrived.at[2 * t + mine],
            mix_send.at[side, step],
            mix_recv.at[mine * 4 + step],
            {"fs": (outer_z, inner_z)[side], "tp": peer},
        )

    def send_mixed(side, start):
        for step in range(4):
            copy = mix_copy(side, step)
            go = copy.start if start else copy.wait_send
            if step:
                go()
            else:
                pl.when(mine != side)(go)

    def wait_mixed():
        for side in range(2):
            for step in range(4):
                cell = 2 * lax.rem(t + 4 - step, 4) + side
                copy = remote(
                    arrived.at[cell], arrived.at[cell], mix_send.at[0, 1],
                    mix_recv.at[side * 4 + step], {"tp": partner},
                )
                if step:
                    copy.wait_recv()
                else:
                    pl.when(mine != side)(copy.wait_recv)

    def norm_ffn():
        squares = 0.0
        for cell in range(8):
            columns = slice(cell * part_width, (cell + 1) * part_width)
            base = rows[span(t, share), columns]
            values = base.astype(jnp.float32) + arrived[cell].astype(jnp.float32)
            resid[cell] = values
            squares += jnp.sum(values * values, axis=1, keepdims=True)
        factor = lax.rsqrt(squares / width + EPS)
        target = span(mine * 4 + t, share)
        for cell in range(8):
            columns = slice(cell * part_width, (cell + 1) * part_width)
            normed_ffn[target, columns] = (
                resid[cell] * factor * gain_ffn[:, columns]
            ).astype(jnp.bfloat16)

    def row_copy(way, side, owner, target):
        part = normed_ffn.at[span(side * 4 + owner, share)]
        return remote(part, part, row_send.at[way], row_recv.at[way], target)

    def row_wait(way):
        side, owner = (
            (mine, partner), (mine, twin), (1 - mine, t), (1 - mine, twin),
            (mine, diagonal), (1 - mine, partner), (1 - mine, diagonal),
        )[way]
        row_copy(way, side, owner, {"tp": partner}).wait_recv()

    def row_turn(first):
        def turn():
            if first == 1:
                row_wait(1)
                row_copy(3, mine, twin, {"fs": pair_z}).start()
                row_copy(4, mine, twin, {"tp": partner}).start()
                row_wait(2)
                row_copy(5, 1 - mine, t, {"tp": partner}).start()
            else:
                row_wait(2)
                row_copy(3, 1 - mine, t, {"tp": twin}).start()
                row_copy(5, 1 - mine, t, {"tp": partner}).start()
                row_wait(1)
                row_copy(4, mine, twin, {"tp": partner}).start()

        return turn

    def chosen(scale):
        full = scale[...][None, :]
        return jnp.where(inner, full[:, units:], full[:, :units])

    def hidden_rows(side):
        here = slice(side * group, (side + 1) * group)

        def projected(place):
            total = 0.0
            for block in range(4):
                left = normed_ffn[here, block * depth : (block + 1) * depth]
                part = span((mine * 4 + block) * 2 + place, units)
                total += dot_t(left, up_w[part, :])
            return total

        gate = projected(0) * chosen(scale_gate)
        upward = projected(1) * chosen(scale_up)
        hidden[here, :] = (gate / (1.0 + jnp.exp(-gate)) * upward).astype(jnp.bfloat16)

    def core_copy(k):
        return remote(
            partial.at[k, 1 - core], from_core.at[k], core_send.at[k], core_recv.at[k],
            {"tp": partner},
        )

    line_targets = (
        ({"fs": pair_z, "tp": twin}, (1 - mine) * 2 + 1 - x),
        ({"tp": twin}, mine * 2 + 1 - x),
        ({"fs": pair_z}, (1 - mine) * 2 + x),
    )

    def line_copy(k, way):
        return remote(
            paired.at[k, way], from_line.at[k, way], line_send.at[k, way], line_recv.at[k, way],
            line_targets[way][0],
        )

    def down(k, cell):
        products = dot(hidden[...], down_w[span(mine * 8 + cell, units), :])
        products = (products * down_scale[cell]).astype(jnp.bfloat16)
        for owner in range(8):
            partial[k, owner % 2, owner // 2] = products[owner * share : (owner + 1) * share]
        core_copy(k).start()

    def both(k, chip):
        return partial[k, core, chip].astype(jnp.float32) + from_core[k, chip].astype(jnp.float32)

    def pair(k):
        core_copy(k).wait_recv()
        for way in range(3):
            paired[k, way] = both(k, line_targets[way][1]).astype(jnp.bfloat16)
            line_copy(k, way).start()

    def finish(k, cell):
        total = both(k, mine * 2 + x)
        for way in (1, 2, 0):
            line_copy(k, way).wait_recv()
            total += from_line[k, way].astype(jnp.float32)
        final[cell] = resid[cell] + total

    for load in loads[:3]:
        load.wait()
    cast(0, 0, y)
    pl.semaphore_wait(pltpu.get_barrier_semaphore(), jnp.where(inner, 9, 8))

    def inside():
        send_own(0, 0, y, near)
        send_own(0, 0, y, outer_z, True)

    def outside():
        send_own(0, 0, y, inner_z)

    by_role(inside, outside)
    loads[3].wait()
    norm_rows(t * share)
    token_copy(mine).start()
    cast(0, 1, y)

    def outside():
        send_own(0, 1, y, inner_z)
        cast(0, 1, 1 - y)
        cast(0, 0, 1 - y)

    def inside():
        for step in range(4):
            inwards(0, near, step)
            cross(0, 0, step)
        cast(0, 1, 1 - y)

    by_role(inside, outside)
    for step in range(1, 4):
        norm_rows(lax.rem(t + step, 4) * share)
    for half in range(2):
        down_scale[z * 2 + half] = scale_down[:, half * part_width : (half + 1) * part_width]
    scale_copy(0, z, pair_z).start()
    token_copy(1 - mine).wait_recv()
    for step in range(1, 4):
        norm_copy(step, t).start()

    def inside():
        scale_copy(1, z, near).start()
        for matrix in (1, 2):
            for load in loads[4 * matrix : 4 * matrix + 4]:
                load.wait()
        cast(1, 0, y)
        for step in range(4):
            inwards(0, far, step)
            if step == 0:
                send_own(0, 1, y, near)
        cast(1, 1, y)
        cast(1, 1, 1 - y)
        cast(2, 0, y)
        cast(2, 1, y)
        cast(2, 1, 1 - y)
        scale_copy(0, outer_z, near).wait_recv()
        scale_copy(2, outer_z, near).start()
        scale_copy(1, near, outer_z).wait_recv()
        scale_copy(3, near, outer_z).start()
        scale_copy(2, far, outer_z).wait_recv()
        scale_copy(4, far, outer_z).start()
        for step in range(4):
            cross(0, 1, step)
        send_own(1, 0, y, near)
        send_own(1, 0, y, outer_z, True)
        swap_all(0, near)

    def outside():
        swap_all(0, inner_z)
        send_own(0, 1, 1 - y, inner_z)
        for matrix in (1, 2):
            for load in loads[4 * matrix : 4 * matrix + 4]:
                load.wait()
            for part in range(2):
                for half in range(2):
                    cast(matrix, part, half)
        swap_all(0, near)
        send_own(1, 0, y, inner_z)

    by_role(inside, outside)
    loads[12].wait()
    for step in range(1, 4):
        norm_copy(step, lax.rem(t + 4 - step, 4)).wait_recv()
    project(z, True)

    def inside():
        wait_pair(0)

    def outside():
        wait_y(0, inner_z)

    by_role(inside, outside)
    project(pair_z, False)
    wait_y(0, near)
    project(near, False)

    def inside():
        for step in range(4):
            swap(0, far, step)
        for step in range(2):
            cross(1, 0, step)
        send_own(1, 1, y, near)

    def outside():
        for step in range(4):
            swap(0, far, step)
        send_own(1, 1, y, inner_z)

    by_role(inside, outside)
    wait_y(0, far)
    project(far, False)

    retain(0)
    retain(1)
    send_mixed(0, True)

    def inside():
        for step in range(2):
            inwards(1, near, step)

    def outside():
        swap_all(1, inner_z)

    by_role(inside, outside)
    retain(2)
    retain(3)
    send_mixed(1, True)
    arrived[2 * t + mine] = mixed[span(mine * 4 + t, share), :]

    def inside():
        for step in range(2):
            cross(1, 1, step)
        send_own(2, 0, y, near)

    pl.when(inner)(inside)
    wait_mixed()
    norm_ffn()
    row_copy(0, mine, t, {"tp": partner}).start()
    row_copy(1, mine, t, {"tp": twin}).start()
    row_copy(2, mine, t, {"fs": pair_z}).start()

    def inside():
        for step in range(2):
            inwards(1, far, step)

    def outside():
        z_copy(1, 1, z, numbers(1, 1 - y)[0], inner_z).start()
        swap_all(1, near)

    by_role(inside, outside)
    pl.when(core == 0)(row_turn(1))
    pl.when(core == 1)(row_turn(2))

    def inside():
        send_own(2, 0, y, outer_z, True)
        swap_all(1, near)

    def outside():
        z_copy(1, 1, z, numbers(1, 1 - y)[1], inner_z).start()
        send_own(2, 0, y, inner_z)
        send_own(2, 1, y, inner_z)
        send_own(2, 1, 1 - y, inner_z)
        swap(1, far, 0)

    by_role(inside, outside)
    row_wait(3)
    row_copy(6, 1 - mine, twin, {"tp": partner}).start()

    def inside():
        for step in range(2):
            cross(2, 0, step)
        send_own(2, 1, y, near)
        swap_all(1, far)
        for step in range(2):
            cross(2, 1, step)
        wait_pair(1)
        for step in range(2):
            inwards(2, near, step)

    def outside():
        swap(1, far, 1)
        swap_all(2, inner_z)
        wait_y(1, inner_z)

    by_role(inside, outside)
    for way in (0, 4, 5, 6):
        row_wait(way)
    wait_y(1, near)
    wait_y(1, far)
    hidden_rows(0)

    def inside():
        for step in range(2):
            inwards(2, far, step)

    pl.when(inner)(inside)
    hidden_rows(1)

    def inside():
        wait_pair(2)

    def outside():
        wait_y(2, inner_z)
        scale_copy(0, inner_z, outer_z).wait_recv()
        scale_copy(3, near, outer_z).wait_recv()
        scale_copy(4, far, outer_z).wait_recv()

    by_role(inside, outside)
    cells = (
        outer_z * 2, outer_z * 2 + 1, inner_z * 2, inner_z * 2 + 1, near * 2 + y, near * 2 + 1 - y,
        far * 2 + y, far * 2 + 1 - y,
    )
    down(0, cells[0])
    down(1, cells[1])
    swap(2, near, 0)
    pair(0)
    down(2, cells[2])
    swap(2, near, 1)
    pair(1)
    down(3, cells[3])
    pair(2)
    finish(0, cells[0])
    down(4, cells[4])
    pair(3)
    finish(1, cells[1])
    swap(2, far, 0)
    wait_y(2, near)
    down(5, cells[5])
    pair(4)
    finish(2, cells[2])
    swap(2, far, 1)
    down(6, cells[6])
    pair(5)
    finish(3, cells[3])
    pair(6)
    wait_y(2, far)
    down(7, cells[7])
    finish(4, cells[4])
    pair(7)
    for k in range(5, 8):
        finish(k, cells[k])
    for cell in range(8):
        out[:, cell * part_width : (cell + 1) * part_width] = final[cell]

    token_copy(mine).wait_send()
    scale_copy(0, z, pair_z).wait_send()

    def inside():
        scale_copy(1, z, near).wait_send()
        scale_copy(2, outer_z, near).wait_send()
        scale_copy(3, near, outer_z).wait_send()
        scale_copy(4, far, outer_z).wait_send()
        for matrix in range(3):
            for number in numbers(matrix, y):
                for part in range(2):
                    z_copy(matrix, part, z, number, near).wait_send()
                    z_copy(matrix, part, outer_z, number, near).wait_send()
                for block in (z, near, far):
                    z_copy(matrix, 0, block, number, outer_z, True).wait_send()
                for block in (near, far):
                    y_copy(matrix, block, number).wait_send()

    def outside():
        for matrix in range(3):
            for part, half in ((0, y), (1, y), (1, 1 - y)):
                for number in numbers(matrix, half):
                    z_copy(matrix, part, z, number, inner_z).wait_send()
            for number in numbers(matrix, y):
                for block in (inner_z, near, far):
                    y_copy(matrix, block, number).wait_send()

    by_role(inside, outside)
    for step in range(1, 4):
        norm_copy(step, t).wait_send()
    for side in range(2):
        send_mixed(side, False)
    for way in range(7):
        row_copy(way, mine, t, {"tp": partner}).wait_send()
    for k in range(8):
        core_copy(k).wait_send()
        for way in range(3):
            line_copy(k, way).wait_send()


ANYWHERE = pl.BlockSpec(memory_space=pl.ANY)
INSIDE = pl.BlockSpec(memory_space=pltpu.VMEM)


def tables(heads):
    places = np.arange(LEN, dtype=np.float64)
    half = DK // 2
    frequency = (THETA ** (-(np.arange(half) / half))).astype(np.float32)
    angle = (places[:, None].astype(np.float32) * frequency).astype(np.float32)
    distance = places[:, None] - places[None, :]
    gamma = 1.0 - 2.0 ** (-5.0 - np.arange(heads, dtype=np.float64))
    powers = gamma[:, None, None] ** np.maximum(distance, 0.0)
    decay = np.where(distance >= 0, powers, 0.0) * DK ** (-0.5)
    wide = angle.astype(np.float64)
    return (
        decay.astype(np.float32),
        np.cos(wide).astype(np.float32),
        np.sin(wide).astype(np.float32),
    )


def layer(stream, gains, mix_w, mix_scales, up_w, up_scales, w_down, scale_down, tp_count):
    group, width = stream.shape
    share = group // tp_count
    depth, heads_width = mix_w[0].shape
    units = w_down.shape[0]
    blocks = width // depth
    narrow, wide = jnp.bfloat16, jnp.float32
    local_heads = heads_width // DK
    decays, cosine, sine = tables(local_heads * tp_count)
    row = lambda vector: vector[None, :]
    most = max(PIECES)
    dma = pltpu.SemaphoreType.DMA
    half_units = units // 2
    cells = 2 * blocks
    part = depth // 2
    scratch = (
        [pltpu.VMEM(w.shape, wide) for w in mix_w]
        + [
            pltpu.VMEM((4 * half_units, depth), wide),
            pltpu.VMEM((4 * half_units, part), wide),
            pltpu.VMEM(stream.shape, narrow),
            pltpu.VMEM((1, LEN, LEN), wide),
            pltpu.VMEM((2 * width, 3 * DK), narrow),
            pltpu.VMEM((cells * units, depth), narrow),
            pltpu.VMEM((cells * units, part), narrow),
            pltpu.VMEM((blocks, 2 * group, depth), narrow),
            pltpu.VMEM((2 * group, 3 * DK), wide),
            pltpu.VMEM((2 * group, DV), narrow),
            pltpu.VMEM((cells, share, DV), narrow),
            pltpu.VMEM((cells, share, part), wide),
            pltpu.VMEM((2 * group, width), narrow),
            pltpu.VMEM((2 * group, half_units), narrow),
            pltpu.VMEM((cells, 2, 4, share, part), narrow),
            pltpu.VMEM((cells, 4, share, part), narrow),
            pltpu.VMEM((cells, 3, share, part), narrow),
            pltpu.VMEM((cells, 3, share, part), narrow),
            pltpu.VMEM((cells, share, part), wide),
            pltpu.VMEM((cells, 1, part), wide),
        ]
        + [
            dma((13,)),
            dma((3, 8, most)), dma((3, 4, most)), dma((3, 8, most)),
            dma((3, 4, most)), dma((3, 4, most)),
            dma((5,)), dma((4,)), dma((1,)), dma((1,)), dma((3,)), dma((3,)),
            dma((2, 4)), dma((8,)), dma((7,)), dma((7,)),
            dma((8,)), dma((8,)), dma((8, 3)), dma((8, 3)),
        ]
    )
    return pl.pallas_call(
        layer_kernel,
        out_shape=jax.ShapeDtypeStruct((share, width), wide),
        in_specs=[ANYWHERE] * 8 + [INSIDE] * 10,
        out_specs=INSIDE,
        scratch_shapes=scratch,
        compiler_params=pltpu.CompilerParams(
            collective_id=0, has_side_effects=True, vmem_limit_bytes=60 * 2**20
        ),
    )(
        stream, *mix_w, *up_w, w_down, decays, cosine, sine, *(row(gain) for gain in gains),
        *(row(scale) for scale in mix_scales), *up_scales, row(scale_down),
    ).astype(narrow)


def summed_over_tp(partial_sum, share):
    partial_sum = partial_sum.reshape(-1, share, partial_sum.shape[1])
    pieces = lax.all_to_all(partial_sum, "tp", split_axis=0, concat_axis=0)
    return jnp.sum(pieces.astype(jnp.float32), axis=0)


def shards(
    stream,
    gain_mix,
    w_query,
    scale_query,
    w_key,
    scale_key,
    w_value,
    scale_value,
    gain_ffn,
    w_gate,
    scale_gate,
    w_up,
    scale_up,
    w_down,
    scale_down,
):
    group_rows = stream.shape[0]
    tp_count = lax.axis_size("tp")
    if (lax.axis_size("rep"), lax.axis_size("fs"), tp_count) == (2, 4, 4):
        return layer(
            stream, (gain_mix, gain_ffn), (w_query, w_key, w_value),
            (scale_query, scale_key, scale_value), (w_gate.T, w_up.T), (scale_gate, scale_up),
            w_down.T, scale_down, tp_count,
        )
    stream_f = stream.astype(jnp.float32)
    normed = (stream_f * rms_scale(stream_f) * gain_mix).astype(jnp.bfloat16)
    mix_w = jnp.concatenate([w.astype(jnp.bfloat16) for w in (w_query, w_key, w_value)], axis=1)
    up_w = jnp.concatenate([w.astype(jnp.bfloat16) for w in (w_gate, w_up)], axis=1)
    down_w = w_down.astype(jnp.bfloat16)
    down_scale = lax.all_gather(scale_down, "fs", axis=0, tiled=True)
    mix_acc = dot(normed, lax.all_gather(mix_w, "fs", axis=0, tiled=True))
    mix_scale = jnp.concatenate([scale_query, scale_key, scale_value])
    query, key, value = jnp.split(
        (mix_acc * mix_scale).astype(jnp.bfloat16),
        [w_query.shape[1], w_query.shape[1] + w_key.shape[1]],
        axis=1,
    )
    local_heads = query.shape[1] // DK
    positions = jnp.arange(group_rows, dtype=jnp.int32) % LEN
    mixed = []
    for head in range(local_heads):
        columns = slice(head * DK, (head + 1) * DK)
        queries = rotate(query[:, columns].astype(jnp.float32), positions)
        keys = rotate(key[:, columns].astype(jnp.float32), positions) * DK ** (-0.5)
        values = value[:, head * DV : (head + 1) * DV].astype(jnp.float32)
        head_id = (lax.axis_index("tp") * local_heads + head).astype(jnp.float32)
        log_decay = jnp.log(1.0 - jnp.power(2.0, -5.0 - head_id))
        retained = retention(queries, keys, values, log_decay)
        mixed.append((retained * head_scale(retained)).astype(jnp.bfloat16))
    mixed = jnp.concatenate(mixed, axis=1)
    share = group_rows // tp_count
    own_rows = lax.dynamic_slice_in_dim(stream, lax.axis_index("tp") * share, share, 0)
    arrived = lax.all_to_all(mixed, "tp", split_axis=0, concat_axis=1, tiled=True)
    resid = own_rows.astype(jnp.float32) + arrived.astype(jnp.float32)
    normed_ffn = (resid * rms_scale(resid) * gain_ffn).astype(jnp.bfloat16)
    piece = lax.all_gather(normed_ffn, "tp", axis=0, tiled=True)
    up_acc = dot(piece, lax.all_gather(up_w, "fs", axis=0, tiled=True))
    units = w_gate.shape[1]
    gate = up_acc[:, :units] * scale_gate
    upward = up_acc[:, units:] * scale_up
    hidden = (jax.nn.silu(gate) * upward).astype(jnp.bfloat16)
    whole = dot_t(hidden, lax.all_gather(down_w, "fs", axis=0, tiled=True))
    channel_out = summed_over_tp((whole * down_scale).astype(jnp.bfloat16), share)
    return (resid + channel_out).astype(jnp.bfloat16)


def solution(mesh):
    placed = (
        P(("rep", "fs"), None),
        P(),
        P("fs", "tp"),
        P("tp"),
        P("fs", "tp"),
        P("tp"),
        P("fs", "tp"),
        P("tp"),
        P(),
        P("fs", "tp"),
        P("tp"),
        P("fs", "tp"),
        P("tp"),
        P("fs", "tp"),
        P("fs"),
    )
    return jax.shard_map(
        shards, mesh=mesh, in_specs=placed, out_specs=P(("rep", "fs", "tp"), None), check_vma=False
    )
```

```python
import numpy as np
import jax
import jax.numpy as jnp
from jax import lax
from jax.experimental import pallas as pl
from jax.experimental.pallas import tpu as pltpu
from jax.sharding import PartitionSpec as P

DK = 256
DV = 256
LEN = 128


EPS = 1e-06
THETA = 10000.0
HIGH = lax.Precision.HIGHEST


def rms_scale(values):
    return lax.rsqrt(jnp.mean(values * values, axis=-1, keepdims=True) + EPS)


def head_scale(values):
    return 1.0 / jnp.maximum(jnp.sqrt(jnp.mean(values * values, axis=-1, keepdims=True)), 1.0)


def rotate(heads_data, positions):
    half = heads_data.shape[-1] // 2
    frequency = THETA ** (-(jnp.arange(half, dtype=jnp.float32) / half))
    angle = positions.astype(jnp.float32)[:, None] * frequency
    cosine = jnp.cos(angle)
    sine = jnp.sin(angle)
    first = heads_data[..., :half]
    second = heads_data[..., half:]
    return jnp.concatenate(
        [first * cosine - second * sine, second * cosine + first * sine], axis=-1
    )


def retention(queries, keys, values, log_decay):
    offsets = jnp.arange(LEN, dtype=jnp.float32)
    distance = offsets[:, None] - offsets[None, :]
    decay = jnp.where(distance >= 0, jnp.exp(log_decay * jnp.maximum(distance, 0.0)), 0.0)
    queries, keys, values = (
        part.reshape(-1, LEN, part.shape[-1]) for part in (queries, keys, values)
    )
    scores = jnp.einsum("sid,sjd->sij", queries, keys, precision=HIGH) * decay
    retained = jnp.einsum("sij,sje->sie", scores, values, precision=HIGH)
    return retained.reshape(-1, values.shape[-1])


def dot(left, right):
    return jnp.dot(left, right, preferred_element_type=jnp.float32)


def dot_t(left, right):
    return lax.dot_general(left, right, (((1,), (1,)), ((), ())), preferred_element_type=jnp.float32)


MESH = pl.DeviceIdType.MESH
PIECES = (8, 4, 4)


def signal(peer):
    barrier = pltpu.get_barrier_semaphore()
    pl.semaphore_signal(barrier, inc=1, device_id=peer, device_id_type=MESH)


def remote(source, target, send, recv, device):
    return pltpu.make_async_remote_copy(
        src_ref=source,
        dst_ref=target,
        send_sem=send,
        recv_sem=recv,
        device_id=device,
        device_id_type=MESH,
    )


def span(index, size):
    return pl.ds(pl.multiple_of(index * size, size), size)


def layer_kernel(
    stream, w_query, w_key, w_value, w_gate, w_up, w_down, decays,
    cosine_in, sine_in, gain_mix_in, gain_ffn_in, scale_query_in, scale_key_in, scale_value_in,
    scale_gate, scale_up, scale_down_in,
    out,
    f_query, f_key, f_value, f_up, f_down, rows, decay,
    cosine, sine, gain_mix, gain_ffn, scale_query, scale_key, scale_value, scale_down,
    mix_w, up_w, down_w, normed, mix_acc, mixed, resid, row_sum, normed_ffn,
    hidden, partial, from_core, paired, from_line, final, down_scale,
    local, cross_send, inward_send, z_recv, y_send, y_recv, scale_send, scale_recv,
    token_send, token_recv, norm_send, norm_recv, row_send, row_recv,
    core_send, core_recv, line_send, line_recv,
):
    z, y, t = lax.axis_index("fs"), lax.axis_index("rep"), lax.axis_index("tp")
    group, width = stream.shape
    share = group // 4
    depth = w_query.shape[0]
    units = w_gate.shape[0] // 2
    part_width = depth // 2
    heights = (depth, 2 * units, 2 * units)
    inner = (z == 1) | (z == 2)
    mine = jnp.where(inner, 1, 0)
    pair_z = z + 1 - 2 * lax.rem(z, 2)
    outer_z, inner_z = jnp.where(inner, pair_z, z), jnp.where(inner, z, pair_z)
    near, far = 3 - inner_z, 3 - outer_z
    core, x = lax.rem(t, 2), t // 2
    partner = t + 1 - 2 * core
    twin = lax.rem(t + 2, 4)
    diagonal = lax.rem(partner + 2, 4)

    for step in range(4):
        for apart in range(2):
            if step or apart:
                signal({"fs": pair_z if apart else z, "tp": lax.rem(t + step, 4)})
    signal({"rep": 1 - y})

    @pl.when(inner)
    def _():
        signal({"fs": near})

    moves = [(w_query, f_query), (w_key, f_key), (w_value, f_value)]
    moves.append((stream, rows.at[span(mine, group)]))
    for part in range(2):
        for place, matrix in enumerate((w_gate, w_up)):
            moves.append((
                matrix.at[pl.ds(part * units, units)],
                f_up.at[pl.ds((2 * part + place) * units, units)],
            ))
    for part in range(2):
        for half in range(2):
            moves.append((
                w_down.at[pl.ds(part * units, units), pl.ds(half * part_width, part_width)],
                f_down.at[pl.ds((2 * part + half) * units, units)],
            ))
    moves.append((decays.at[pl.ds(2 * t + mine, 1)], decay))
    moves += [
        (cosine_in, cosine), (sine_in, sine), (gain_mix_in, gain_mix), (gain_ffn_in, gain_ffn),
        (scale_query_in, scale_query), (scale_key_in, scale_key), (scale_value_in, scale_value),
        (scale_down_in, scale_down),
    ]
    loads = [
        pltpu.make_async_copy(source, target, local.at[index])
        for index, (source, target) in enumerate(moves)
    ]
    for load in loads:
        load.start()

    weights = (mix_w, up_w, down_w)

    def place_of(matrix, block, number):
        height = heights[matrix]
        piece = height // PIECES[matrix]
        return pl.ds(pl.multiple_of(block * height + number * piece, piece), piece)

    def numbers(matrix, half):
        count = PIECES[matrix] // 2
        return [count * half + step for step in range(count)]

    def cast(matrix, part, half):
        for number in numbers(matrix, half):
            there = place_of(matrix, part * 4 + z, number)
            if matrix == 0:
                here = place_of(0, 0, number)
                for place, full in enumerate((f_query, f_key, f_value)):
                    columns = slice(place * DK, (place + 1) * DK)
                    source = full[here, part * DK : (part + 1) * DK]
                    mix_w[there, columns] = source.astype(jnp.bfloat16)
            else:
                full = f_up if matrix == 1 else f_down
                source = full[place_of(matrix, part, number), :]
                weights[matrix][there, :] = source.astype(jnp.bfloat16)

    def z_copy(matrix, part, block, number, target, inward=False):
        cell = part * 4 + block
        view = weights[matrix].at[place_of(matrix, cell, number)]
        if inward:
            send = inward_send.at[matrix, block, number]
        else:
            send = cross_send.at[matrix, cell, number]
        return remote(view, view, send, z_recv.at[matrix, cell, number], {"fs": target})

    def y_copy(matrix, block, number):
        view = weights[matrix].at[place_of(matrix, mine * 4 + block, number)]
        return remote(
            view, view, y_send.at[matrix, block, number], y_recv.at[matrix, block, number],
            {"rep": 1 - y},
        )

    def send_own(matrix, part, half, target, inward=False):
        for number in numbers(matrix, half):
            z_copy(matrix, part, z, number, target, inward).start()

    def own_piece(matrix, part, half, step, target, inward=False):
        z_copy(matrix, part, z, numbers(matrix, half)[step], target, inward).start()

    def scale_pass(slot, block, target):
        scale_copy(1 if block is near else 0 if slot == 2 else 2, block, target).wait_recv()
        scale_copy(slot, block, target).start()

    def tokens_on():
        token_copy(1 - mine).wait_recv()
        for step in range(1, 4):
            norm_copy(step, t).start()

    def pair_rows():
        for step in range(1, 4):
            norm_copy(step, lax.rem(t + 4 - step, 4)).wait_recv()
        for number in range(4):
            norm_rows(1 - mine, number)

    def scales_in():
        for block in (inner_z, near, far):
            scale_copy(0, block, outer_z).wait_recv()

    def wait_y(matrix, block):
        for number in numbers(matrix, 1 - y):
            y_copy(matrix, block, number).wait_recv()

    def cross(matrix, part, step):
        number = numbers(matrix, y)[step]
        z_copy(matrix, part, outer_z, number, near).wait_recv()
        z_copy(matrix, part, outer_z, number, near).start()

    def inwards(matrix, block, step):
        number = numbers(matrix, y)[step]
        z_copy(matrix, 0, block, number, outer_z, True).wait_recv()
        z_copy(matrix, 0, block, number, outer_z, True).start()

    def swap(matrix, block, step):
        number = numbers(matrix, y)[step]
        z_copy(matrix, mine, block, number, pair_z).wait_recv()
        y_copy(matrix, block, number).start()

    def swap_all(matrix, block):
        for step in range(PIECES[matrix] // 2):
            swap(matrix, block, step)

    def wait_pair(matrix):
        for number in numbers(matrix, 1 - y):
            z_copy(matrix, 1, outer_z, number, near).wait_recv()

    def by_role(inside, outside):
        pl.when(inner)(inside)
        pl.when(jnp.logical_not(inner))(outside)

    def norm_rows(side, number):
        here = span(side * 4 + number, share)
        values = rows[here, :].astype(jnp.float32)
        factor = lax.rsqrt(jnp.mean(values * values, axis=1, keepdims=True) + EPS)
        values = (values * factor * gain_mix[...]).astype(jnp.bfloat16)
        for block in range(4):
            normed[block, here, :] = values[:, block * depth : (block + 1) * depth]

    def token_copy(side):
        part = rows.at[span(side * 4 + t, share)]
        return remote(part, part, token_send.at[0], token_recv.at[0], {"fs": pair_z})

    def norm_copy(step, owner):
        part = rows.at[span((1 - mine) * 4 + owner, share)]
        peer = lax.rem(t + step, 4)
        return remote(part, part, norm_send.at[step - 1], norm_recv.at[step - 1], {"tp": peer})

    def scale_copy(slot, block, target):
        cells = down_scale.at[pl.ds(2 * block, 2)]
        return remote(cells, cells, scale_send.at[slot], scale_recv.at[block], {"fs": target})

    def project(block, first):
        product = dot(normed[block], mix_w[span(mine * 4 + block, depth), :])
        if first:
            mix_acc[...] = product
        else:
            mix_acc[...] += product

    lanes = pl.ds(pl.multiple_of(mine * DK, DK), DK)

    def retain(s):
        here = slice(s * LEN, (s + 1) * LEN)
        cos, sin = cosine[...], sine[...]

        def turned(offset, scale):
            values = mix_acc[here, offset : offset + DK] * scale
            values = values.astype(jnp.bfloat16).astype(jnp.float32)
            first, second = values[:, : DK // 2], values[:, DK // 2 :]
            return jnp.concatenate(
                [first * cos - second * sin, second * cos + first * sin], axis=1
            ).astype(jnp.bfloat16)

        queries = turned(0, scale_query[:, lanes])
        keys = turned(DK, scale_key[:, lanes])
        values = (mix_acc[here, 2 * DK :] * scale_value[:, lanes]).astype(jnp.bfloat16)
        scores = (dot_t(queries, keys) * decay[0]).astype(jnp.bfloat16)
        retained = dot(scores, values)
        mixed[2 * t + mine, here, :] = (retained * head_scale(retained)).astype(jnp.bfloat16)
        own = 2 * t + mine
        row_copy(1, s, own, {"tp": twin}).start()
        row_copy(2, s, own, {"fs": pair_z}).start()
        row_copy(0, s, own, {"tp": partner}).start()

    def row_copy(way, s, cell, target):
        part = mixed.at[cell, pl.ds(s * LEN, LEN)]
        return remote(part, part, row_send.at[way, s], row_recv.at[way, s], target)

    def row_wait(way, s):
        cell = (
            2 * partner + mine, 2 * twin + mine, 2 * t + 1 - mine, 2 * twin + 1 - mine,
            2 * diagonal + mine, 2 * partner + 1 - mine, 2 * diagonal + 1 - mine,
        )[way]
        row_copy(way, s, cell, {"tp": partner}).wait_recv()

    def row_line(s):
        cell = 2 * twin + mine
        row_wait(1, s)
        pl.when(core == 0)(row_copy(3, s, cell, {"fs": pair_z}).start)
        row_copy(4, s, cell, {"tp": partner}).start()

    def row_depth(s):
        cell = 2 * t + 1 - mine
        row_wait(2, s)
        pl.when(core == 1)(row_copy(3, s, cell, {"tp": twin}).start)
        row_copy(5, s, cell, {"tp": partner}).start()

    def row_last(s):
        row_wait(3, s)
        row_copy(6, s, 2 * twin + 1 - mine, {"tp": partner}).start()

    def norm_ffn(s):
        for way in (0, 4, 5, 6):
            row_wait(way, s)
        for first in range(s * LEN, (s + 1) * LEN, share):
            here = slice(first, first + share)
            squares = 0.0
            for cell in range(8):
                columns = slice(cell * part_width, (cell + 1) * part_width)
                values = rows[here, columns].astype(jnp.float32)
                values += mixed[cell, here, :].astype(jnp.float32)
                row_sum[:, columns] = values
                squares += jnp.sum(values * values, axis=1, keepdims=True)
            factor = lax.rsqrt(squares / width + EPS)
            for cell in range(8):
                columns = slice(cell * part_width, (cell + 1) * part_width)
                normed_ffn[here, columns] = (
                    row_sum[:, columns] * factor * gain_ffn[:, columns]
                ).astype(jnp.bfloat16)

    def own_resid():
        here = span(mine * 4 + t, share)
        for cell in range(8):
            columns = slice(cell * part_width, (cell + 1) * part_width)
            values = rows[here, columns].astype(jnp.float32)
            resid[cell] = values + mixed[cell, here, :].astype(jnp.float32)

    def chosen(scale):
        full = scale[...][None, :]
        return jnp.where(inner, full[:, units:], full[:, :units])

    def hidden_rows(side):
        here = slice(side * group, (side + 1) * group)

        def projected(place):
            total = 0.0
            for block in range(4):
                left = normed_ffn[here, block * depth : (block + 1) * depth]
                part = span((mine * 4 + block) * 2 + place, units)
                total += dot_t(left, up_w[part, :])
            return total

        gate = projected(0) * chosen(scale_gate)
        upward = projected(1) * chosen(scale_up)
        hidden[here, :] = (gate / (1.0 + jnp.exp(-gate)) * upward).astype(jnp.bfloat16)

    def core_copy(k):
        return remote(
            partial.at[k, 1 - core], from_core.at[k], core_send.at[k], core_recv.at[k],
            {"tp": partner},
        )

    line_targets = (
        ({"fs": pair_z, "tp": twin}, (1 - mine) * 2 + 1 - x),
        ({"tp": twin}, mine * 2 + 1 - x),
        ({"fs": pair_z}, (1 - mine) * 2 + x),
    )

    def line_copy(k, way):
        return remote(
            paired.at[k, way], from_line.at[k, way], line_send.at[k, way], line_recv.at[k, way],
            line_targets[way][0],
        )

    def down(k, cell):
        products = dot(hidden[...], down_w[span(mine * 8 + cell, units), :])
        products = (products * down_scale[cell]).astype(jnp.bfloat16)
        for owner in range(8):
            partial[k, owner % 2, owner // 2] = products[owner * share : (owner + 1) * share]
        core_copy(k).start()

    def both(k, chip):
        return partial[k, core, chip].astype(jnp.float32) + from_core[k, chip].astype(jnp.float32)

    def pair(k):
        core_copy(k).wait_recv()
        for way in range(3):
            paired[k, way] = both(k, line_targets[way][1]).astype(jnp.bfloat16)
            line_copy(k, way).start()

    def finish(k, cell):
        total = both(k, mine * 2 + x)
        for way in (1, 2, 0):
            line_copy(k, way).wait_recv()
            total += from_line[k, way].astype(jnp.float32)
        final[cell] = resid[cell] + total

    for load in loads[:3]:
        load.wait()
    cast(0, 0, y)
    pl.semaphore_wait(pltpu.get_barrier_semaphore(), jnp.where(inner, 9, 8))

    def inside():
        send_own(0, 0, y, near)
        send_own(0, 0, y, outer_z, True)

    def outside():
        send_own(0, 0, y, inner_z)

    by_role(inside, outside)
    loads[3].wait()
    token_copy(mine).start()
    cast(0, 1, y)

    def outside():
        send_own(0, 1, y, inner_z)
        cast(0, 0, 1 - y)

    pl.when(jnp.logical_not(inner))(outside)
    cast(0, 1, 1 - y)
    for load in loads[4:]:
        load.wait()
    for half in range(2):
        down_scale[z * 2 + half] = scale_down[:, half * part_width : (half + 1) * part_width]
    scale_copy(0, z, pair_z).start()

    def inside():
        scale_copy(1, z, near).start()

    pl.when(inner)(inside)
    for matrix in (1, 2):
        for part in range(2):
            for half in range(2):
                cast(matrix, part, half)
    for number in range(4):
        norm_rows(mine, number)
    cells = (
        outer_z * 2 + y, inner_z * 2 + y, inner_z * 2 + 1 - y, outer_z * 2 + 1 - y,
        near * 2 + y, near * 2 + 1 - y,
        far * 2 + y, far * 2 + 1 - y,
    )

    def inside():
        own_piece(0, 1, y, 0, near)
        own_piece(0, 1, y, 1, near)
        own_piece(1, 0, y, 0, outer_z, True)
        own_piece(0, 1, y, 2, near)
        inwards(0, near, 0)
        cross(0, 0, 0)
        inwards(0, near, 1)
        cross(0, 0, 1)
        inwards(0, near, 2)
        cross(0, 0, 2)
        inwards(0, near, 3)
        scale_pass(3, near, outer_z)
        cross(0, 0, 3)
        swap(0, near, 0)
        own_piece(0, 1, y, 3, near)
        own_piece(1, 0, y, 1, outer_z, True)
        swap(0, near, 1)
        own_piece(1, 0, y, 0, near)
        tokens_on()
        swap(0, near, 2)
        cross(0, 1, 0)
        inwards(0, far, 0)
        cross(0, 1, 1)
        inwards(0, far, 1)
        cross(0, 1, 2)
        inwards(0, far, 2)

    def outside():
        swap(0, inner_z, 0)
        swap(0, inner_z, 1)
        swap(0, inner_z, 2)
        own_piece(1, 0, y, 0, inner_z)
        swap(0, inner_z, 3)
        own_piece(1, 0, y, 1, inner_z)
        wait_y(0, inner_z)
        tokens_on()
        own_piece(1, 1, y, 0, inner_z)
        swap(1, inner_z, 0)
        own_piece(1, 1, y, 1, inner_z)
        swap(0, near, 0)
        swap(0, near, 1)

    by_role(inside, outside)
    pair_rows()

    def inside():
        scale_pass(2, outer_z, near)
        inwards(0, far, 3)
        cross(0, 1, 3)

    pl.when(inner)(inside)
    project(z, True)

    def inside():
        own_piece(1, 0, y, 1, near)
        swap(0, near, 3)
        cross(1, 0, 0)
        inwards(1, near, 0)
        wait_y(0, near)
        swap(0, far, 0)
        cross(1, 0, 1)
        swap(0, far, 1)
        swap(0, far, 2)
        scale_pass(4, far, outer_z)
        own_piece(1, 1, y, 0, near)
        own_piece(2, 0, y, 0, outer_z, True)
        swap(0, far, 3)
        own_piece(2, 0, y, 1, outer_z, True)
        own_piece(1, 1, y, 1, near)
        inwards(1, near, 1)
        wait_y(0, far)
        cross(1, 1, 0)
        inwards(1, far, 0)
        wait_pair(0)

    def outside():
        swap(0, near, 2)

    by_role(inside, outside)
    project(pair_z, False)

    def outside():
        swap(0, near, 3)
        swap(1, inner_z, 1)
        swap(0, far, 0)
        wait_y(0, near)

    pl.when(jnp.logical_not(inner))(outside)
    project(near, False)

    def outside():
        own_piece(0, 1, 1 - y, 0, inner_z)
        swap(0, far, 1)
        own_piece(0, 1, 1 - y, 1, inner_z)
        swap(0, far, 2)
        wait_y(1, inner_z)
        own_piece(0, 1, 1 - y, 2, inner_z)
        swap(0, far, 3)
        own_piece(0, 1, 1 - y, 3, inner_z)
        own_piece(1, 1, 1 - y, 0, inner_z)
        swap(1, near, 0)
        scales_in()
        swap(2, inner_z, 0)
        wait_y(0, far)

    pl.when(jnp.logical_not(inner))(outside)
    project(far, False)

    def inside():
        cross(1, 1, 1)

    def outside():
        own_piece(1, 1, 1 - y, 1, inner_z)

    by_role(inside, outside)
    retain(0)

    def inside():
        inwards(1, far, 1)

    def outside():
        swap(2, inner_z, 1)

    by_role(inside, outside)
    retain(1)
    retain(2)
    retain(3)

    def inside():
        own_piece(2, 0, y, 0, near)
        swap(1, near, 0)
        row_line(0)
        own_piece(2, 0, y, 1, near)
        wait_pair(1)
        row_line(1)
        row_depth(0)
        own_piece(2, 1, y, 0, near)
        row_line(2)
        row_depth(1)
        swap(1, near, 1)
        own_piece(2, 1, y, 1, near)
        row_line(3)
        row_depth(2)
        row_depth(3)
        swap(1, far, 0)
        row_last(0)

    def outside():
        swap(1, near, 1)
        row_line(0)
        row_line(1)
        wait_y(2, inner_z)
        row_line(2)
        swap(1, far, 0)
        row_line(3)
        row_depth(0)
        wait_y(1, near)
        swap(1, far, 1)
        own_piece(2, 0, y, 0, inner_z)
        row_depth(1)
        own_piece(2, 0, y, 1, inner_z)
        row_depth(2)
        row_depth(3)
        own_piece(2, 1, y, 0, inner_z)
        row_last(0)

    by_role(inside, outside)
    norm_ffn(0)

    def inside():
        row_last(1)

    def outside():
        wait_y(1, far)
        own_piece(2, 1, y, 1, inner_z)
        row_last(1)

    by_role(inside, outside)
    norm_ffn(1)

    def inside():
        wait_y(1, near)
        row_last(2)

    def outside():
        row_last(2)

    by_role(inside, outside)
    norm_ffn(2)

    def inside():
        swap(1, far, 1)
        row_last(3)

    def outside():
        own_piece(2, 1, 1 - y, 0, inner_z)
        row_last(3)

    by_role(inside, outside)
    norm_ffn(3)
    own_resid()

    def inside():
        inwards(2, near, 0)
        cross(2, 0, 0)
        inwards(2, near, 1)
        cross(2, 0, 1)
        swap(2, near, 0)
        wait_y(1, far)
        cross(2, 1, 0)

    def outside():
        own_piece(2, 1, 1 - y, 1, inner_z)

    by_role(inside, outside)
    hidden_rows(0)

    def inside():
        swap(2, near, 1)

    def outside():
        swap(2, near, 0)

    by_role(inside, outside)
    hidden_rows(1)

    def inside():
        inwards(2, far, 0)
        cross(2, 1, 1)

    def outside():
        swap(2, near, 1)

    by_role(inside, outside)
    down(0, cells[0])
    down(1, cells[1])
    pair(0)
    down(2, cells[2])
    pair(1)

    def inside():
        inwards(2, far, 1)
        wait_pair(2)

    pl.when(inner)(inside)
    down(3, cells[3])

    def inside():
        wait_y(2, near)

    pl.when(inner)(inside)
    pair(2)

    def inside():
        swap(2, far, 0)

    pl.when(inner)(inside)
    pair(3)
    down(4, cells[4])

    def inside():
        swap(2, far, 1)

    def outside():
        wait_y(2, near)
        swap(2, far, 0)

    by_role(inside, outside)
    pair(4)
    finish(0, cells[0])
    down(5, cells[5])
    pair(5)
    finish(1, cells[1])

    def outside():
        swap(2, far, 1)

    pl.when(jnp.logical_not(inner))(outside)
    down(6, cells[6])
    pair(6)
    finish(2, cells[2])

    def inside():
        wait_y(2, far)

    def outside():
        wait_y(2, far)

    by_role(inside, outside)
    down(7, cells[7])
    pair(7)
    finish(3, cells[3])
    finish(4, cells[4])
    finish(5, cells[5])
    finish(6, cells[6])
    finish(7, cells[7])
    for cell in range(8):
        out[:, cell * part_width : (cell + 1) * part_width] = final[cell]

    token_copy(mine).wait_send()
    scale_copy(0, z, pair_z).wait_send()

    def inside():
        scale_copy(1, z, near).wait_send()
        scale_copy(2, outer_z, near).wait_send()
        scale_copy(3, near, outer_z).wait_send()
        scale_copy(4, far, outer_z).wait_send()
        for matrix in range(3):
            for number in numbers(matrix, y):
                for part in range(2):
                    z_copy(matrix, part, z, number, near).wait_send()
                    z_copy(matrix, part, outer_z, number, near).wait_send()
                for block in (z, near, far):
                    z_copy(matrix, 0, block, number, outer_z, True).wait_send()
                for block in (near, far):
                    y_copy(matrix, block, number).wait_send()

    def outside():
        for matrix in range(3):
            for part, half in ((0, y), (1, y), (1, 1 - y)):
                for number in numbers(matrix, half):
                    z_copy(matrix, part, z, number, inner_z).wait_send()
            for number in numbers(matrix, y):
                for block in (inner_z, near, far):
                    y_copy(matrix, block, number).wait_send()

    by_role(inside, outside)
    for step in range(1, 4):
        norm_copy(step, t).wait_send()
    for way in range(7):
        for s in range(4):
            row_copy(way, s, t, {"tp": partner}).wait_send()
    for k in range(8):
        core_copy(k).wait_send()
        for way in range(3):
            line_copy(k, way).wait_send()


ANYWHERE = pl.BlockSpec(memory_space=pl.ANY)
INSIDE = pl.BlockSpec(memory_space=pltpu.VMEM)


def tables(heads):
    places = np.arange(LEN, dtype=np.float64)
    half = DK // 2
    frequency = (THETA ** (-(np.arange(half) / half))).astype(np.float32)
    angle = (places[:, None].astype(np.float32) * frequency).astype(np.float32)
    distance = places[:, None] - places[None, :]
    gamma = 1.0 - 2.0 ** (-5.0 - np.arange(heads, dtype=np.float64))
    powers = gamma[:, None, None] ** np.maximum(distance, 0.0)
    decay = np.where(distance >= 0, powers, 0.0) * DK ** (-0.5)
    wide = angle.astype(np.float64)
    return (
        decay.astype(np.float32),
        np.cos(wide).astype(np.float32),
        np.sin(wide).astype(np.float32),
    )


def layer(stream, gains, mix_w, mix_scales, up_w, up_scales, w_down, scale_down, tp_count):
    group, width = stream.shape
    share = group // tp_count
    depth, heads_width = mix_w[0].shape
    units = w_down.shape[0]
    blocks = width // depth
    narrow, wide = jnp.bfloat16, jnp.float32
    local_heads = heads_width // DK
    decays, cosine, sine = tables(local_heads * tp_count)
    row = lambda vector: vector[None, :]
    most = max(PIECES)
    dma = pltpu.SemaphoreType.DMA
    half_units = units // 2
    cells = 2 * blocks
    part = depth // 2
    scratch = (
        [pltpu.VMEM(w.shape, wide) for w in mix_w]
        + [
            pltpu.VMEM((4 * half_units, depth), wide),
            pltpu.VMEM((4 * half_units, part), wide),
            pltpu.VMEM((2 * group, width), narrow),
            pltpu.VMEM((1, LEN, LEN), wide),
            pltpu.VMEM(cosine.shape, wide),
            pltpu.VMEM(sine.shape, wide),
            *(pltpu.VMEM((1, width), wide) for _ in gains),
            *(pltpu.VMEM((1, heads_width), wide) for _ in mix_scales),
            pltpu.VMEM((1, depth), wide),
            pltpu.VMEM((2 * width, 3 * DK), narrow),
            pltpu.VMEM((cells * units, depth), narrow),
            pltpu.VMEM((cells * units, part), narrow),
            pltpu.VMEM((blocks, 2 * group, depth), narrow),
            pltpu.VMEM((2 * group, 3 * DK), wide),
            pltpu.VMEM((cells, 2 * group, DV), narrow),
            pltpu.VMEM((cells, share, part), wide),
            pltpu.VMEM((share, width), wide),
            pltpu.VMEM((2 * group, width), narrow),
            pltpu.VMEM((2 * group, half_units), narrow),
            pltpu.VMEM((cells, 2, 4, share, part), narrow),
            pltpu.VMEM((cells, 4, share, part), narrow),
            pltpu.VMEM((cells, 3, share, part), narrow),
            pltpu.VMEM((cells, 3, share, part), narrow),
            pltpu.VMEM((cells, share, part), wide),
            pltpu.VMEM((cells, 1, part), wide),
        ]
        + [
            dma((21,)),
            dma((3, 8, most)), dma((3, 4, most)), dma((3, 8, most)),
            dma((3, 4, most)), dma((3, 4, most)),
            dma((5,)), dma((4,)), dma((1,)), dma((1,)), dma((3,)), dma((3,)),
            dma((7, 4)), dma((7, 4)),
            dma((8,)), dma((8,)), dma((8, 3)), dma((8, 3)),
        ]
    )
    return pl.pallas_call(
        layer_kernel,
        out_shape=jax.ShapeDtypeStruct((share, width), wide),
        in_specs=[ANYWHERE] * 15 + [INSIDE] * 2 + [ANYWHERE],
        out_specs=INSIDE,
        scratch_shapes=scratch,
        compiler_params=pltpu.CompilerParams(
            collective_id=0, has_side_effects=True, vmem_limit_bytes=60 * 2**20
        ),
    )(
        stream, *mix_w, *up_w, w_down, decays, cosine, sine, *(row(gain) for gain in gains),
        *(row(scale) for scale in mix_scales), *up_scales, row(scale_down),
    ).astype(narrow)


def summed_over_tp(partial_sum, share):
    partial_sum = partial_sum.reshape(-1, share, partial_sum.shape[1])
    pieces = lax.all_to_all(partial_sum, "tp", split_axis=0, concat_axis=0)
    return jnp.sum(pieces.astype(jnp.float32), axis=0)


def shards(
    stream,
    gain_mix,
    w_query,
    scale_query,
    w_key,
    scale_key,
    w_value,
    scale_value,
    gain_ffn,
    w_gate,
    scale_gate,
    w_up,
    scale_up,
    w_down,
    scale_down,
):
    group_rows = stream.shape[0]
    tp_count = lax.axis_size("tp")
    if (lax.axis_size("rep"), lax.axis_size("fs"), tp_count) == (2, 4, 4):
        return layer(
            stream, (gain_mix, gain_ffn), (w_query, w_key, w_value),
            (scale_query, scale_key, scale_value), (w_gate.T, w_up.T), (scale_gate, scale_up),
            w_down.T, scale_down, tp_count,
        )
    stream_f = stream.astype(jnp.float32)
    normed = (stream_f * rms_scale(stream_f) * gain_mix).astype(jnp.bfloat16)
    mix_w = jnp.concatenate([w.astype(jnp.bfloat16) for w in (w_query, w_key, w_value)], axis=1)
    up_w = jnp.concatenate([w.astype(jnp.bfloat16) for w in (w_gate, w_up)], axis=1)
    down_w = w_down.astype(jnp.bfloat16)
    down_scale = lax.all_gather(scale_down, "fs", axis=0, tiled=True)
    mix_acc = dot(normed, lax.all_gather(mix_w, "fs", axis=0, tiled=True))
    mix_scale = jnp.concatenate([scale_query, scale_key, scale_value])
    query, key, value = jnp.split(
        (mix_acc * mix_scale).astype(jnp.bfloat16),
        [w_query.shape[1], w_query.shape[1] + w_key.shape[1]],
        axis=1,
    )
    local_heads = query.shape[1] // DK
    positions = jnp.arange(group_rows, dtype=jnp.int32) % LEN
    mixed = []
    for head in range(local_heads):
        columns = slice(head * DK, (head + 1) * DK)
        queries = rotate(query[:, columns].astype(jnp.float32), positions)
        keys = rotate(key[:, columns].astype(jnp.float32), positions) * DK ** (-0.5)
        values = value[:, head * DV : (head + 1) * DV].astype(jnp.float32)
        head_id = (lax.axis_index("tp") * local_heads + head).astype(jnp.float32)
        log_decay = jnp.log(1.0 - jnp.power(2.0, -5.0 - head_id))
        retained = retention(queries, keys, values, log_decay)
        mixed.append((retained * head_scale(retained)).astype(jnp.bfloat16))
    mixed = jnp.concatenate(mixed, axis=1)
    share = group_rows // tp_count
    own_rows = lax.dynamic_slice_in_dim(stream, lax.axis_index("tp") * share, share, 0)
    arrived = lax.all_to_all(mixed, "tp", split_axis=0, concat_axis=1, tiled=True)
    resid = own_rows.astype(jnp.float32) + arrived.astype(jnp.float32)
    normed_ffn = (resid * rms_scale(resid) * gain_ffn).astype(jnp.bfloat16)
    piece = lax.all_gather(normed_ffn, "tp", axis=0, tiled=True)
    up_acc = dot(piece, lax.all_gather(up_w, "fs", axis=0, tiled=True))
    units = w_gate.shape[1]
    gate = up_acc[:, :units] * scale_gate
    upward = up_acc[:, units:] * scale_up
    hidden = (jax.nn.silu(gate) * upward).astype(jnp.bfloat16)
    whole = dot_t(hidden, lax.all_gather(down_w, "fs", axis=0, tiled=True))
    channel_out = summed_over_tp((whole * down_scale).astype(jnp.bfloat16), share)
    return (resid + channel_out).astype(jnp.bfloat16)


def solution(mesh):
    placed = (
        P(("rep", "fs"), None),
        P(),
        P("fs", "tp"),
        P("tp"),
        P("fs", "tp"),
        P("tp"),
        P("fs", "tp"),
        P("tp"),
        P(),
        P("fs", "tp"),
        P("tp"),
        P("fs", "tp"),
        P("tp"),
        P("fs", "tp"),
        P("fs"),
    )
    return jax.shard_map(
        shards, mesh=mesh, in_specs=placed, out_specs=P(("rep", "fs", "tp"), None), check_vma=False
    )
```

```python
import numpy as np
import jax
import jax.numpy as jnp
from jax import lax
from jax.experimental import pallas as pl
from jax.experimental.pallas import tpu as pltpu
from jax.sharding import PartitionSpec as P

DK = 256
DV = 256
LEN = 128


EPS = 1e-06
THETA = 10000.0
HIGH = lax.Precision.HIGHEST


def rms_scale(values):
    return lax.rsqrt(jnp.mean(values * values, axis=-1, keepdims=True) + EPS)


def head_scale(values):
    return 1.0 / jnp.maximum(jnp.sqrt(jnp.mean(values * values, axis=-1, keepdims=True)), 1.0)


def rotate(heads_data, positions):
    half = heads_data.shape[-1] // 2
    frequency = THETA ** (-(jnp.arange(half, dtype=jnp.float32) / half))
    angle = positions.astype(jnp.float32)[:, None] * frequency
    cosine = jnp.cos(angle)
    sine = jnp.sin(angle)
    first = heads_data[..., :half]
    second = heads_data[..., half:]
    return jnp.concatenate(
        [first * cosine - second * sine, second * cosine + first * sine], axis=-1
    )


def retention(queries, keys, values, log_decay):
    offsets = jnp.arange(LEN, dtype=jnp.float32)
    distance = offsets[:, None] - offsets[None, :]
    decay = jnp.where(distance >= 0, jnp.exp(log_decay * jnp.maximum(distance, 0.0)), 0.0)
    queries, keys, values = (
        part.reshape(-1, LEN, part.shape[-1]) for part in (queries, keys, values)
    )
    scores = jnp.einsum("sid,sjd->sij", queries, keys, precision=HIGH) * decay
    retained = jnp.einsum("sij,sje->sie", scores, values, precision=HIGH)
    return retained.reshape(-1, values.shape[-1])


def dot(left, right):
    return jnp.dot(left, right, preferred_element_type=jnp.float32)


def dot_t(left, right):
    return lax.dot_general(left, right, (((1,), (1,)), ((), ())), preferred_element_type=jnp.float32)


MESH = pl.DeviceIdType.MESH
PIECES = (8, 4, 4)


def signal(peer):
    barrier = pltpu.get_barrier_semaphore()
    pl.semaphore_signal(barrier, inc=1, device_id=peer, device_id_type=MESH)


def remote(source, target, send, recv, device):
    return pltpu.make_async_remote_copy(
        src_ref=source,
        dst_ref=target,
        send_sem=send,
        recv_sem=recv,
        device_id=device,
        device_id_type=MESH,
    )


def span(index, size):
    return pl.ds(pl.multiple_of(index * size, size), size)


def layer_kernel(
    stream, w_query, w_key, w_value, w_gate, w_up, w_down, decays,
    cosine_in, sine_in, gain_mix_in, gain_ffn_in, scale_query_in, scale_key_in, scale_value_in,
    scale_gate, scale_up, scale_down_in,
    out,
    f_query, f_key, f_value, f_up, f_down, rows, decay,
    cosine, sine, gain_mix, gain_ffn, scale_query, scale_key, scale_value, scale_down,
    mix_w, up_w, down_w, normed, mix_acc, mixed, resid, row_sum, normed_ffn,
    hidden, partial, from_core, paired, from_line, final, down_scale,
    local, cross_send, inward_send, z_recv, y_send, y_recv, scale_send, scale_recv,
    token_send, token_recv, norm_send, norm_recv, row_send, row_recv,
    core_send, core_recv, line_send, line_recv,
):
    z, y, t = lax.axis_index("fs"), lax.axis_index("rep"), lax.axis_index("tp")
    group, width = stream.shape
    share = group // 4
    depth = w_query.shape[0]
    units = w_gate.shape[0] // 2
    part_width = depth // 2
    heights = (depth, 2 * units, 2 * units)
    inner = (z == 1) | (z == 2)
    mine = jnp.where(inner, 1, 0)
    pair_z = z + 1 - 2 * lax.rem(z, 2)
    outer_z, inner_z = jnp.where(inner, pair_z, z), jnp.where(inner, z, pair_z)
    near, far = 3 - inner_z, 3 - outer_z
    core, x = lax.rem(t, 2), t // 2
    partner = t + 1 - 2 * core
    twin = lax.rem(t + 2, 4)
    diagonal = lax.rem(partner + 2, 4)

    for step in range(4):
        for apart in range(2):
            if step or apart:
                signal({"fs": pair_z if apart else z, "tp": lax.rem(t + step, 4)})
    signal({"rep": 1 - y})

    @pl.when(inner)
    def _():
        signal({"fs": near})

    moves = [(w_query, f_query), (w_key, f_key), (w_value, f_value)]
    moves.append((stream, rows.at[span(mine, group)]))
    for part in range(2):
        for place, matrix in enumerate((w_gate, w_up)):
            moves.append((
                matrix.at[pl.ds(part * units, units)],
                f_up.at[pl.ds((2 * part + place) * units, units)],
            ))
    for part in range(2):
        for half in range(2):
            moves.append((
                w_down.at[pl.ds(part * units, units), pl.ds(half * part_width, part_width)],
                f_down.at[pl.ds((2 * part + half) * units, units)],
            ))
    moves.append((decays.at[pl.ds(2 * t + mine, 1)], decay))
    moves += [
        (cosine_in, cosine), (sine_in, sine), (gain_mix_in, gain_mix), (gain_ffn_in, gain_ffn),
        (scale_query_in, scale_query), (scale_key_in, scale_key), (scale_value_in, scale_value),
        (scale_down_in, scale_down),
    ]
    loads = [
        pltpu.make_async_copy(source, target, local.at[index])
        for index, (source, target) in enumerate(moves)
    ]
    for load in loads:
        load.start()

    weights = (mix_w, up_w, down_w)

    def place_of(matrix, block, number):
        height = heights[matrix]
        piece = height // PIECES[matrix]
        return pl.ds(pl.multiple_of(block * height + number * piece, piece), piece)

    def numbers(matrix, half):
        count = PIECES[matrix] // 2
        return [count * half + step for step in range(count)]

    def cast(matrix, part, half):
        for number in numbers(matrix, half):
            there = place_of(matrix, part * 4 + z, number)
            if matrix == 0:
                here = place_of(0, 0, number)
                for place, full in enumerate((f_query, f_key, f_value)):
                    columns = slice(place * DK, (place + 1) * DK)
                    source = full[here, part * DK : (part + 1) * DK]
                    mix_w[there, columns] = source.astype(jnp.bfloat16)
            else:
                full = f_up if matrix == 1 else f_down
                source = full[place_of(matrix, part, number), :]
                weights[matrix][there, :] = source.astype(jnp.bfloat16)

    def z_copy(matrix, part, block, number, target, inward=False):
        cell = part * 4 + block
        view = weights[matrix].at[place_of(matrix, cell, number)]
        if inward:
            send = inward_send.at[matrix, block, number]
        else:
            send = cross_send.at[matrix, cell, number]
        return remote(view, view, send, z_recv.at[matrix, cell, number], {"fs": target})

    def y_copy(matrix, block, number):
        view = weights[matrix].at[place_of(matrix, mine * 4 + block, number)]
        return remote(
            view, view, y_send.at[matrix, block, number], y_recv.at[matrix, block, number],
            {"rep": 1 - y},
        )

    def send_own(matrix, part, half, target, inward=False):
        for number in numbers(matrix, half):
            z_copy(matrix, part, z, number, target, inward).start()

    def own_piece(matrix, part, half, step, target, inward=False):
        z_copy(matrix, part, z, numbers(matrix, half)[step], target, inward).start()

    def scale_pass(slot, block, target):
        scale_copy(1 if block is near else 0 if slot == 2 else 2, block, target).wait_recv()
        scale_copy(slot, block, target).start()

    def tokens_on():
        token_copy(1 - mine).wait_recv()
        for step in range(1, 4):
            norm_copy(step, t).start()

    def pair_rows():
        for step in range(1, 4):
            norm_copy(step, lax.rem(t + 4 - step, 4)).wait_recv()
        for number in range(4):
            norm_rows(1 - mine, number)

    def cross_last():
        z_copy(2, 1, outer_z, numbers(2, 1 - y)[1], near).start()

    def take_last():
        z_copy(2, 1, far, numbers(2, y)[1], pair_z).wait_recv()

    def wait_last():
        y_copy(2, far, numbers(2, 1 - y)[0]).wait_recv()
        z_copy(2, 1, far, numbers(2, 1 - y)[1], pair_z).wait_recv()

    def scales_in():
        for block in (inner_z, near, far):
            scale_copy(0, block, outer_z).wait_recv()

    def wait_y(matrix, block):
        for number in numbers(matrix, 1 - y):
            y_copy(matrix, block, number).wait_recv()

    def cross(matrix, part, step):
        number = numbers(matrix, y)[step]
        z_copy(matrix, part, outer_z, number, near).wait_recv()
        z_copy(matrix, part, outer_z, number, near).start()

    def inwards(matrix, block, step):
        number = numbers(matrix, y)[step]
        z_copy(matrix, 0, block, number, outer_z, True).wait_recv()
        z_copy(matrix, 0, block, number, outer_z, True).start()

    def swap(matrix, block, step):
        number = numbers(matrix, y)[step]
        z_copy(matrix, mine, block, number, pair_z).wait_recv()
        y_copy(matrix, block, number).start()

    def swap_all(matrix, block):
        for step in range(PIECES[matrix] // 2):
            swap(matrix, block, step)

    def wait_pair(matrix):
        for number in numbers(matrix, 1 - y):
            z_copy(matrix, 1, outer_z, number, near).wait_recv()

    def by_role(inside, outside):
        pl.when(inner)(inside)
        pl.when(jnp.logical_not(inner))(outside)

    def norm_rows(side, number):
        here = span(side * 4 + number, share)
        values = rows[here, :].astype(jnp.float32)
        factor = lax.rsqrt(jnp.mean(values * values, axis=1, keepdims=True) + EPS)
        values = (values * factor * gain_mix[...]).astype(jnp.bfloat16)
        for block in range(4):
            normed[block, here, :] = values[:, block * depth : (block + 1) * depth]

    def token_copy(side):
        part = rows.at[span(side * 4 + t, share)]
        return remote(part, part, token_send.at[0], token_recv.at[0], {"fs": pair_z})

    def norm_copy(step, owner):
        part = rows.at[span((1 - mine) * 4 + owner, share)]
        peer = lax.rem(t + step, 4)
        return remote(part, part, norm_send.at[step - 1], norm_recv.at[step - 1], {"tp": peer})

    def scale_copy(slot, block, target):
        cells = down_scale.at[pl.ds(2 * block, 2)]
        return remote(cells, cells, scale_send.at[slot], scale_recv.at[block], {"fs": target})

    def project(block, first):
        product = dot(normed[block], mix_w[span(mine * 4 + block, depth), :])
        if first:
            mix_acc[...] = product
        else:
            mix_acc[...] += product

    lanes = pl.ds(pl.multiple_of(mine * DK, DK), DK)

    def retain(s):
        here = slice(s * LEN, (s + 1) * LEN)
        cos, sin = cosine[...], sine[...]

        def turned(offset, scale):
            values = mix_acc[here, offset : offset + DK] * scale
            values = values.astype(jnp.bfloat16).astype(jnp.float32)
            first, second = values[:, : DK // 2], values[:, DK // 2 :]
            return jnp.concatenate(
                [first * cos - second * sin, second * cos + first * sin], axis=1
            ).astype(jnp.bfloat16)

        queries = turned(0, scale_query[:, lanes])
        keys = turned(DK, scale_key[:, lanes])
        values = (mix_acc[here, 2 * DK :] * scale_value[:, lanes]).astype(jnp.bfloat16)
        scores = (dot_t(queries, keys) * decay[0]).astype(jnp.bfloat16)
        retained = dot(scores, values)
        mixed[2 * t + mine, here, :] = (retained * head_scale(retained)).astype(jnp.bfloat16)
        own = 2 * t + mine
        row_copy(1, s, own, {"tp": twin}).start()
        row_copy(2, s, own, {"fs": pair_z}).start()
        row_copy(0, s, own, {"tp": partner}).start()

    def row_copy(way, s, cell, target):
        part = mixed.at[cell, pl.ds(s * LEN, LEN)]
        return remote(part, part, row_send.at[way, s], row_recv.at[way, s], target)

    def row_wait(way, s):
        cell = (
            2 * partner + mine, 2 * twin + mine, 2 * t + 1 - mine, 2 * twin + 1 - mine,
            2 * diagonal + mine, 2 * partner + 1 - mine, 2 * diagonal + 1 - mine,
        )[way]
        row_copy(way, s, cell, {"tp": partner}).wait_recv()

    def row_line(s):
        cell = 2 * twin + mine
        row_wait(1, s)
        pl.when(core == 0)(row_copy(3, s, cell, {"fs": pair_z}).start)
        row_copy(4, s, cell, {"tp": partner}).start()

    def row_depth(s):
        cell = 2 * t + 1 - mine
        row_wait(2, s)
        pl.when(core == 1)(row_copy(3, s, cell, {"tp": twin}).start)
        row_copy(5, s, cell, {"tp": partner}).start()

    def row_last(s):
        row_wait(3, s)
        row_copy(6, s, 2 * twin + 1 - mine, {"tp": partner}).start()

    def norm_ffn(s):
        for way in (0, 4, 5, 6):
            row_wait(way, s)
        for first in range(s * LEN, (s + 1) * LEN, share):
            here = slice(first, first + share)
            squares = 0.0
            for cell in range(8):
                columns = slice(cell * part_width, (cell + 1) * part_width)
                values = rows[here, columns].astype(jnp.float32)
                values += mixed[cell, here, :].astype(jnp.float32)
                row_sum[:, columns] = values
                squares += jnp.sum(values * values, axis=1, keepdims=True)
            factor = lax.rsqrt(squares / width + EPS)
            for cell in range(8):
                columns = slice(cell * part_width, (cell + 1) * part_width)
                normed_ffn[here, columns] = (
                    row_sum[:, columns] * factor * gain_ffn[:, columns]
                ).astype(jnp.bfloat16)

    def own_resid():
        here = span(mine * 4 + t, share)
        for cell in range(8):
            columns = slice(cell * part_width, (cell + 1) * part_width)
            values = rows[here, columns].astype(jnp.float32)
            resid[cell] = values + mixed[cell, here, :].astype(jnp.float32)

    def chosen(scale):
        full = scale[...][None, :]
        return jnp.where(inner, full[:, units:], full[:, :units])

    def hidden_rows(side):
        here = slice(side * group, (side + 1) * group)

        def projected(place):
            total = 0.0
            for block in range(4):
                left = normed_ffn[here, block * depth : (block + 1) * depth]
                part = span((mine * 4 + block) * 2 + place, units)
                total += dot_t(left, up_w[part, :])
            return total

        gate = projected(0) * chosen(scale_gate)
        upward = projected(1) * chosen(scale_up)
        hidden[here, :] = (gate / (1.0 + jnp.exp(-gate)) * upward).astype(jnp.bfloat16)

    def core_copy(k):
        return remote(
            partial.at[k, 1 - core], from_core.at[k], core_send.at[k], core_recv.at[k],
            {"tp": partner},
        )

    line_targets = (
        ({"fs": pair_z, "tp": twin}, (1 - mine) * 2 + 1 - x),
        ({"tp": twin}, mine * 2 + 1 - x),
        ({"fs": pair_z}, (1 - mine) * 2 + x),
    )

    def line_copy(k, way):
        return remote(
            paired.at[k, way], from_line.at[k, way], line_send.at[k, way], line_recv.at[k, way],
            line_targets[way][0],
        )

    def down(k, cell):
        products = dot(hidden[...], down_w[span(mine * 8 + cell, units), :])
        products = (products * down_scale[cell]).astype(jnp.bfloat16)
        for owner in range(8):
            partial[k, owner % 2, owner // 2] = products[owner * share : (owner + 1) * share]
        core_copy(k).start()

    def both(k, chip):
        return partial[k, core, chip].astype(jnp.float32) + from_core[k, chip].astype(jnp.float32)

    def pair(k):
        core_copy(k).wait_recv()
        for way in range(3):
            paired[k, way] = both(k, line_targets[way][1]).astype(jnp.bfloat16)
            line_copy(k, way).start()

    def finish(k, cell):
        total = both(k, mine * 2 + x)
        for way in (1, 2, 0):
            line_copy(k, way).wait_recv()
            total += from_line[k, way].astype(jnp.float32)
        final[cell] = resid[cell] + total

    for load in loads[:3]:
        load.wait()
    cast(0, 0, y)
    pl.semaphore_wait(pltpu.get_barrier_semaphore(), jnp.where(inner, 9, 8))

    def inside():
        send_own(0, 0, y, near)
        send_own(0, 0, y, outer_z, True)

    def outside():
        send_own(0, 0, y, inner_z)

    by_role(inside, outside)
    loads[3].wait()
    token_copy(mine).start()
    cast(0, 1, y)

    def outside():
        send_own(0, 1, y, inner_z)
        cast(0, 0, 1 - y)

    pl.when(jnp.logical_not(inner))(outside)
    cast(0, 1, 1 - y)
    for load in loads[4:]:
        load.wait()
    for half in range(2):
        down_scale[z * 2 + half] = scale_down[:, half * part_width : (half + 1) * part_width]
    scale_copy(0, z, pair_z).start()

    def inside():
        scale_copy(1, z, near).start()

    pl.when(inner)(inside)
    for matrix in (1, 2):
        for part in range(2):
            for half in range(2):
                cast(matrix, part, half)
    for number in range(4):
        norm_rows(mine, number)
    cells = (
        outer_z * 2 + y, inner_z * 2 + y, inner_z * 2 + 1 - y, outer_z * 2 + 1 - y,
        near * 2 + y, near * 2 + 1 - y,
        far * 2 + y, far * 2 + 1 - y,
    )

    def inside():
        own_piece(0, 1, y, 0, near)
        own_piece(0, 1, y, 1, near)
        own_piece(1, 0, y, 0, outer_z, True)
        own_piece(0, 1, y, 2, near)
        inwards(0, near, 0)
        cross(0, 0, 0)
        inwards(0, near, 1)
        cross(0, 0, 1)
        inwards(0, near, 2)
        cross(0, 0, 2)
        inwards(0, near, 3)
        scale_pass(3, near, outer_z)
        cross(0, 0, 3)
        swap(0, near, 0)
        own_piece(0, 1, y, 3, near)
        own_piece(1, 0, y, 1, outer_z, True)
        swap(0, near, 1)
        own_piece(1, 0, y, 0, near)
        tokens_on()
        swap(0, near, 2)
        cross(0, 1, 0)
        inwards(0, far, 0)
        cross(0, 1, 1)
        inwards(0, far, 1)
        cross(0, 1, 2)
        inwards(0, far, 2)

    def outside():
        swap(0, inner_z, 0)
        swap(0, inner_z, 1)
        swap(0, inner_z, 2)
        own_piece(1, 0, y, 0, inner_z)
        swap(0, inner_z, 3)
        own_piece(1, 0, y, 1, inner_z)
        wait_y(0, inner_z)
        tokens_on()
        own_piece(1, 1, y, 0, inner_z)
        swap(1, inner_z, 0)
        own_piece(1, 1, y, 1, inner_z)
        swap(0, near, 0)
        swap(0, near, 1)

    by_role(inside, outside)
    pair_rows()

    def inside():
        scale_pass(2, outer_z, near)
        inwards(0, far, 3)
        cross(0, 1, 3)

    pl.when(inner)(inside)
    project(z, True)

    def inside():
        own_piece(1, 0, y, 1, near)
        swap(0, near, 3)
        cross(1, 0, 0)
        inwards(1, near, 0)
        wait_y(0, near)
        swap(0, far, 0)
        cross(1, 0, 1)
        swap(0, far, 1)
        swap(0, far, 2)
        scale_pass(4, far, outer_z)
        own_piece(1, 1, y, 0, near)
        own_piece(2, 0, y, 0, outer_z, True)
        swap(0, far, 3)
        own_piece(2, 0, y, 1, outer_z, True)
        own_piece(1, 1, y, 1, near)
        inwards(1, near, 1)
        wait_y(0, far)
        cross(1, 1, 0)
        inwards(1, far, 0)
        cross(1, 1, 1)
        inwards(1, far, 1)
        wait_pair(0)

    def outside():
        swap(0, near, 2)

    by_role(inside, outside)
    project(pair_z, False)

    def outside():
        swap(0, near, 3)
        own_piece(2, 0, y, 0, inner_z)
        swap(1, inner_z, 1)
        own_piece(2, 0, y, 1, inner_z)
        swap(0, far, 0)
        wait_y(0, near)

    pl.when(jnp.logical_not(inner))(outside)
    project(near, False)

    def outside():
        swap(0, far, 1)
        swap(0, far, 2)
        wait_y(1, inner_z)
        own_piece(0, 1, 1 - y, 0, inner_z)
        swap(0, far, 3)
        own_piece(0, 1, 1 - y, 1, inner_z)
        own_piece(0, 1, 1 - y, 2, inner_z)
        swap(1, near, 0)
        scales_in()
        own_piece(0, 1, 1 - y, 3, inner_z)
        swap(2, inner_z, 0)
        wait_y(0, far)

    pl.when(jnp.logical_not(inner))(outside)
    project(far, False)

    def inside():
        own_piece(2, 0, y, 0, near)

    def outside():
        own_piece(1, 1, 1 - y, 0, inner_z)

    by_role(inside, outside)
    retain(0)

    def inside():
        swap(1, near, 0)

    def outside():
        swap(2, inner_z, 1)

    by_role(inside, outside)
    retain(1)

    def inside():
        own_piece(2, 0, y, 1, near)

    pl.when(inner)(inside)
    retain(2)
    retain(3)

    def inside():
        row_depth(0)
        cross(2, 0, 0)
        row_depth(1)
        swap(1, near, 1)
        row_line(0)
        cross(2, 0, 1)
        row_depth(2)
        row_line(1)
        row_depth(3)
        own_piece(2, 1, y, 0, near)
        row_line(2)
        swap(1, far, 0)
        row_last(0)

    def outside():
        swap(1, near, 1)
        row_line(0)
        row_line(1)
        wait_y(2, inner_z)
        row_line(2)
        swap(1, far, 0)
        row_line(3)
        wait_y(1, near)
        swap(1, far, 1)
        row_depth(0)
        own_piece(1, 1, 1 - y, 1, inner_z)
        row_depth(1)
        row_depth(2)
        row_depth(3)
        own_piece(2, 1, y, 0, inner_z)
        wait_y(1, far)
        row_last(0)

    by_role(inside, outside)
    norm_ffn(0)

    def inside():
        own_piece(2, 1, y, 1, near)
        row_line(3)
        row_last(1)

    def outside():
        own_piece(2, 1, y, 1, inner_z)
        row_last(1)

    by_role(inside, outside)
    norm_ffn(1)

    def inside():
        row_last(2)

    def outside():
        row_last(2)

    by_role(inside, outside)
    norm_ffn(2)

    def inside():
        wait_y(1, near)
        swap(1, far, 1)
        row_last(3)
        inwards(2, near, 0)

    def outside():
        own_piece(2, 1, 1 - y, 0, inner_z)
        row_last(3)

    by_role(inside, outside)
    norm_ffn(3)
    own_resid()

    def inside():
        inwards(2, near, 1)
        wait_pair(1)
        inwards(2, far, 0)
        cross(2, 1, 0)
        wait_y(1, far)

    def outside():
        own_piece(2, 1, 1 - y, 1, inner_z)

    by_role(inside, outside)
    hidden_rows(0)

    def inside():
        inwards(2, far, 1)
        cross(2, 1, 1)

    def outside():
        swap(2, near, 0)

    by_role(inside, outside)
    hidden_rows(1)

    def inside():
        swap(2, near, 0)

    def outside():
        swap(2, near, 1)

    by_role(inside, outside)
    down(0, cells[0])
    down(1, cells[1])

    def outside():
        swap(2, far, 0)

    pl.when(jnp.logical_not(inner))(outside)
    pair(0)

    def inside():
        swap(2, near, 1)

    pl.when(inner)(inside)
    down(2, cells[2])
    pair(1)

    def inside():
        wait_pair(2)
        cross_last()

    pl.when(inner)(inside)
    down(3, cells[3])

    def inside():
        swap(2, far, 0)

    pl.when(inner)(inside)
    pair(2)

    def outside():
        swap(2, far, 1)

    pl.when(jnp.logical_not(inner))(outside)
    pair(3)
    down(4, cells[4])

    def inside():
        take_last()

    def outside():
        wait_y(2, near)

    by_role(inside, outside)
    pair(4)
    finish(0, cells[0])

    def inside():
        wait_y(2, near)

    pl.when(inner)(inside)
    down(5, cells[5])
    pair(5)

    def outside():
        wait_y(2, far)

    pl.when(jnp.logical_not(inner))(outside)
    finish(1, cells[1])
    down(6, cells[6])

    def inside():
        wait_last()

    pl.when(inner)(inside)
    pair(6)
    finish(2, cells[2])
    down(7, cells[7])
    pair(7)
    finish(3, cells[3])
    finish(4, cells[4])
    finish(5, cells[5])
    finish(6, cells[6])
    finish(7, cells[7])
    for cell in range(8):
        out[:, cell * part_width : (cell + 1) * part_width] = final[cell].astype(jnp.bfloat16)

    token_copy(mine).wait_send()
    scale_copy(0, z, pair_z).wait_send()

    def inside():
        scale_copy(1, z, near).wait_send()
        scale_copy(2, outer_z, near).wait_send()
        scale_copy(3, near, outer_z).wait_send()
        scale_copy(4, far, outer_z).wait_send()
        for matrix in range(3):
            for number in numbers(matrix, y):
                for part in range(2):
                    z_copy(matrix, part, z, number, near).wait_send()
                    z_copy(matrix, part, outer_z, number, near).wait_send()
                for block in (z, near, far):
                    z_copy(matrix, 0, block, number, outer_z, True).wait_send()
                y_copy(matrix, near, number).wait_send()
            for number in numbers(matrix, y)[: -1 if matrix == 2 else None]:
                y_copy(matrix, far, number).wait_send()
        z_copy(2, 1, outer_z, numbers(2, 1 - y)[1], near).wait_send()

    def outside():
        for matrix in range(3):
            for part, half in ((0, y), (1, y), (1, 1 - y)):
                for number in numbers(matrix, half):
                    z_copy(matrix, part, z, number, inner_z).wait_send()
            for number in numbers(matrix, y):
                for block in (inner_z, near, far):
                    y_copy(matrix, block, number).wait_send()

    by_role(inside, outside)
    for step in range(1, 4):
        norm_copy(step, t).wait_send()
    for way in range(7):
        for s in range(4):
            row_copy(way, s, t, {"tp": partner}).wait_send()
    for k in range(8):
        core_copy(k).wait_send()
        for way in range(3):
            line_copy(k, way).wait_send()


ANYWHERE = pl.BlockSpec(memory_space=pl.ANY)
INSIDE = pl.BlockSpec(memory_space=pltpu.VMEM)


def tables(heads):
    places = np.arange(LEN, dtype=np.float64)
    half = DK // 2
    frequency = (THETA ** (-(np.arange(half) / half))).astype(np.float32)
    angle = (places[:, None].astype(np.float32) * frequency).astype(np.float32)
    distance = places[:, None] - places[None, :]
    gamma = 1.0 - 2.0 ** (-5.0 - np.arange(heads, dtype=np.float64))
    powers = gamma[:, None, None] ** np.maximum(distance, 0.0)
    decay = np.where(distance >= 0, powers, 0.0) * DK ** (-0.5)
    wide = angle.astype(np.float64)
    return (
        decay.astype(np.float32),
        np.cos(wide).astype(np.float32),
        np.sin(wide).astype(np.float32),
    )


def layer(stream, gains, mix_w, mix_scales, up_w, up_scales, w_down, scale_down, tp_count):
    group, width = stream.shape
    share = group // tp_count
    depth, heads_width = mix_w[0].shape
    units = w_down.shape[0]
    blocks = width // depth
    narrow, wide = jnp.bfloat16, jnp.float32
    local_heads = heads_width // DK
    decays, cosine, sine = tables(local_heads * tp_count)
    row = lambda vector: vector[None, :]
    most = max(PIECES)
    dma = pltpu.SemaphoreType.DMA
    half_units = units // 2
    cells = 2 * blocks
    part = depth // 2
    scratch = (
        [pltpu.VMEM(w.shape, wide) for w in mix_w]
        + [
            pltpu.VMEM((4 * half_units, depth), wide),
            pltpu.VMEM((4 * half_units, part), wide),
            pltpu.VMEM((2 * group, width), narrow),
            pltpu.VMEM((1, LEN, LEN), wide),
            pltpu.VMEM(cosine.shape, wide),
            pltpu.VMEM(sine.shape, wide),
            *(pltpu.VMEM((1, width), wide) for _ in gains),
            *(pltpu.VMEM((1, heads_width), wide) for _ in mix_scales),
            pltpu.VMEM((1, depth), wide),
            pltpu.VMEM((2 * width, 3 * DK), narrow),
            pltpu.VMEM((cells * units, depth), narrow),
            pltpu.VMEM((cells * units, part), narrow),
            pltpu.VMEM((blocks, 2 * group, depth), narrow),
            pltpu.VMEM((2 * group, 3 * DK), wide),
            pltpu.VMEM((cells, 2 * group, DV), narrow),
            pltpu.VMEM((cells, share, part), wide),
            pltpu.VMEM((share, width), wide),
            pltpu.VMEM((2 * group, width), narrow),
            pltpu.VMEM((2 * group, half_units), narrow),
            pltpu.VMEM((cells, 2, 4, share, part), narrow),
            pltpu.VMEM((cells, 4, share, part), narrow),
            pltpu.VMEM((cells, 3, share, part), narrow),
            pltpu.VMEM((cells, 3, share, part), narrow),
            pltpu.VMEM((cells, share, part), wide),
            pltpu.VMEM((cells, 1, part), wide),
        ]
        + [
            dma((21,)),
            dma((3, 8, most)), dma((3, 4, most)), dma((3, 8, most)),
            dma((3, 4, most)), dma((3, 4, most)),
            dma((5,)), dma((4,)), dma((1,)), dma((1,)), dma((3,)), dma((3,)),
            dma((7, 4)), dma((7, 4)),
            dma((8,)), dma((8,)), dma((8, 3)), dma((8, 3)),
        ]
    )
    return pl.pallas_call(
        layer_kernel,
        out_shape=pltpu.VMEM((share, width), narrow),
        in_specs=[ANYWHERE] * 15 + [INSIDE] * 2 + [ANYWHERE],
        out_specs=INSIDE,
        scratch_shapes=scratch,
        compiler_params=pltpu.CompilerParams(
            collective_id=0, has_side_effects=True, vmem_limit_bytes=56 * 2**20
        ),
    )(
        stream, *mix_w, *up_w, w_down, decays, cosine, sine, *(row(gain) for gain in gains),
        *(row(scale) for scale in mix_scales), *up_scales, row(scale_down),
    )


def summed_over_tp(partial_sum, share):
    partial_sum = partial_sum.reshape(-1, share, partial_sum.shape[1])
    pieces = lax.all_to_all(partial_sum, "tp", split_axis=0, concat_axis=0)
    return jnp.sum(pieces.astype(jnp.float32), axis=0)


def shards(
    stream,
    gain_mix,
    w_query,
    scale_query,
    w_key,
    scale_key,
    w_value,
    scale_value,
    gain_ffn,
    w_gate,
    scale_gate,
    w_up,
    scale_up,
    w_down,
    scale_down,
):
    group_rows = stream.shape[0]
    tp_count = lax.axis_size("tp")
    if (lax.axis_size("rep"), lax.axis_size("fs"), tp_count) == (2, 4, 4):
        return layer(
            stream, (gain_mix, gain_ffn), (w_query, w_key, w_value),
            (scale_query, scale_key, scale_value), (w_gate.T, w_up.T), (scale_gate, scale_up),
            w_down.T, scale_down, tp_count,
        )
    stream_f = stream.astype(jnp.float32)
    normed = (stream_f * rms_scale(stream_f) * gain_mix).astype(jnp.bfloat16)
    mix_w = jnp.concatenate([w.astype(jnp.bfloat16) for w in (w_query, w_key, w_value)], axis=1)
    up_w = jnp.concatenate([w.astype(jnp.bfloat16) for w in (w_gate, w_up)], axis=1)
    down_w = w_down.astype(jnp.bfloat16)
    down_scale = lax.all_gather(scale_down, "fs", axis=0, tiled=True)
    mix_acc = dot(normed, lax.all_gather(mix_w, "fs", axis=0, tiled=True))
    mix_scale = jnp.concatenate([scale_query, scale_key, scale_value])
    query, key, value = jnp.split(
        (mix_acc * mix_scale).astype(jnp.bfloat16),
        [w_query.shape[1], w_query.shape[1] + w_key.shape[1]],
        axis=1,
    )
    local_heads = query.shape[1] // DK
    positions = jnp.arange(group_rows, dtype=jnp.int32) % LEN
    mixed = []
    for head in range(local_heads):
        columns = slice(head * DK, (head + 1) * DK)
        queries = rotate(query[:, columns].astype(jnp.float32), positions)
        keys = rotate(key[:, columns].astype(jnp.float32), positions) * DK ** (-0.5)
        values = value[:, head * DV : (head + 1) * DV].astype(jnp.float32)
        head_id = (lax.axis_index("tp") * local_heads + head).astype(jnp.float32)
        log_decay = jnp.log(1.0 - jnp.power(2.0, -5.0 - head_id))
        retained = retention(queries, keys, values, log_decay)
        mixed.append((retained * head_scale(retained)).astype(jnp.bfloat16))
    mixed = jnp.concatenate(mixed, axis=1)
    share = group_rows // tp_count
    own_rows = lax.dynamic_slice_in_dim(stream, lax.axis_index("tp") * share, share, 0)
    arrived = lax.all_to_all(mixed, "tp", split_axis=0, concat_axis=1, tiled=True)
    resid = own_rows.astype(jnp.float32) + arrived.astype(jnp.float32)
    normed_ffn = (resid * rms_scale(resid) * gain_ffn).astype(jnp.bfloat16)
    piece = lax.all_gather(normed_ffn, "tp", axis=0, tiled=True)
    up_acc = dot(piece, lax.all_gather(up_w, "fs", axis=0, tiled=True))
    units = w_gate.shape[1]
    gate = up_acc[:, :units] * scale_gate
    upward = up_acc[:, units:] * scale_up
    hidden = (jax.nn.silu(gate) * upward).astype(jnp.bfloat16)
    whole = dot_t(hidden, lax.all_gather(down_w, "fs", axis=0, tiled=True))
    channel_out = summed_over_tp((whole * down_scale).astype(jnp.bfloat16), share)
    return (resid + channel_out).astype(jnp.bfloat16)


def solution(mesh):
    placed = (
        P(("rep", "fs"), None),
        P(),
        P("fs", "tp"),
        P("tp"),
        P("fs", "tp"),
        P("tp"),
        P("fs", "tp"),
        P("tp"),
        P(),
        P("fs", "tp"),
        P("tp"),
        P("fs", "tp"),
        P("tp"),
        P("fs", "tp"),
        P("fs"),
    )
    return jax.shard_map(
        shards, mesh=mesh, in_specs=placed, out_specs=P(("rep", "fs", "tp"), None), check_vma=False
    )
```

```python
import numpy as np
import jax
import jax.numpy as jnp
from jax import lax
from jax.experimental import pallas as pl
from jax.experimental.pallas import tpu as pltpu
from jax.sharding import PartitionSpec as P

DK = 256
DV = 256
LEN = 128


EPS = 1e-06
THETA = 10000.0
HIGH = lax.Precision.HIGHEST


def rms_scale(values):
    return lax.rsqrt(jnp.mean(values * values, axis=-1, keepdims=True) + EPS)


def head_scale(values):
    return 1.0 / jnp.maximum(jnp.sqrt(jnp.mean(values * values, axis=-1, keepdims=True)), 1.0)


def rotate(heads_data, positions):
    half = heads_data.shape[-1] // 2
    frequency = THETA ** (-(jnp.arange(half, dtype=jnp.float32) / half))
    angle = positions.astype(jnp.float32)[:, None] * frequency
    cosine = jnp.cos(angle)
    sine = jnp.sin(angle)
    first = heads_data[..., :half]
    second = heads_data[..., half:]
    return jnp.concatenate(
        [first * cosine - second * sine, second * cosine + first * sine], axis=-1
    )


def retention(queries, keys, values, log_decay):
    offsets = jnp.arange(LEN, dtype=jnp.float32)
    distance = offsets[:, None] - offsets[None, :]
    decay = jnp.where(distance >= 0, jnp.exp(log_decay * jnp.maximum(distance, 0.0)), 0.0)
    queries, keys, values = (
        part.reshape(-1, LEN, part.shape[-1]) for part in (queries, keys, values)
    )
    scores = jnp.einsum("sid,sjd->sij", queries, keys, precision=HIGH) * decay
    retained = jnp.einsum("sij,sje->sie", scores, values, precision=HIGH)
    return retained.reshape(-1, values.shape[-1])


def dot(left, right):
    return jnp.dot(left, right, preferred_element_type=jnp.float32)


def dot_t(left, right):
    return lax.dot_general(left, right, (((1,), (1,)), ((), ())), preferred_element_type=jnp.float32)


MESH = pl.DeviceIdType.MESH
PIECES = (8, 4, 4)


def signal(peer):
    barrier = pltpu.get_barrier_semaphore()
    pl.semaphore_signal(barrier, inc=1, device_id=peer, device_id_type=MESH)


def remote(source, target, send, recv, device):
    return pltpu.make_async_remote_copy(
        src_ref=source,
        dst_ref=target,
        send_sem=send,
        recv_sem=recv,
        device_id=device,
        device_id_type=MESH,
    )


def span(index, size):
    return pl.ds(pl.multiple_of(index * size, size), size)


def layer_kernel(
    stream, w_query, w_key, w_value, w_gate, w_up, w_down, decays,
    cosine_in, sine_in, gain_mix_in, gain_ffn_in, scale_query_in, scale_key_in, scale_value_in,
    scale_gate_in, scale_up_in, scale_down_in,
    out,
    f_query, f_key, f_value, f_up, f_down, rows, decay,
    cosine, sine, gain_mix, gain_ffn, scale_query, scale_key, scale_value, scale_down,
    scale_gate, scale_up,
    mix_w, up_w, down_w, normed, mix_acc, mixed, resid, row_sum, normed_ffn,
    hidden, partial, from_core, paired, from_line, final, down_scale,
    local, cross_send, inward_send, z_recv, y_send, y_recv, scale_send, scale_recv,
    token_send, token_recv, norm_send, norm_recv, row_send, row_recv,
    core_send, core_recv, line_send, line_recv,
):
    z, y, t = lax.axis_index("fs"), lax.axis_index("rep"), lax.axis_index("tp")
    group, width = stream.shape
    share = group // 4
    depth = w_query.shape[0]
    units = w_gate.shape[0] // 2
    part_width = depth // 2
    heights = (depth, 2 * units, 2 * units)
    inner = (z == 1) | (z == 2)
    mine = jnp.where(inner, 1, 0)
    pair_z = z + 1 - 2 * lax.rem(z, 2)
    outer_z, inner_z = jnp.where(inner, pair_z, z), jnp.where(inner, z, pair_z)
    near, far = 3 - inner_z, 3 - outer_z
    core, x = lax.rem(t, 2), t // 2
    partner = t + 1 - 2 * core
    twin = lax.rem(t + 2, 4)
    diagonal = lax.rem(partner + 2, 4)

    for step in range(4):
        for apart in range(2):
            if step or apart:
                signal({"fs": pair_z if apart else z, "tp": lax.rem(t + step, 4)})
    signal({"rep": 1 - y})

    @pl.when(inner)
    def _():
        signal({"fs": near})

    moves = [(w_query, f_query), (w_key, f_key), (w_value, f_value)]
    moves.append((stream, rows.at[span(mine, group)]))
    for part in range(2):
        for place, matrix in enumerate((w_gate, w_up)):
            moves.append((
                matrix.at[pl.ds(part * units, units)],
                f_up.at[pl.ds((2 * part + place) * units, units)],
            ))
    for part in range(2):
        for half in range(2):
            moves.append((
                w_down.at[pl.ds(part * units, units), pl.ds(half * part_width, part_width)],
                f_down.at[pl.ds((2 * part + half) * units, units)],
            ))
    moves.append((decays.at[pl.ds(2 * t + mine, 1)], decay))
    moves += [
        (cosine_in, cosine), (sine_in, sine), (gain_mix_in, gain_mix), (gain_ffn_in, gain_ffn),
        (scale_query_in, scale_query), (scale_key_in, scale_key), (scale_value_in, scale_value),
        (scale_down_in, scale_down), (scale_gate_in, scale_gate), (scale_up_in, scale_up),
    ]
    loads = [
        pltpu.make_async_copy(source, target, local.at[index])
        for index, (source, target) in enumerate(moves)
    ]
    for load in loads:
        load.start()

    weights = (mix_w, up_w, down_w)

    def place_of(matrix, block, number):
        height = heights[matrix]
        piece = height // PIECES[matrix]
        return pl.ds(pl.multiple_of(block * height + number * piece, piece), piece)

    def numbers(matrix, half):
        count = PIECES[matrix] // 2
        return [count * half + step for step in range(count)]

    def cast(matrix, part, half):
        for number in numbers(matrix, half):
            there = place_of(matrix, part * 4 + z, number)
            if matrix == 0:
                here = place_of(0, 0, number)
                for place, full in enumerate((f_query, f_key, f_value)):
                    columns = slice(place * DK, (place + 1) * DK)
                    source = full[here, part * DK : (part + 1) * DK]
                    mix_w[there, columns] = source.astype(jnp.bfloat16)
            else:
                full = f_up if matrix == 1 else f_down
                source = full[place_of(matrix, part, number), :]
                weights[matrix][there, :] = source.astype(jnp.bfloat16)

    def z_copy(matrix, part, block, number, target, inward=False):
        cell = part * 4 + block
        view = weights[matrix].at[place_of(matrix, cell, number)]
        if inward:
            send = inward_send.at[matrix, block, number]
        else:
            send = cross_send.at[matrix, cell, number]
        return remote(view, view, send, z_recv.at[matrix, cell, number], {"fs": target})

    def y_copy(matrix, block, number):
        view = weights[matrix].at[place_of(matrix, mine * 4 + block, number)]
        return remote(
            view, view, y_send.at[matrix, block, number], y_recv.at[matrix, block, number],
            {"rep": 1 - y},
        )

    def send_own(matrix, part, half, target, inward=False):
        for number in numbers(matrix, half):
            z_copy(matrix, part, z, number, target, inward).start()

    def own_piece(matrix, part, half, step, target, inward=False):
        z_copy(matrix, part, z, numbers(matrix, half)[step], target, inward).start()

    def scale_pass(slot, block, target):
        scale_copy(1 if block is near else 0 if slot == 2 else 2, block, target).wait_recv()
        scale_copy(slot, block, target).start()

    def tokens_on():
        token_copy(1 - mine).wait_recv()
        for step in range(1, 4):
            norm_copy(step, t).start()

    def pair_rows():
        for step in range(1, 4):
            norm_copy(step, lax.rem(t + 4 - step, 4)).wait_recv()
        for number in range(4):
            norm_rows(1 - mine, number)

    def cross_last():
        z_copy(2, 1, outer_z, numbers(2, 1 - y)[1], near).start()

    def take_last():
        z_copy(2, 1, far, numbers(2, y)[1], pair_z).wait_recv()

    def wait_last():
        y_copy(2, far, numbers(2, 1 - y)[0]).wait_recv()
        z_copy(2, 1, far, numbers(2, 1 - y)[1], pair_z).wait_recv()

    def scales_in():
        for block in (inner_z, near, far):
            scale_copy(0, block, outer_z).wait_recv()

    def wait_y(matrix, block):
        for number in numbers(matrix, 1 - y):
            y_copy(matrix, block, number).wait_recv()

    def cross(matrix, part, step):
        number = numbers(matrix, y)[step]
        z_copy(matrix, part, outer_z, number, near).wait_recv()
        z_copy(matrix, part, outer_z, number, near).start()

    def inwards(matrix, block, step):
        number = numbers(matrix, y)[step]
        z_copy(matrix, 0, block, number, outer_z, True).wait_recv()
        z_copy(matrix, 0, block, number, outer_z, True).start()

    def swap(matrix, block, step):
        number = numbers(matrix, y)[step]
        z_copy(matrix, mine, block, number, pair_z).wait_recv()
        y_copy(matrix, block, number).start()

    def swap_all(matrix, block):
        for step in range(PIECES[matrix] // 2):
            swap(matrix, block, step)

    def wait_pair(matrix):
        for number in numbers(matrix, 1 - y):
            z_copy(matrix, 1, outer_z, number, near).wait_recv()

    def by_role(inside, outside):
        pl.when(inner)(inside)
        pl.when(jnp.logical_not(inner))(outside)

    def norm_rows(side, number):
        here = span(side * 4 + number, share)
        values = rows[here, :].astype(jnp.float32)
        factor = lax.rsqrt(jnp.mean(values * values, axis=1, keepdims=True) + EPS)
        values = (values * factor * gain_mix[...]).astype(jnp.bfloat16)
        for block in range(4):
            normed[block, here, :] = values[:, block * depth : (block + 1) * depth]

    def token_copy(side):
        part = rows.at[span(side * 4 + t, share)]
        return remote(part, part, token_send.at[0], token_recv.at[0], {"fs": pair_z})

    def norm_copy(step, owner):
        part = rows.at[span((1 - mine) * 4 + owner, share)]
        peer = lax.rem(t + step, 4)
        return remote(part, part, norm_send.at[step - 1], norm_recv.at[step - 1], {"tp": peer})

    def scale_copy(slot, block, target):
        cells = down_scale.at[pl.ds(2 * block, 2)]
        return remote(cells, cells, scale_send.at[slot], scale_recv.at[block], {"fs": target})

    def project(block, first):
        product = dot(normed[block], mix_w[span(mine * 4 + block, depth), :])
        if first:
            mix_acc[...] = product
        else:
            mix_acc[...] += product

    lanes = pl.ds(pl.multiple_of(mine * DK, DK), DK)

    def retain(s):
        here = slice(s * LEN, (s + 1) * LEN)
        cos, sin = cosine[...], sine[...]

        def turned(offset, scale):
            values = mix_acc[here, offset : offset + DK] * scale
            values = values.astype(jnp.bfloat16).astype(jnp.float32)
            first, second = values[:, : DK // 2], values[:, DK // 2 :]
            return jnp.concatenate(
                [first * cos - second * sin, second * cos + first * sin], axis=1
            ).astype(jnp.bfloat16)

        queries = turned(0, scale_query[:, lanes])
        keys = turned(DK, scale_key[:, lanes])
        values = (mix_acc[here, 2 * DK :] * scale_value[:, lanes]).astype(jnp.bfloat16)
        scores = (dot_t(queries, keys) * decay[0]).astype(jnp.bfloat16)
        retained = dot(scores, values)
        mixed[2 * t + mine, here, :] = (retained * head_scale(retained)).astype(jnp.bfloat16)
        own = 2 * t + mine
        row_copy(1, s, own, {"tp": twin}).start()
        row_copy(2, s, own, {"fs": pair_z}).start()
        row_copy(0, s, own, {"tp": partner}).start()

    def row_copy(way, s, cell, target):
        part = mixed.at[cell, pl.ds(s * LEN, LEN)]
        return remote(part, part, row_send.at[way, s], row_recv.at[way, s], target)

    def row_wait(way, s):
        cell = (
            2 * partner + mine, 2 * twin + mine, 2 * t + 1 - mine, 2 * twin + 1 - mine,
            2 * diagonal + mine, 2 * partner + 1 - mine, 2 * diagonal + 1 - mine,
        )[way]
        row_copy(way, s, cell, {"tp": partner}).wait_recv()

    def row_line(s):
        cell = 2 * twin + mine
        row_wait(1, s)
        pl.when(core == 0)(row_copy(3, s, cell, {"fs": pair_z}).start)
        row_copy(4, s, cell, {"tp": partner}).start()

    def row_depth(s):
        cell = 2 * t + 1 - mine
        row_wait(2, s)
        pl.when(core == 1)(row_copy(3, s, cell, {"tp": twin}).start)
        row_copy(5, s, cell, {"tp": partner}).start()

    def row_last(s):
        row_wait(3, s)
        row_copy(6, s, 2 * twin + 1 - mine, {"tp": partner}).start()

    def norm_ffn(s):
        for way in (0, 4, 5, 6):
            row_wait(way, s)
        for first in range(s * LEN, (s + 1) * LEN, share):
            here = slice(first, first + share)
            squares = 0.0
            for cell in range(8):
                columns = slice(cell * part_width, (cell + 1) * part_width)
                values = rows[here, columns].astype(jnp.float32)
                values += mixed[cell, here, :].astype(jnp.float32)
                row_sum[:, columns] = values
                squares += jnp.sum(values * values, axis=1, keepdims=True)
            factor = lax.rsqrt(squares / width + EPS)
            for cell in range(8):
                columns = slice(cell * part_width, (cell + 1) * part_width)
                normed_ffn[here, columns] = (
                    row_sum[:, columns] * factor * gain_ffn[:, columns]
                ).astype(jnp.bfloat16)

    def own_resid():
        here = span(mine * 4 + t, share)
        for cell in range(8):
            columns = slice(cell * part_width, (cell + 1) * part_width)
            values = rows[here, columns].astype(jnp.float32)
            resid[cell] = values + mixed[cell, here, :].astype(jnp.float32)

    def chosen(scale):
        full = scale[...][None, :]
        return jnp.where(inner, full[:, units:], full[:, :units])

    def hidden_rows(side):
        here = slice(side * group, (side + 1) * group)

        def projected(place):
            total = 0.0
            for block in range(4):
                left = normed_ffn[here, block * depth : (block + 1) * depth]
                part = span((mine * 4 + block) * 2 + place, units)
                total += dot_t(left, up_w[part, :])
            return total

        gate = projected(0) * chosen(scale_gate)
        upward = projected(1) * chosen(scale_up)
        hidden[here, :] = (gate / (1.0 + jnp.exp(-gate)) * upward).astype(jnp.bfloat16)

    def core_copy(k):
        return remote(
            partial.at[k, 1 - core], from_core.at[k], core_send.at[k], core_recv.at[k],
            {"tp": partner},
        )

    line_targets = (
        ({"fs": pair_z, "tp": twin}, (1 - mine) * 2 + 1 - x),
        ({"tp": twin}, mine * 2 + 1 - x),
        ({"fs": pair_z}, (1 - mine) * 2 + x),
    )

    def line_copy(k, way):
        return remote(
            paired.at[k, way], from_line.at[k, way], line_send.at[k, way], line_recv.at[k, way],
            line_targets[way][0],
        )

    def down(k, cell):
        products = dot(hidden[...], down_w[span(mine * 8 + cell, units), :])
        products = (products * down_scale[cell]).astype(jnp.bfloat16)
        for owner in range(8):
            partial[k, owner % 2, owner // 2] = products[owner * share : (owner + 1) * share]
        core_copy(k).start()

    def both(k, chip):
        return partial[k, core, chip].astype(jnp.float32) + from_core[k, chip].astype(jnp.float32)

    def pair(k):
        core_copy(k).wait_recv()
        for way in range(3):
            paired[k, way] = both(k, line_targets[way][1]).astype(jnp.bfloat16)
            line_copy(k, way).start()

    def finish(k, cell):
        total = both(k, mine * 2 + x)
        for way in (1, 2, 0):
            line_copy(k, way).wait_recv()
            total += from_line[k, way].astype(jnp.float32)
        final[cell] = resid[cell] + total

    for load in loads[:3]:
        load.wait()
    cast(0, 0, y)
    pl.semaphore_wait(pltpu.get_barrier_semaphore(), jnp.where(inner, 9, 8))

    def inside():
        send_own(0, 0, y, near)
        send_own(0, 0, y, outer_z, True)

    def outside():
        send_own(0, 0, y, inner_z)

    by_role(inside, outside)
    loads[3].wait()
    token_copy(mine).start()
    cast(0, 1, y)

    def outside():
        send_own(0, 1, y, inner_z)
        cast(0, 0, 1 - y)

    pl.when(jnp.logical_not(inner))(outside)
    cast(0, 1, 1 - y)
    for load in loads[4:]:
        load.wait()
    for half in range(2):
        down_scale[z * 2 + half] = scale_down[:, half * part_width : (half + 1) * part_width]
    scale_copy(0, z, pair_z).start()

    def inside():
        scale_copy(1, z, near).start()

    pl.when(inner)(inside)
    for matrix in (1, 2):
        for part in range(2):
            for half in range(2):
                cast(matrix, part, half)
    for number in range(4):
        norm_rows(mine, number)
    cells = (
        outer_z * 2 + y, inner_z * 2 + y, inner_z * 2 + 1 - y, outer_z * 2 + 1 - y,
        near * 2 + y, near * 2 + 1 - y,
        far * 2 + y, far * 2 + 1 - y,
    )

    def inside():
        own_piece(0, 1, y, 0, near)
        own_piece(0, 1, y, 1, near)
        own_piece(1, 0, y, 0, outer_z, True)
        own_piece(0, 1, y, 2, near)
        inwards(0, near, 0)
        cross(0, 0, 0)
        inwards(0, near, 1)
        cross(0, 0, 1)
        inwards(0, near, 2)
        cross(0, 0, 2)
        inwards(0, near, 3)
        scale_pass(3, near, outer_z)
        cross(0, 0, 3)
        swap(0, near, 0)
        own_piece(0, 1, y, 3, near)
        own_piece(1, 0, y, 1, outer_z, True)
        swap(0, near, 1)
        own_piece(1, 0, y, 0, near)
        tokens_on()
        swap(0, near, 2)
        cross(0, 1, 0)
        inwards(0, far, 0)
        cross(0, 1, 1)
        inwards(0, far, 1)
        cross(0, 1, 2)
        inwards(0, far, 2)

    def outside():
        swap(0, inner_z, 0)
        swap(0, inner_z, 1)
        swap(0, inner_z, 2)
        own_piece(1, 0, y, 0, inner_z)
        swap(0, inner_z, 3)
        own_piece(1, 0, y, 1, inner_z)
        wait_y(0, inner_z)
        tokens_on()
        own_piece(1, 1, y, 0, inner_z)
        swap(1, inner_z, 0)
        own_piece(1, 1, y, 1, inner_z)
        swap(0, near, 0)
        swap(0, near, 1)

    by_role(inside, outside)
    pair_rows()

    def inside():
        scale_pass(2, outer_z, near)
        inwards(0, far, 3)
        cross(0, 1, 3)

    pl.when(inner)(inside)
    project(z, True)

    def inside():
        own_piece(1, 0, y, 1, near)
        swap(0, near, 3)
        cross(1, 0, 0)
        inwards(1, near, 0)
        wait_y(0, near)
        swap(0, far, 0)
        cross(1, 0, 1)
        swap(0, far, 1)
        swap(0, far, 2)
        scale_pass(4, far, outer_z)
        own_piece(1, 1, y, 0, near)
        own_piece(2, 0, y, 0, outer_z, True)
        swap(0, far, 3)
        own_piece(2, 0, y, 1, outer_z, True)
        own_piece(1, 1, y, 1, near)
        inwards(1, near, 1)
        wait_y(0, far)
        cross(1, 1, 0)
        inwards(1, far, 0)
        cross(1, 1, 1)
        inwards(1, far, 1)
        wait_pair(0)

    def outside():
        swap(0, near, 2)

    by_role(inside, outside)
    project(pair_z, False)

    def outside():
        swap(0, near, 3)
        own_piece(2, 0, y, 0, inner_z)
        swap(1, inner_z, 1)
        own_piece(2, 0, y, 1, inner_z)
        swap(0, far, 0)
        wait_y(0, near)

    pl.when(jnp.logical_not(inner))(outside)
    project(near, False)

    def outside():
        swap(0, far, 1)
        swap(0, far, 2)
        wait_y(1, inner_z)
        own_piece(0, 1, 1 - y, 0, inner_z)
        swap(0, far, 3)
        own_piece(0, 1, 1 - y, 1, inner_z)
        own_piece(0, 1, 1 - y, 2, inner_z)
        swap(1, near, 0)
        scales_in()
        own_piece(0, 1, 1 - y, 3, inner_z)
        swap(2, inner_z, 0)
        wait_y(0, far)

    pl.when(jnp.logical_not(inner))(outside)
    project(far, False)

    def inside():
        own_piece(2, 0, y, 0, near)

    def outside():
        own_piece(1, 1, 1 - y, 0, inner_z)

    by_role(inside, outside)
    retain(0)

    def inside():
        swap(1, near, 0)

    def outside():
        swap(2, inner_z, 1)

    by_role(inside, outside)
    retain(1)

    def inside():
        own_piece(2, 0, y, 1, near)

    pl.when(inner)(inside)
    retain(2)
    retain(3)

    def inside():
        row_depth(0)
        cross(2, 0, 0)
        row_depth(1)
        swap(1, near, 1)
        row_line(0)
        cross(2, 0, 1)
        row_depth(2)
        row_line(1)
        row_depth(3)
        own_piece(2, 1, y, 0, near)
        row_line(2)
        swap(1, far, 0)
        row_last(0)

    def outside():
        swap(1, near, 1)
        row_line(0)
        row_line(1)
        wait_y(2, inner_z)
        row_line(2)
        swap(1, far, 0)
        row_line(3)
        wait_y(1, near)
        swap(1, far, 1)
        row_depth(0)
        own_piece(1, 1, 1 - y, 1, inner_z)
        row_depth(1)
        row_depth(2)
        row_depth(3)
        own_piece(2, 1, y, 0, inner_z)
        wait_y(1, far)
        row_last(0)

    by_role(inside, outside)
    norm_ffn(0)

    def inside():
        own_piece(2, 1, y, 1, near)
        row_line(3)
        row_last(1)

    def outside():
        own_piece(2, 1, y, 1, inner_z)
        row_last(1)

    by_role(inside, outside)
    norm_ffn(1)

    def inside():
        row_last(2)

    def outside():
        row_last(2)

    by_role(inside, outside)
    norm_ffn(2)

    def inside():
        wait_y(1, near)
        swap(1, far, 1)
        row_last(3)
        inwards(2, near, 0)

    def outside():
        own_piece(2, 1, 1 - y, 0, inner_z)
        row_last(3)

    by_role(inside, outside)
    norm_ffn(3)
    own_resid()

    def inside():
        inwards(2, near, 1)
        wait_pair(1)
        inwards(2, far, 0)
        cross(2, 1, 0)
        wait_y(1, far)

    def outside():
        own_piece(2, 1, 1 - y, 1, inner_z)

    by_role(inside, outside)
    hidden_rows(0)

    def inside():
        inwards(2, far, 1)
        cross(2, 1, 1)

    def outside():
        swap(2, near, 0)

    by_role(inside, outside)
    hidden_rows(1)

    def inside():
        swap(2, near, 0)

    def outside():
        swap(2, near, 1)

    by_role(inside, outside)
    down(0, cells[0])
    down(1, cells[1])

    def outside():
        swap(2, far, 0)

    pl.when(jnp.logical_not(inner))(outside)
    pair(0)

    def inside():
        swap(2, near, 1)

    pl.when(inner)(inside)
    down(2, cells[2])
    pair(1)

    def inside():
        wait_pair(2)
        cross_last()

    pl.when(inner)(inside)
    down(3, cells[3])

    def inside():
        swap(2, far, 0)

    pl.when(inner)(inside)
    pair(2)

    def outside():
        swap(2, far, 1)

    pl.when(jnp.logical_not(inner))(outside)
    pair(3)
    down(4, cells[4])

    def inside():
        take_last()

    def outside():
        wait_y(2, near)

    by_role(inside, outside)
    pair(4)
    finish(0, cells[0])

    def inside():
        wait_y(2, near)

    pl.when(inner)(inside)
    down(5, cells[5])
    pair(5)

    def outside():
        wait_y(2, far)

    pl.when(jnp.logical_not(inner))(outside)
    finish(1, cells[1])
    down(6, cells[6])

    def inside():
        wait_last()

    pl.when(inner)(inside)
    pair(6)
    finish(2, cells[2])
    down(7, cells[7])
    pair(7)
    finish(3, cells[3])
    finish(4, cells[4])
    finish(5, cells[5])
    finish(6, cells[6])
    finish(7, cells[7])
    for cell in range(8):
        out[:, cell * part_width : (cell + 1) * part_width] = final[cell].astype(jnp.bfloat16)

    token_copy(mine).wait_send()
    scale_copy(0, z, pair_z).wait_send()

    def inside():
        scale_copy(1, z, near).wait_send()
        scale_copy(2, outer_z, near).wait_send()
        scale_copy(3, near, outer_z).wait_send()
        scale_copy(4, far, outer_z).wait_send()
        for matrix in range(3):
            for number in numbers(matrix, y):
                for part in range(2):
                    z_copy(matrix, part, z, number, near).wait_send()
                    z_copy(matrix, part, outer_z, number, near).wait_send()
                for block in (z, near, far):
                    z_copy(matrix, 0, block, number, outer_z, True).wait_send()
                y_copy(matrix, near, number).wait_send()
            for number in numbers(matrix, y)[: -1 if matrix == 2 else None]:
                y_copy(matrix, far, number).wait_send()
        z_copy(2, 1, outer_z, numbers(2, 1 - y)[1], near).wait_send()

    def outside():
        for matrix in range(3):
            for part, half in ((0, y), (1, y), (1, 1 - y)):
                for number in numbers(matrix, half):
                    z_copy(matrix, part, z, number, inner_z).wait_send()
            for number in numbers(matrix, y):
                for block in (inner_z, near, far):
                    y_copy(matrix, block, number).wait_send()

    by_role(inside, outside)
    for step in range(1, 4):
        norm_copy(step, t).wait_send()
    for way in range(7):
        for s in range(4):
            row_copy(way, s, t, {"tp": partner}).wait_send()
    for k in range(8):
        core_copy(k).wait_send()
        for way in range(3):
            line_copy(k, way).wait_send()


ANYWHERE = pl.BlockSpec(memory_space=pl.ANY)
INSIDE = pl.BlockSpec(memory_space=pltpu.VMEM)


def tables(heads):
    places = np.arange(LEN, dtype=np.float64)
    half = DK // 2
    frequency = (THETA ** (-(np.arange(half) / half))).astype(np.float32)
    angle = (places[:, None].astype(np.float32) * frequency).astype(np.float32)
    distance = places[:, None] - places[None, :]
    gamma = 1.0 - 2.0 ** (-5.0 - np.arange(heads, dtype=np.float64))
    powers = gamma[:, None, None] ** np.maximum(distance, 0.0)
    decay = np.where(distance >= 0, powers, 0.0) * DK ** (-0.5)
    wide = angle.astype(np.float64)
    return (
        decay.astype(np.float32),
        np.cos(wide).astype(np.float32),
        np.sin(wide).astype(np.float32),
    )


def layer(stream, gains, mix_w, mix_scales, up_w, up_scales, w_down, scale_down, tp_count):
    group, width = stream.shape
    share = group // tp_count
    depth, heads_width = mix_w[0].shape
    units = w_down.shape[0]
    blocks = width // depth
    narrow, wide = jnp.bfloat16, jnp.float32
    local_heads = heads_width // DK
    decays, cosine, sine = tables(local_heads * tp_count)
    row = lambda vector: vector[None, :]
    most = max(PIECES)
    dma = pltpu.SemaphoreType.DMA
    half_units = units // 2
    cells = 2 * blocks
    part = depth // 2
    scratch = (
        [pltpu.VMEM(w.shape, wide) for w in mix_w]
        + [
            pltpu.VMEM((4 * half_units, depth), wide),
            pltpu.VMEM((4 * half_units, part), wide),
            pltpu.VMEM((2 * group, width), narrow),
            pltpu.VMEM((1, LEN, LEN), wide),
            pltpu.VMEM(cosine.shape, wide),
            pltpu.VMEM(sine.shape, wide),
            *(pltpu.VMEM((1, width), wide) for _ in gains),
            *(pltpu.VMEM((1, heads_width), wide) for _ in mix_scales),
            pltpu.VMEM((1, depth), wide),
            *(pltpu.VMEM(scale.shape, wide) for scale in up_scales),
            pltpu.VMEM((2 * width, 3 * DK), narrow),
            pltpu.VMEM((cells * units, depth), narrow),
            pltpu.VMEM((cells * units, part), narrow),
            pltpu.VMEM((blocks, 2 * group, depth), narrow),
            pltpu.VMEM((2 * group, 3 * DK), wide),
            pltpu.VMEM((cells, 2 * group, DV), narrow),
            pltpu.VMEM((cells, share, part), wide),
            pltpu.VMEM((share, width), wide),
            pltpu.VMEM((2 * group, width), narrow),
            pltpu.VMEM((2 * group, half_units), narrow),
            pltpu.VMEM((cells, 2, 4, share, part), narrow),
            pltpu.VMEM((cells, 4, share, part), narrow),
            pltpu.VMEM((cells, 3, share, part), narrow),
            pltpu.VMEM((cells, 3, share, part), narrow),
            pltpu.VMEM((cells, share, part), wide),
            pltpu.VMEM((cells, 1, part), wide),
        ]
        + [
            dma((23,)),
            dma((3, 8, most)), dma((3, 4, most)), dma((3, 8, most)),
            dma((3, 4, most)), dma((3, 4, most)),
            dma((5,)), dma((4,)), dma((1,)), dma((1,)), dma((3,)), dma((3,)),
            dma((7, 4)), dma((7, 4)),
            dma((8,)), dma((8,)), dma((8, 3)), dma((8, 3)),
        ]
    )
    return pl.pallas_call(
        layer_kernel,
        out_shape=pltpu.VMEM((share, width), narrow),
        in_specs=[ANYWHERE] * 18,
        out_specs=INSIDE,
        scratch_shapes=scratch,
        compiler_params=pltpu.CompilerParams(
            collective_id=0, has_side_effects=True, vmem_limit_bytes=56 * 2**20
        ),
    )(
        stream, *mix_w, *up_w, w_down, decays, cosine, sine, *(row(gain) for gain in gains),
        *(row(scale) for scale in mix_scales), *up_scales, row(scale_down),
    )


def summed_over_tp(partial_sum, share):
    partial_sum = partial_sum.reshape(-1, share, partial_sum.shape[1])
    pieces = lax.all_to_all(partial_sum, "tp", split_axis=0, concat_axis=0)
    return jnp.sum(pieces.astype(jnp.float32), axis=0)


def shards(
    stream,
    gain_mix,
    w_query,
    scale_query,
    w_key,
    scale_key,
    w_value,
    scale_value,
    gain_ffn,
    w_gate,
    scale_gate,
    w_up,
    scale_up,
    w_down,
    scale_down,
):
    group_rows = stream.shape[0]
    tp_count = lax.axis_size("tp")
    if (lax.axis_size("rep"), lax.axis_size("fs"), tp_count) == (2, 4, 4):
        return layer(
            stream, (gain_mix, gain_ffn), (w_query, w_key, w_value),
            (scale_query, scale_key, scale_value), (w_gate.T, w_up.T), (scale_gate, scale_up),
            w_down.T, scale_down, tp_count,
        )
    stream_f = stream.astype(jnp.float32)
    normed = (stream_f * rms_scale(stream_f) * gain_mix).astype(jnp.bfloat16)
    mix_w = jnp.concatenate([w.astype(jnp.bfloat16) for w in (w_query, w_key, w_value)], axis=1)
    up_w = jnp.concatenate([w.astype(jnp.bfloat16) for w in (w_gate, w_up)], axis=1)
    down_w = w_down.astype(jnp.bfloat16)
    down_scale = lax.all_gather(scale_down, "fs", axis=0, tiled=True)
    mix_acc = dot(normed, lax.all_gather(mix_w, "fs", axis=0, tiled=True))
    mix_scale = jnp.concatenate([scale_query, scale_key, scale_value])
    query, key, value = jnp.split(
        (mix_acc * mix_scale).astype(jnp.bfloat16),
        [w_query.shape[1], w_query.shape[1] + w_key.shape[1]],
        axis=1,
    )
    local_heads = query.shape[1] // DK
    positions = jnp.arange(group_rows, dtype=jnp.int32) % LEN
    mixed = []
    for head in range(local_heads):
        columns = slice(head * DK, (head + 1) * DK)
        queries = rotate(query[:, columns].astype(jnp.float32), positions)
        keys = rotate(key[:, columns].astype(jnp.float32), positions) * DK ** (-0.5)
        values = value[:, head * DV : (head + 1) * DV].astype(jnp.float32)
        head_id = (lax.axis_index("tp") * local_heads + head).astype(jnp.float32)
        log_decay = jnp.log(1.0 - jnp.power(2.0, -5.0 - head_id))
        retained = retention(queries, keys, values, log_decay)
        mixed.append((retained * head_scale(retained)).astype(jnp.bfloat16))
    mixed = jnp.concatenate(mixed, axis=1)
    share = group_rows // tp_count
    own_rows = lax.dynamic_slice_in_dim(stream, lax.axis_index("tp") * share, share, 0)
    arrived = lax.all_to_all(mixed, "tp", split_axis=0, concat_axis=1, tiled=True)
    resid = own_rows.astype(jnp.float32) + arrived.astype(jnp.float32)
    normed_ffn = (resid * rms_scale(resid) * gain_ffn).astype(jnp.bfloat16)
    piece = lax.all_gather(normed_ffn, "tp", axis=0, tiled=True)
    up_acc = dot(piece, lax.all_gather(up_w, "fs", axis=0, tiled=True))
    units = w_gate.shape[1]
    gate = up_acc[:, :units] * scale_gate
    upward = up_acc[:, units:] * scale_up
    hidden = (jax.nn.silu(gate) * upward).astype(jnp.bfloat16)
    whole = dot_t(hidden, lax.all_gather(down_w, "fs", axis=0, tiled=True))
    channel_out = summed_over_tp((whole * down_scale).astype(jnp.bfloat16), share)
    return (resid + channel_out).astype(jnp.bfloat16)


def solution(mesh):
    placed = (
        P(("rep", "fs"), None),
        P(),
        P("fs", "tp"),
        P("tp"),
        P("fs", "tp"),
        P("tp"),
        P("fs", "tp"),
        P("tp"),
        P(),
        P("fs", "tp"),
        P("tp"),
        P("fs", "tp"),
        P("tp"),
        P("fs", "tp"),
        P("fs"),
    )
    return jax.shard_map(
        shards, mesh=mesh, in_specs=placed, out_specs=P(("rep", "fs", "tp"), None), check_vma=False
    )
```

```python
import numpy as np
import jax
import jax.numpy as jnp
from jax import lax
from jax.experimental import pallas as pl
from jax.experimental.pallas import tpu as pltpu
from jax.sharding import PartitionSpec as P

DK = 256
DV = 256
LEN = 128


EPS = 1e-06
THETA = 10000.0
HIGH = lax.Precision.HIGHEST


def rms_scale(values):
    return lax.rsqrt(jnp.mean(values * values, axis=-1, keepdims=True) + EPS)


def head_scale(values):
    return 1.0 / jnp.maximum(jnp.sqrt(jnp.mean(values * values, axis=-1, keepdims=True)), 1.0)


def rotate(heads_data, positions):
    half = heads_data.shape[-1] // 2
    frequency = THETA ** (-(jnp.arange(half, dtype=jnp.float32) / half))
    angle = positions.astype(jnp.float32)[:, None] * frequency
    cosine = jnp.cos(angle)
    sine = jnp.sin(angle)
    first = heads_data[..., :half]
    second = heads_data[..., half:]
    return jnp.concatenate(
        [first * cosine - second * sine, second * cosine + first * sine], axis=-1
    )


def retention(queries, keys, values, log_decay):
    offsets = jnp.arange(LEN, dtype=jnp.float32)
    distance = offsets[:, None] - offsets[None, :]
    decay = jnp.where(distance >= 0, jnp.exp(log_decay * jnp.maximum(distance, 0.0)), 0.0)
    queries, keys, values = (
        part.reshape(-1, LEN, part.shape[-1]) for part in (queries, keys, values)
    )
    scores = jnp.einsum("sid,sjd->sij", queries, keys, precision=HIGH) * decay
    retained = jnp.einsum("sij,sje->sie", scores, values, precision=HIGH)
    return retained.reshape(-1, values.shape[-1])


def dot(left, right):
    return jnp.dot(left, right, preferred_element_type=jnp.float32)


def dot_t(left, right):
    return lax.dot_general(left, right, (((1,), (1,)), ((), ())), preferred_element_type=jnp.float32)


MESH = pl.DeviceIdType.MESH
PIECES = (8, 4, 4)


def signal(peer):
    barrier = pltpu.get_barrier_semaphore()
    pl.semaphore_signal(barrier, inc=1, device_id=peer, device_id_type=MESH)


def remote(source, target, send, recv, device):
    return pltpu.make_async_remote_copy(
        src_ref=source,
        dst_ref=target,
        send_sem=send,
        recv_sem=recv,
        device_id=device,
        device_id_type=MESH,
    )


def span(index, size):
    return pl.ds(pl.multiple_of(index * size, size), size)


def layer_kernel(
    stream, w_query, w_key, w_value, w_gate, w_up, w_down, decays,
    cosine_in, sine_in, gain_mix_in, gain_ffn_in, scale_query_in, scale_key_in, scale_value_in,
    scale_gate_in, scale_up_in, scale_down_in,
    out,
    f_query, f_key, f_value, f_up, f_down, rows, decay,
    cosine, sine, gain_mix, gain_ffn, scale_query, scale_key, scale_value, scale_down,
    scale_gate, scale_up,
    mix_w, up_w, down_w, normed, mix_acc, mixed, resid, row_sum, normed_ffn,
    hidden, partial, from_core, paired, from_line, final, down_scale,
    local, cross_send, inward_send, z_recv, y_send, y_recv, scale_send, scale_recv,
    token_send, token_recv, norm_send, norm_recv, row_send, row_recv,
    core_send, core_recv, line_send, line_recv,
):
    z, y, t = lax.axis_index("fs"), lax.axis_index("rep"), lax.axis_index("tp")
    group, width = stream.shape
    share = group // 4
    depth = w_query.shape[0]
    units = w_gate.shape[0] // 2
    part_width = depth // 2
    heights = (depth, 2 * units, 2 * units)
    inner = (z == 1) | (z == 2)
    mine = jnp.where(inner, 1, 0)
    pair_z = z + 1 - 2 * lax.rem(z, 2)
    outer_z, inner_z = jnp.where(inner, pair_z, z), jnp.where(inner, z, pair_z)
    near, far = 3 - inner_z, 3 - outer_z
    core, x = lax.rem(t, 2), t // 2
    partner = t + 1 - 2 * core
    twin = lax.rem(t + 2, 4)
    diagonal = lax.rem(partner + 2, 4)

    for step in range(4):
        for apart in range(2):
            if step or apart:
                signal({"fs": pair_z if apart else z, "tp": lax.rem(t + step, 4)})
    signal({"rep": 1 - y})

    @pl.when(inner)
    def _():
        signal({"fs": near})

    pairs = ((w_query, f_query), (w_key, f_key), (w_value, f_value))
    first, last = span(y, depth // 2), span(1 - y, depth // 2)
    moves = [
        (source.at[first, pl.ds(0, DK)], target.at[first, pl.ds(0, DK)]) for source, target in pairs
    ]
    moves.append((stream, rows.at[span(mine, group)]))
    for source, target in pairs:
        moves.append((source.at[first, pl.ds(DK, DK)], target.at[first, pl.ds(DK, DK)]))
        moves.append((source.at[last], target.at[last]))
    for part in range(2):
        for place, matrix in enumerate((w_gate, w_up)):
            moves.append((
                matrix.at[pl.ds(part * units, units)],
                f_up.at[pl.ds((2 * part + place) * units, units)],
            ))
    for part in range(2):
        for half in range(2):
            moves.append((
                w_down.at[pl.ds(part * units, units), pl.ds(half * part_width, part_width)],
                f_down.at[pl.ds((2 * part + half) * units, units)],
            ))
    moves.append((decays.at[pl.ds(2 * t + mine, 1)], decay))
    moves += [
        (cosine_in, cosine), (sine_in, sine), (gain_mix_in, gain_mix), (gain_ffn_in, gain_ffn),
        (scale_query_in, scale_query), (scale_key_in, scale_key), (scale_value_in, scale_value),
        (scale_down_in, scale_down), (scale_gate_in, scale_gate), (scale_up_in, scale_up),
    ]
    loads = [
        pltpu.make_async_copy(source, target, local.at[index])
        for index, (source, target) in enumerate(moves)
    ]
    for load in loads:
        load.start()

    weights = (mix_w, up_w, down_w)

    def place_of(matrix, block, number):
        height = heights[matrix]
        piece = height // PIECES[matrix]
        return pl.ds(pl.multiple_of(block * height + number * piece, piece), piece)

    def numbers(matrix, half):
        count = PIECES[matrix] // 2
        return [count * half + step for step in range(count)]

    def cast(matrix, part, half):
        for number in numbers(matrix, half):
            there = place_of(matrix, part * 4 + z, number)
            if matrix == 0:
                here = place_of(0, 0, number)
                for place, full in enumerate((f_query, f_key, f_value)):
                    columns = slice(place * DK, (place + 1) * DK)
                    source = full[here, part * DK : (part + 1) * DK]
                    mix_w[there, columns] = source.astype(jnp.bfloat16)
            else:
                full = f_up if matrix == 1 else f_down
                source = full[place_of(matrix, part, number), :]
                weights[matrix][there, :] = source.astype(jnp.bfloat16)

    def z_copy(matrix, part, block, number, target, inward=False):
        cell = part * 4 + block
        view = weights[matrix].at[place_of(matrix, cell, number)]
        if inward:
            send = inward_send.at[matrix, block, number]
        else:
            send = cross_send.at[matrix, cell, number]
        return remote(view, view, send, z_recv.at[matrix, cell, number], {"fs": target})

    def y_copy(matrix, block, number):
        view = weights[matrix].at[place_of(matrix, mine * 4 + block, number)]
        return remote(
            view, view, y_send.at[matrix, block, number], y_recv.at[matrix, block, number],
            {"rep": 1 - y},
        )

    def send_own(matrix, part, half, target, inward=False):
        for number in numbers(matrix, half):
            z_copy(matrix, part, z, number, target, inward).start()

    def own_piece(matrix, part, half, step, target, inward=False):
        z_copy(matrix, part, z, numbers(matrix, half)[step], target, inward).start()

    def scale_pass(slot, block, target):
        scale_copy(1 if block is near else 0 if slot == 2 else 2, block, target).wait_recv()
        scale_copy(slot, block, target).start()

    def tokens_on():
        token_copy(1 - mine).wait_recv()
        for step in range(1, 4):
            norm_copy(step, t).start()

    def pair_rows():
        for step in range(1, 4):
            norm_copy(step, lax.rem(t + 4 - step, 4)).wait_recv()
        for number in range(4):
            norm_rows(1 - mine, number)

    def cross_last():
        z_copy(2, 1, outer_z, numbers(2, 1 - y)[1], near).start()

    def take_last():
        z_copy(2, 1, far, numbers(2, y)[1], pair_z).wait_recv()

    def wait_last():
        y_copy(2, far, numbers(2, 1 - y)[0]).wait_recv()
        z_copy(2, 1, far, numbers(2, 1 - y)[1], pair_z).wait_recv()

    def scales_in():
        for block in (inner_z, near, far):
            scale_copy(0, block, outer_z).wait_recv()

    def wait_y(matrix, block):
        for number in numbers(matrix, 1 - y):
            y_copy(matrix, block, number).wait_recv()

    def cross(matrix, part, step):
        number = numbers(matrix, y)[step]
        z_copy(matrix, part, outer_z, number, near).wait_recv()
        z_copy(matrix, part, outer_z, number, near).start()

    def inwards(matrix, block, step):
        number = numbers(matrix, y)[step]
        z_copy(matrix, 0, block, number, outer_z, True).wait_recv()
        z_copy(matrix, 0, block, number, outer_z, True).start()

    def swap(matrix, block, step):
        number = numbers(matrix, y)[step]
        z_copy(matrix, mine, block, number, pair_z).wait_recv()
        y_copy(matrix, block, number).start()

    def swap_all(matrix, block):
        for step in range(PIECES[matrix] // 2):
            swap(matrix, block, step)

    def wait_pair(matrix):
        for number in numbers(matrix, 1 - y):
            z_copy(matrix, 1, outer_z, number, near).wait_recv()

    def by_role(inside, outside):
        pl.when(inner)(inside)
        pl.when(jnp.logical_not(inner))(outside)

    def norm_rows(side, number):
        here = span(side * 4 + number, share)
        values = rows[here, :].astype(jnp.float32)
        factor = lax.rsqrt(jnp.mean(values * values, axis=1, keepdims=True) + EPS)
        values = (values * factor * gain_mix[...]).astype(jnp.bfloat16)
        for block in range(4):
            normed[block, here, :] = values[:, block * depth : (block + 1) * depth]

    def token_copy(side):
        part = rows.at[span(side * 4 + t, share)]
        return remote(part, part, token_send.at[0], token_recv.at[0], {"fs": pair_z})

    def norm_copy(step, owner):
        part = rows.at[span((1 - mine) * 4 + owner, share)]
        peer = lax.rem(t + step, 4)
        return remote(part, part, norm_send.at[step - 1], norm_recv.at[step - 1], {"tp": peer})

    def scale_copy(slot, block, target):
        cells = down_scale.at[pl.ds(2 * block, 2)]
        return remote(cells, cells, scale_send.at[slot], scale_recv.at[block], {"fs": target})

    def project(block, first):
        product = dot(normed[block], mix_w[span(mine * 4 + block, depth), :])
        if first:
            mix_acc[...] = product
        else:
            mix_acc[...] += product

    lanes = pl.ds(pl.multiple_of(mine * DK, DK), DK)

    def retain(s):
        here = slice(s * LEN, (s + 1) * LEN)
        cos, sin = cosine[...], sine[...]

        def turned(offset, scale):
            values = mix_acc[here, offset : offset + DK] * scale
            values = values.astype(jnp.bfloat16).astype(jnp.float32)
            first, second = values[:, : DK // 2], values[:, DK // 2 :]
            return jnp.concatenate(
                [first * cos - second * sin, second * cos + first * sin], axis=1
            ).astype(jnp.bfloat16)

        queries = turned(0, scale_query[:, lanes])
        keys = turned(DK, scale_key[:, lanes])
        values = (mix_acc[here, 2 * DK :] * scale_value[:, lanes]).astype(jnp.bfloat16)
        scores = (dot_t(queries, keys) * decay[0]).astype(jnp.bfloat16)
        retained = dot(scores, values)
        mixed[2 * t + mine, here, :] = (retained * head_scale(retained)).astype(jnp.bfloat16)
        own = 2 * t + mine
        row_copy(1, s, own, {"tp": twin}).start()
        row_copy(2, s, own, {"fs": pair_z}).start()
        row_copy(0, s, own, {"tp": partner}).start()

    def row_copy(way, s, cell, target):
        part = mixed.at[cell, pl.ds(s * LEN, LEN)]
        return remote(part, part, row_send.at[way, s], row_recv.at[way, s], target)

    def row_wait(way, s):
        cell = (
            2 * partner + mine, 2 * twin + mine, 2 * t + 1 - mine, 2 * twin + 1 - mine,
            2 * diagonal + mine, 2 * partner + 1 - mine, 2 * diagonal + 1 - mine,
        )[way]
        row_copy(way, s, cell, {"tp": partner}).wait_recv()

    def row_line(s):
        cell = 2 * twin + mine
        row_wait(1, s)
        pl.when(core == 0)(row_copy(3, s, cell, {"fs": pair_z}).start)
        row_copy(4, s, cell, {"tp": partner}).start()

    def row_depth(s):
        cell = 2 * t + 1 - mine
        row_wait(2, s)
        pl.when(core == 1)(row_copy(3, s, cell, {"tp": twin}).start)
        row_copy(5, s, cell, {"tp": partner}).start()

    def row_last(s):
        row_wait(3, s)
        row_copy(6, s, 2 * twin + 1 - mine, {"tp": partner}).start()

    def norm_ffn(s):
        for way in (0, 4, 5, 6):
            row_wait(way, s)
        for first in range(s * LEN, (s + 1) * LEN, share):
            here = slice(first, first + share)
            squares = 0.0
            for cell in range(8):
                columns = slice(cell * part_width, (cell + 1) * part_width)
                values = rows[here, columns].astype(jnp.float32)
                values += mixed[cell, here, :].astype(jnp.float32)
                row_sum[:, columns] = values
                squares += jnp.sum(values * values, axis=1, keepdims=True)
            factor = lax.rsqrt(squares / width + EPS)
            for cell in range(8):
                columns = slice(cell * part_width, (cell + 1) * part_width)
                normed_ffn[here, columns] = (
                    row_sum[:, columns] * factor * gain_ffn[:, columns]
                ).astype(jnp.bfloat16)

    def own_resid():
        here = span(mine * 4 + t, share)
        for cell in range(8):
            columns = slice(cell * part_width, (cell + 1) * part_width)
            values = rows[here, columns].astype(jnp.float32)
            resid[cell] = values + mixed[cell, here, :].astype(jnp.float32)

    def chosen(scale):
        full = scale[...][None, :]
        return jnp.where(inner, full[:, units:], full[:, :units])

    def hidden_rows(side):
        here = slice(side * group, (side + 1) * group)

        def projected(place):
            total = 0.0
            for block in range(4):
                left = normed_ffn[here, block * depth : (block + 1) * depth]
                part = span((mine * 4 + block) * 2 + place, units)
                total += dot_t(left, up_w[part, :])
            return total

        gate = projected(0) * chosen(scale_gate)
        upward = projected(1) * chosen(scale_up)
        hidden[here, :] = (gate / (1.0 + jnp.exp(-gate)) * upward).astype(jnp.bfloat16)

    def core_copy(k):
        return remote(
            partial.at[k, 1 - core], from_core.at[k], core_send.at[k], core_recv.at[k],
            {"tp": partner},
        )

    line_targets = (
        ({"fs": pair_z, "tp": twin}, (1 - mine) * 2 + 1 - x),
        ({"tp": twin}, mine * 2 + 1 - x),
        ({"fs": pair_z}, (1 - mine) * 2 + x),
    )

    def line_copy(k, way):
        return remote(
            paired.at[k, way], from_line.at[k, way], line_send.at[k, way], line_recv.at[k, way],
            line_targets[way][0],
        )

    def down(k, cell):
        products = dot(hidden[...], down_w[span(mine * 8 + cell, units), :])
        products = (products * down_scale[cell]).astype(jnp.bfloat16)
        for owner in range(8):
            partial[k, owner % 2, owner // 2] = products[owner * share : (owner + 1) * share]
        core_copy(k).start()

    def both(k, chip):
        return partial[k, core, chip].astype(jnp.float32) + from_core[k, chip].astype(jnp.float32)

    def pair(k):
        core_copy(k).wait_recv()
        for way in range(3):
            paired[k, way] = both(k, line_targets[way][1]).astype(jnp.bfloat16)
            line_copy(k, way).start()

    def finish(k, cell):
        total = both(k, mine * 2 + x)
        for way in (1, 2, 0):
            line_copy(k, way).wait_recv()
            total += from_line[k, way].astype(jnp.float32)
        final[cell] = resid[cell] + total

    for load in loads[:3]:
        load.wait()
    cast(0, 0, y)
    pl.semaphore_wait(pltpu.get_barrier_semaphore(), jnp.where(inner, 9, 8))

    def inside():
        send_own(0, 0, y, near)
        send_own(0, 0, y, outer_z, True)

    def outside():
        send_own(0, 0, y, inner_z)

    by_role(inside, outside)
    loads[3].wait()
    token_copy(mine).start()
    for load in loads[4:10]:
        load.wait()
    cast(0, 1, y)

    def outside():
        send_own(0, 1, y, inner_z)
        cast(0, 0, 1 - y)

    pl.when(jnp.logical_not(inner))(outside)
    cast(0, 1, 1 - y)
    for load in loads[10:]:
        load.wait()
    for half in range(2):
        down_scale[z * 2 + half] = scale_down[:, half * part_width : (half + 1) * part_width]
    scale_copy(0, z, pair_z).start()

    def inside():
        scale_copy(1, z, near).start()

    pl.when(inner)(inside)
    for matrix in (1, 2):
        for part in range(2):
            for half in range(2):
                cast(matrix, part, half)
    for number in range(4):
        norm_rows(mine, number)
    cells = (
        outer_z * 2 + y, inner_z * 2 + y, inner_z * 2 + 1 - y, outer_z * 2 + 1 - y,
        near * 2 + y, near * 2 + 1 - y,
        far * 2 + y, far * 2 + 1 - y,
    )

    def inside():
        own_piece(0, 1, y, 0, near)
        own_piece(0, 1, y, 1, near)
        own_piece(1, 0, y, 0, outer_z, True)
        own_piece(0, 1, y, 2, near)
        inwards(0, near, 0)
        cross(0, 0, 0)
        inwards(0, near, 1)
        cross(0, 0, 1)
        inwards(0, near, 2)
        cross(0, 0, 2)
        inwards(0, near, 3)
        scale_pass(3, near, outer_z)
        cross(0, 0, 3)
        swap(0, near, 0)
        own_piece(0, 1, y, 3, near)
        own_piece(1, 0, y, 1, outer_z, True)
        swap(0, near, 1)
        own_piece(1, 0, y, 0, near)
        tokens_on()
        swap(0, near, 2)
        cross(0, 1, 0)
        inwards(0, far, 0)
        cross(0, 1, 1)
        inwards(0, far, 1)
        cross(0, 1, 2)
        inwards(0, far, 2)

    def outside():
        swap(0, inner_z, 0)
        swap(0, inner_z, 1)
        swap(0, inner_z, 2)
        own_piece(1, 0, y, 0, inner_z)
        swap(0, inner_z, 3)
        own_piece(1, 0, y, 1, inner_z)
        wait_y(0, inner_z)
        tokens_on()
        own_piece(1, 1, y, 0, inner_z)
        swap(1, inner_z, 0)
        own_piece(1, 1, y, 1, inner_z)
        swap(0, near, 0)
        swap(0, near, 1)

    by_role(inside, outside)
    pair_rows()

    def inside():
        scale_pass(2, outer_z, near)
        inwards(0, far, 3)
        cross(0, 1, 3)

    pl.when(inner)(inside)
    project(z, True)

    def inside():
        own_piece(1, 0, y, 1, near)
        swap(0, near, 3)
        cross(1, 0, 0)
        inwards(1, near, 0)
        wait_y(0, near)
        swap(0, far, 0)
        cross(1, 0, 1)
        swap(0, far, 1)
        swap(0, far, 2)
        scale_pass(4, far, outer_z)
        own_piece(1, 1, y, 0, near)
        own_piece(2, 0, y, 0, outer_z, True)
        swap(0, far, 3)
        own_piece(2, 0, y, 1, outer_z, True)
        own_piece(1, 1, y, 1, near)
        inwards(1, near, 1)
        wait_y(0, far)
        cross(1, 1, 0)
        inwards(1, far, 0)
        cross(1, 1, 1)
        inwards(1, far, 1)
        wait_pair(0)

    def outside():
        swap(0, near, 2)

    by_role(inside, outside)
    project(pair_z, False)

    def outside():
        swap(0, near, 3)
        own_piece(2, 0, y, 0, inner_z)
        swap(1, inner_z, 1)
        own_piece(2, 0, y, 1, inner_z)
        swap(0, far, 0)
        wait_y(0, near)

    pl.when(jnp.logical_not(inner))(outside)
    project(near, False)

    def outside():
        swap(0, far, 1)
        swap(0, far, 2)
        wait_y(1, inner_z)
        own_piece(0, 1, 1 - y, 0, inner_z)
        swap(0, far, 3)
        own_piece(0, 1, 1 - y, 1, inner_z)
        own_piece(0, 1, 1 - y, 2, inner_z)
        swap(1, near, 0)
        scales_in()
        own_piece(0, 1, 1 - y, 3, inner_z)
        swap(2, inner_z, 0)
        wait_y(0, far)

    pl.when(jnp.logical_not(inner))(outside)
    project(far, False)

    def inside():
        own_piece(2, 0, y, 0, near)

    def outside():
        own_piece(1, 1, 1 - y, 0, inner_z)

    by_role(inside, outside)
    retain(0)

    def inside():
        swap(1, near, 0)

    def outside():
        swap(2, inner_z, 1)

    by_role(inside, outside)
    retain(1)

    def inside():
        own_piece(2, 0, y, 1, near)

    pl.when(inner)(inside)
    retain(2)
    retain(3)

    def inside():
        row_depth(0)
        cross(2, 0, 0)
        row_depth(1)
        swap(1, near, 1)
        row_line(0)
        cross(2, 0, 1)
        row_depth(2)
        row_line(1)
        row_depth(3)
        own_piece(2, 1, y, 0, near)
        row_line(2)
        swap(1, far, 0)
        row_last(0)

    def outside():
        swap(1, near, 1)
        row_line(0)
        row_line(1)
        wait_y(2, inner_z)
        row_line(2)
        swap(1, far, 0)
        row_line(3)
        wait_y(1, near)
        swap(1, far, 1)
        row_depth(0)
        own_piece(1, 1, 1 - y, 1, inner_z)
        row_depth(1)
        row_depth(2)
        row_depth(3)
        own_piece(2, 1, y, 0, inner_z)
        wait_y(1, far)
        row_last(0)

    by_role(inside, outside)
    norm_ffn(0)

    def inside():
        own_piece(2, 1, y, 1, near)
        row_line(3)
        row_last(1)

    def outside():
        own_piece(2, 1, y, 1, inner_z)
        row_last(1)

    by_role(inside, outside)
    norm_ffn(1)

    def inside():
        row_last(2)

    def outside():
        row_last(2)

    by_role(inside, outside)
    norm_ffn(2)

    def inside():
        wait_y(1, near)
        swap(1, far, 1)
        row_last(3)
        inwards(2, near, 0)

    def outside():
        own_piece(2, 1, 1 - y, 0, inner_z)
        row_last(3)

    by_role(inside, outside)
    norm_ffn(3)
    own_resid()

    def inside():
        inwards(2, near, 1)
        wait_pair(1)
        inwards(2, far, 0)
        cross(2, 1, 0)
        wait_y(1, far)

    def outside():
        own_piece(2, 1, 1 - y, 1, inner_z)

    by_role(inside, outside)
    hidden_rows(0)

    def inside():
        inwards(2, far, 1)
        cross(2, 1, 1)

    def outside():
        swap(2, near, 0)

    by_role(inside, outside)
    hidden_rows(1)

    def inside():
        swap(2, near, 0)

    def outside():
        swap(2, near, 1)

    by_role(inside, outside)
    down(0, cells[0])
    down(1, cells[1])

    def outside():
        swap(2, far, 0)

    pl.when(jnp.logical_not(inner))(outside)
    pair(0)

    def inside():
        swap(2, near, 1)

    pl.when(inner)(inside)
    down(2, cells[2])
    pair(1)

    def inside():
        wait_pair(2)
        cross_last()

    pl.when(inner)(inside)
    down(3, cells[3])

    def inside():
        swap(2, far, 0)

    pl.when(inner)(inside)
    pair(2)

    def outside():
        swap(2, far, 1)

    pl.when(jnp.logical_not(inner))(outside)
    pair(3)
    down(4, cells[4])

    def inside():
        take_last()

    def outside():
        wait_y(2, near)

    by_role(inside, outside)
    pair(4)
    finish(0, cells[0])

    def inside():
        wait_y(2, near)

    pl.when(inner)(inside)
    down(5, cells[5])
    pair(5)

    def outside():
        wait_y(2, far)

    pl.when(jnp.logical_not(inner))(outside)
    finish(1, cells[1])
    down(6, cells[6])

    def inside():
        wait_last()

    pl.when(inner)(inside)
    pair(6)
    finish(2, cells[2])
    down(7, cells[7])
    pair(7)
    finish(3, cells[3])
    finish(4, cells[4])
    finish(5, cells[5])
    finish(6, cells[6])
    finish(7, cells[7])
    for cell in range(8):
        out[:, cell * part_width : (cell + 1) * part_width] = final[cell].astype(jnp.bfloat16)

    token_copy(mine).wait_send()
    scale_copy(0, z, pair_z).wait_send()

    def inside():
        scale_copy(1, z, near).wait_send()
        scale_copy(2, outer_z, near).wait_send()
        scale_copy(3, near, outer_z).wait_send()
        scale_copy(4, far, outer_z).wait_send()
        for matrix in range(3):
            for number in numbers(matrix, y):
                for part in range(2):
                    z_copy(matrix, part, z, number, near).wait_send()
                    z_copy(matrix, part, outer_z, number, near).wait_send()
                for block in (z, near, far):
                    z_copy(matrix, 0, block, number, outer_z, True).wait_send()
                y_copy(matrix, near, number).wait_send()
            for number in numbers(matrix, y)[: -1 if matrix == 2 else None]:
                y_copy(matrix, far, number).wait_send()
        z_copy(2, 1, outer_z, numbers(2, 1 - y)[1], near).wait_send()

    def outside():
        for matrix in range(3):
            for part, half in ((0, y), (1, y), (1, 1 - y)):
                for number in numbers(matrix, half):
                    z_copy(matrix, part, z, number, inner_z).wait_send()
            for number in numbers(matrix, y):
                for block in (inner_z, near, far):
                    y_copy(matrix, block, number).wait_send()

    by_role(inside, outside)
    for step in range(1, 4):
        norm_copy(step, t).wait_send()
    for way in range(7):
        for s in range(4):
            row_copy(way, s, t, {"tp": partner}).wait_send()
    for k in range(8):
        core_copy(k).wait_send()
        for way in range(3):
            line_copy(k, way).wait_send()


ANYWHERE = pl.BlockSpec(memory_space=pl.ANY)
INSIDE = pl.BlockSpec(memory_space=pltpu.VMEM)


def tables(heads):
    places = np.arange(LEN, dtype=np.float64)
    half = DK // 2
    frequency = (THETA ** (-(np.arange(half) / half))).astype(np.float32)
    angle = (places[:, None].astype(np.float32) * frequency).astype(np.float32)
    distance = places[:, None] - places[None, :]
    gamma = 1.0 - 2.0 ** (-5.0 - np.arange(heads, dtype=np.float64))
    powers = gamma[:, None, None] ** np.maximum(distance, 0.0)
    decay = np.where(distance >= 0, powers, 0.0) * DK ** (-0.5)
    wide = angle.astype(np.float64)
    return (
        decay.astype(np.float32),
        np.cos(wide).astype(np.float32),
        np.sin(wide).astype(np.float32),
    )


def layer(stream, gains, mix_w, mix_scales, up_w, up_scales, w_down, scale_down, tp_count):
    group, width = stream.shape
    share = group // tp_count
    depth, heads_width = mix_w[0].shape
    units = w_down.shape[0]
    blocks = width // depth
    narrow, wide = jnp.bfloat16, jnp.float32
    local_heads = heads_width // DK
    decays, cosine, sine = tables(local_heads * tp_count)
    row = lambda vector: vector[None, :]
    most = max(PIECES)
    dma = pltpu.SemaphoreType.DMA
    half_units = units // 2
    cells = 2 * blocks
    part = depth // 2
    scratch = (
        [pltpu.VMEM(w.shape, wide) for w in mix_w]
        + [
            pltpu.VMEM((4 * half_units, depth), wide),
            pltpu.VMEM((4 * half_units, part), wide),
            pltpu.VMEM((2 * group, width), narrow),
            pltpu.VMEM((1, LEN, LEN), wide),
            pltpu.VMEM(cosine.shape, wide),
            pltpu.VMEM(sine.shape, wide),
            *(pltpu.VMEM((1, width), wide) for _ in gains),
            *(pltpu.VMEM((1, heads_width), wide) for _ in mix_scales),
            pltpu.VMEM((1, depth), wide),
            *(pltpu.VMEM(scale.shape, wide) for scale in up_scales),
            pltpu.VMEM((2 * width, 3 * DK), narrow),
            pltpu.VMEM((cells * units, depth), narrow),
            pltpu.VMEM((cells * units, part), narrow),
            pltpu.VMEM((blocks, 2 * group, depth), narrow),
            pltpu.VMEM((2 * group, 3 * DK), wide),
            pltpu.VMEM((cells, 2 * group, DV), narrow),
            pltpu.VMEM((cells, share, part), wide),
            pltpu.VMEM((share, width), wide),
            pltpu.VMEM((2 * group, width), narrow),
            pltpu.VMEM((2 * group, half_units), narrow),
            pltpu.VMEM((cells, 2, 4, share, part), narrow),
            pltpu.VMEM((cells, 4, share, part), narrow),
            pltpu.VMEM((cells, 3, share, part), narrow),
            pltpu.VMEM((cells, 3, share, part), narrow),
            pltpu.VMEM((cells, share, part), wide),
            pltpu.VMEM((cells, 1, part), wide),
        ]
        + [
            dma((29,)),
            dma((3, 8, most)), dma((3, 4, most)), dma((3, 8, most)),
            dma((3, 4, most)), dma((3, 4, most)),
            dma((5,)), dma((4,)), dma((1,)), dma((1,)), dma((3,)), dma((3,)),
            dma((7, 4)), dma((7, 4)),
            dma((8,)), dma((8,)), dma((8, 3)), dma((8, 3)),
        ]
    )
    return pl.pallas_call(
        layer_kernel,
        out_shape=pltpu.VMEM((share, width), narrow),
        in_specs=[ANYWHERE] * 18,
        out_specs=INSIDE,
        scratch_shapes=scratch,
        compiler_params=pltpu.CompilerParams(
            collective_id=0, has_side_effects=True, vmem_limit_bytes=56 * 2**20
        ),
    )(
        stream, *mix_w, *up_w, w_down, decays, cosine, sine, *(row(gain) for gain in gains),
        *(row(scale) for scale in mix_scales), *up_scales, row(scale_down),
    )


def summed_over_tp(partial_sum, share):
    partial_sum = partial_sum.reshape(-1, share, partial_sum.shape[1])
    pieces = lax.all_to_all(partial_sum, "tp", split_axis=0, concat_axis=0)
    return jnp.sum(pieces.astype(jnp.float32), axis=0)


def shards(
    stream,
    gain_mix,
    w_query,
    scale_query,
    w_key,
    scale_key,
    w_value,
    scale_value,
    gain_ffn,
    w_gate,
    scale_gate,
    w_up,
    scale_up,
    w_down,
    scale_down,
):
    group_rows = stream.shape[0]
    tp_count = lax.axis_size("tp")
    if (lax.axis_size("rep"), lax.axis_size("fs"), tp_count) == (2, 4, 4):
        return layer(
            stream, (gain_mix, gain_ffn), (w_query, w_key, w_value),
            (scale_query, scale_key, scale_value), (w_gate.T, w_up.T), (scale_gate, scale_up),
            w_down.T, scale_down, tp_count,
        )
    stream_f = stream.astype(jnp.float32)
    normed = (stream_f * rms_scale(stream_f) * gain_mix).astype(jnp.bfloat16)
    mix_w = jnp.concatenate([w.astype(jnp.bfloat16) for w in (w_query, w_key, w_value)], axis=1)
    up_w = jnp.concatenate([w.astype(jnp.bfloat16) for w in (w_gate, w_up)], axis=1)
    down_w = w_down.astype(jnp.bfloat16)
    down_scale = lax.all_gather(scale_down, "fs", axis=0, tiled=True)
    mix_acc = dot(normed, lax.all_gather(mix_w, "fs", axis=0, tiled=True))
    mix_scale = jnp.concatenate([scale_query, scale_key, scale_value])
    query, key, value = jnp.split(
        (mix_acc * mix_scale).astype(jnp.bfloat16),
        [w_query.shape[1], w_query.shape[1] + w_key.shape[1]],
        axis=1,
    )
    local_heads = query.shape[1] // DK
    positions = jnp.arange(group_rows, dtype=jnp.int32) % LEN
    mixed = []
    for head in range(local_heads):
        columns = slice(head * DK, (head + 1) * DK)
        queries = rotate(query[:, columns].astype(jnp.float32), positions)
        keys = rotate(key[:, columns].astype(jnp.float32), positions) * DK ** (-0.5)
        values = value[:, head * DV : (head + 1) * DV].astype(jnp.float32)
        head_id = (lax.axis_index("tp") * local_heads + head).astype(jnp.float32)
        log_decay = jnp.log(1.0 - jnp.power(2.0, -5.0 - head_id))
        retained = retention(queries, keys, values, log_decay)
        mixed.append((retained * head_scale(retained)).astype(jnp.bfloat16))
    mixed = jnp.concatenate(mixed, axis=1)
    share = group_rows // tp_count
    own_rows = lax.dynamic_slice_in_dim(stream, lax.axis_index("tp") * share, share, 0)
    arrived = lax.all_to_all(mixed, "tp", split_axis=0, concat_axis=1, tiled=True)
    resid = own_rows.astype(jnp.float32) + arrived.astype(jnp.float32)
    normed_ffn = (resid * rms_scale(resid) * gain_ffn).astype(jnp.bfloat16)
    piece = lax.all_gather(normed_ffn, "tp", axis=0, tiled=True)
    up_acc = dot(piece, lax.all_gather(up_w, "fs", axis=0, tiled=True))
    units = w_gate.shape[1]
    gate = up_acc[:, :units] * scale_gate
    upward = up_acc[:, units:] * scale_up
    hidden = (jax.nn.silu(gate) * upward).astype(jnp.bfloat16)
    whole = dot_t(hidden, lax.all_gather(down_w, "fs", axis=0, tiled=True))
    channel_out = summed_over_tp((whole * down_scale).astype(jnp.bfloat16), share)
    return (resid + channel_out).astype(jnp.bfloat16)


def solution(mesh):
    placed = (
        P(("rep", "fs"), None),
        P(),
        P("fs", "tp"),
        P("tp"),
        P("fs", "tp"),
        P("tp"),
        P("fs", "tp"),
        P("tp"),
        P(),
        P("fs", "tp"),
        P("tp"),
        P("fs", "tp"),
        P("tp"),
        P("fs", "tp"),
        P("fs"),
    )
    return jax.shard_map(
        shards, mesh=mesh, in_specs=placed, out_specs=P(("rep", "fs", "tp"), None), check_vma=False
    )
```
